256 devices in a mesh: sp: 64 (over z, x, core), tp: 4 (over y).
Axes of the slice: x: 4, y: 4, z: 8, core: 2. Of those that a mesh axis runs over, the one named last changes fastest.
Arguments:
- residual: bfloat16 [16384, 2048], P(('sp', 'tp')), may hold values from -6 to 6
- query_wide: bfloat16 [16384, 512], P('sp', 'tp'), may hold values from -8 to 8
- key_wide: bfloat16 [16384, 512], P('sp', 'tp'), may hold values from -8 to 8
- value_wide: bfloat16 [16384, 512], P('sp', 'tp'), may hold values from -6 to 6
- query_narrow: bfloat16 [16384, 512], P('sp', 'tp'), may hold values from -8 to 8
- key_narrow: bfloat16 [16384, 512], P('sp', 'tp'), may hold values from -8 to 8
- value_narrow: bfloat16 [16384, 512], P('sp', 'tp'), may hold values from -6 to 6
- gate_wide: float32 [16384, 4], P('sp', 'tp'), may hold values from -2 to 20
- gate_narrow: float32 [16384, 8], P('sp', 'tp'), may hold values from -2 to 20
- out_wide: bfloat16 [512, 2048], replicated, may hold values from -0.1875 to 0.1875
- out_narrow: bfloat16 [512, 2048], replicated, may hold values from -0.1875 to 0.1875
- norm_gain: float32 [2048], replicated, may hold values from 0.1 to 1.9
- routing: int32 [16384, 2], P(('sp', 'tp')), may hold values from 0 to 63, as said below
- route_weight: float32 [16384, 2], P(('sp', 'tp')), may hold values from 0.3 to 1.5
- gate_weight: bfloat16 [64, 2048, 1024], P('sp', None, 'tp'), may hold values from -0.125 to 0.125
- up_weight: bfloat16 [64, 2048, 1024], P('sp', None, 'tp'), may hold values from -0.125 to 0.125
- down_weight: bfloat16 [64, 1024, 2048], P('sp', 'tp'), may hold values from -0.1875 to 0.1875
Outputs:
- result: bfloat16 [16384, 2048], P(('sp', 'tp'))
The draws below stay inside these ranges and needn't reach their ends.
Inputs may be any that keep to these rules, and one draw needn't show every extreme that they name: `routing`: each row names 2 different experts of one group (experts g * 16 to g * 16 + 15). In each aligned block of 64 rows (the rows of one device) no expert is named by more than 4 rows; one group, the same for all blocks, has each of its experts named by exactly 4 rows of every block.
All inputs are finite; a program needn't handle non-finite values.
Results may differ from the reference program's by a relative error of at most 0.017.
Values may be sent and summed in bfloat16 or wider, within the bound.
A program may use at most 128 MiB of HBM per device.

```python
import math
import jax
import jax.numpy as jnp
from jax import lax

D = 2048
WIDE = 4
HW = 128
NARROW = 8
HN = 64
FFE = 1024
GROUPS = 4
TOP = 2
TOK_DEV = 256
TOKENS = 16384
EXPERTS = 64
EPG = 16
ROWS_DEV = 64
CAP = 4
N_TP = 4


def projected(key, breadth, salt_value):
    values = 1.7 * jax.random.normal(jax.random.fold_in(key, salt_value), (TOKENS, breadth), jnp.float32)
    values = jnp.clip(values, -8.0, 8.0)
    return values.astype(jnp.bfloat16)


def forget(key, head_count, salt_value):
    seeded = jax.random.fold_in(key, salt_value)
    order_key, drift_key, jitter_key = jax.random.split(seeded, 3)
    ranking = jax.random.permutation(order_key, head_count)
    keeping = head_count // 2
    baseline = jnp.where(ranking < keeping, jnp.log(1.0 * TOKENS), jnp.log(40.0))
    shards = TOKENS // TOK_DEV
    drift_part = jax.random.uniform(drift_key, (shards, 1, head_count), jnp.float32, -0.8, 0.8)
    drift_part = jnp.broadcast_to(drift_part, (shards, TOK_DEV, head_count)).reshape(TOKENS, head_count)
    jitter = jnp.clip(jax.random.normal(jitter_key, (TOKENS, head_count), jnp.float32), -4.0, 4.0)
    return (baseline[None, :] + drift_part + jitter).astype(jnp.float32)


def draw_query_wide(key, part):
    return projected(key, WIDE * HW, 11)


def draw_key_wide(key, part):
    return projected(key, WIDE * HW, 12)


def draw_query_narrow(key, part):
    return projected(key, NARROW * HN, 21)


def draw_key_narrow(key, part):
    return projected(key, NARROW * HN, 22)


def draw_gate_wide(key, part):
    return forget(key, WIDE, 31)


def draw_gate_narrow(key, part):
    return forget(key, NARROW, 32)


def route_block(key, full_group):
    cut_key, label_key, row_key = jax.random.split(key, 3)
    half_rows = ROWS_DEV // 2
    ordinal = jnp.arange(ROWS_DEV, dtype=jnp.int32)
    cut_points = jnp.sort(jax.random.randint(cut_key, (GROUPS - 2,), 0, half_rows + 1))
    remainder = ordinal - half_rows
    other_group = jnp.sum((remainder[:, None] >= cut_points[None, :]).astype(jnp.int32), axis=1)
    group_starts = jnp.concatenate([jnp.zeros((1,), jnp.int32), cut_points.astype(jnp.int32)])
    in_full = ordinal < half_rows
    ranking = jnp.where(in_full, ordinal, remainder - group_starts[other_group])
    chosen_group = jnp.where(in_full, full_group, (full_group + 1 + other_group) % GROUPS)

    def labels_of(group_number):
        return jax.random.permutation(jax.random.fold_in(label_key, group_number), EPG)
    labels = jax.vmap(labels_of)(jnp.arange(GROUPS, dtype=jnp.int32))
    slot_number = TOP * ranking[:, None] + jnp.arange(TOP, dtype=jnp.int32)[None, :]
    local_expert = labels[chosen_group[:, None], slot_number % EPG]
    expert_ids = (chosen_group[:, None] * EPG + local_expert).astype(jnp.int32)
    shuffled = jax.random.permutation(row_key, ROWS_DEV)
    return jnp.zeros((ROWS_DEV, TOP), jnp.int32).at[shuffled].set(expert_ids)


def draw_routing(key, part):
    seeded = jax.random.fold_in(key, 4242)
    full_group = jax.random.randint(jax.random.fold_in(seeded, 1), (), 0, GROUPS)

    def one_block(block_number):
        return route_block(jax.random.fold_in(seeded, block_number + 2), full_group)
    blocks = jax.vmap(one_block)(jnp.arange(TOKENS // ROWS_DEV, dtype=jnp.int32))
    return blocks.reshape(TOKENS, TOP)


def block_scale(own_key, dims, cuts, low, largest):
    loudness, own = 1.0, jax.random.fold_in(own_key, 6)
    for axis_at, shards_of in cuts:
        heights = jnp.exp(jax.random.uniform(jax.random.fold_in(own, axis_at), (shards_of,), jnp.float32, low / len(cuts), largest / len(cuts)))
        loudness = loudness * jnp.repeat(heights, dims[axis_at] // shards_of).reshape([-1 if axis == axis_at else 1 for axis in range(len(dims))])
    return loudness


def bell_draw(stream_key, shape, scale, most, cuts=(), kind=jnp.bfloat16):
    array = jax.random.normal(stream_key, shape, jnp.float32) * scale
    if len(cuts) > 0:
        array = block_scale(stream_key, shape, cuts, -0.22, 0.18) * array
    return jnp.clip(array, min=-most, max=most).astype(kind)


def setup_inputs(seed: int = 0) -> dict:
    key_list = jax.random.split(jax.random.key(seed), 18)
    return {
        "residual": bell_draw(key_list[0], (TOKENS, D), 1.0, 6.0, ((0, 256),)),
        "query_wide": draw_query_wide(jax.random.fold_in(key_list[17], 71), 0),
        "key_wide": draw_key_wide(jax.random.fold_in(key_list[17], 71), 0),
        "value_wide": bell_draw(key_list[3], (TOKENS, WIDE * HW), 1.0, 6.0, ((0, 64), (1, 4))),
        "query_narrow": draw_query_narrow(jax.random.fold_in(key_list[17], 71), 0),
        "key_narrow": draw_key_narrow(jax.random.fold_in(key_list[17], 71), 0),
        "value_narrow": bell_draw(key_list[6], (TOKENS, NARROW * HN), 1.0, 6.0, ((0, 64), (1, 4))),
        "gate_wide": draw_gate_wide(jax.random.fold_in(key_list[17], 71), 0),
        "gate_narrow": draw_gate_narrow(jax.random.fold_in(key_list[17], 71), 0),
        "out_wide": bell_draw(key_list[9], (WIDE * HW, D), (WIDE * HW + NARROW * HN) ** -0.5, 0.1875),
        "out_narrow": bell_draw(key_list[10], (NARROW * HN, D), (WIDE * HW + NARROW * HN) ** -0.5, 0.1875),
        "norm_gain": jnp.clip(1.0 + 0.18 * jax.random.normal(key_list[11], (D,), jnp.float32), 0.1, 1.9),
        "routing": draw_routing(jax.random.fold_in(key_list[17], 71), 0),
        "route_weight": jnp.clip(jnp.exp(math.log(1.5) - 1.60943787 * jax.random.uniform(key_list[13], (TOKENS, TOP), jnp.float32) ** block_scale(key_list[13], (TOKENS, TOP), ((0, 256),), -0.2, 0.2)), 0.3, 1.5),
        "gate_weight": bell_draw(key_list[14], (EXPERTS, D, FFE), D ** -0.5, 0.125, ((0, 64), (2, 4))),
        "up_weight": bell_draw(key_list[15], (EXPERTS, D, FFE), D ** -0.5, 0.125, ((0, 64), (2, 4))),
        "down_weight": bell_draw(key_list[16], (EXPERTS, FFE, D), FFE ** -0.5, 0.1875, ((0, 64), (1, 4))),
    }


epsilon = 1e-06

def attend(queries, keys, values, gates, head_width):
    length = queries.shape[0]
    head_count = gates.shape[1]
    decay = jnp.cumsum(jax.nn.log_sigmoid(gates.astype(jnp.float32)), axis=0)
    grid_query = queries.reshape(length, head_count, head_width).astype(jnp.float32)
    grid_key = keys.reshape(length, head_count, head_width).astype(jnp.float32)
    grid_value = values.reshape(length, head_count, head_width).astype(jnp.float32)
    block_size = math.gcd(length, 512)
    key_place = jnp.arange(length, dtype=jnp.int32)

    def one_block(position):
        begin = (position * block_size).astype(jnp.int32)
        part_query = lax.dynamic_slice_in_dim(grid_query, begin, block_size, 0)
        part_decay = lax.dynamic_slice_in_dim(decay, begin, block_size, 0)
        scores = jnp.einsum('thd,phd->htp', part_query, grid_key) * head_width ** (-0.5)
        scores = scores + part_decay.T[:, :, None] - decay.T[:, None, :]
        query_place = begin + jnp.arange(block_size, dtype=jnp.int32)
        scores = jnp.where(key_place[None, None, :] <= query_place[None, :, None], scores, -jnp.inf)
        weights = jnp.exp(scores - lax.optimization_barrier(jnp.max(scores, axis=2, keepdims=True)))
        weight_sum = lax.optimization_barrier(jnp.sum(weights, axis=2))
        rounded = lax.optimization_barrier(weights.astype(jnp.bfloat16)).astype(jnp.float32)
        mixed_heads = jnp.einsum('htp,phd->htd', rounded, grid_value) / weight_sum[:, :, None]
        return jnp.transpose(mixed_heads, (1, 0, 2)).reshape(block_size, head_count * head_width).astype(jnp.bfloat16)
    blocks = lax.map(one_block, jnp.arange(length // block_size, dtype=jnp.int32))
    return blocks.reshape(length, head_count * head_width)

def experts_apply(normed, routing, route_weight, gate_weight, up_weight, down_weight):
    length = normed.shape[0]
    chosen_count = routing.shape[1]
    expert_count = gate_weight.shape[0]
    flat_routes = routing.reshape(-1).astype(jnp.int32)
    matches = (flat_routes[:, None] == jnp.arange(expert_count, dtype=jnp.int32)[None, :]).astype(jnp.int32)
    ranking = lax.optimization_barrier(jnp.sum((jnp.cumsum(matches, axis=0) - matches) * matches, axis=1)).astype(jnp.int32)
    capacity_all = length // ROWS_DEV * CAP
    lookup = jnp.full((expert_count, capacity_all), length * chosen_count, jnp.int32)
    lookup = lookup.at[flat_routes, ranking].set(jnp.arange(length * chosen_count, dtype=jnp.int32))
    flat_weights = route_weight.reshape(-1)

    def one_expert(carried, pieces):
        copies, gate_part, up_part, down_part = pieces
        positions = (copies // chosen_count).astype(jnp.int32)
        chosen_rows = jnp.take(normed, positions, axis=0, mode='clip')
        gate_value = jnp.dot(chosen_rows, gate_part, preferred_element_type=jnp.float32)
        up_value = jnp.dot(chosen_rows, up_part, preferred_element_type=jnp.float32)
        hidden = (jax.nn.silu(gate_value) * up_value).astype(jnp.bfloat16)
        hidden_blocks = hidden.reshape(capacity_all, N_TP, -1).astype(jnp.float32)
        down_blocks = down_part.reshape(N_TP, -1, down_part.shape[1]).astype(jnp.float32)
        partial_out = jnp.einsum('lnf,nfd->nld', hidden_blocks, down_blocks)
        partial_out = lax.optimization_barrier(partial_out.astype(jnp.bfloat16)).astype(jnp.float32)
        expert_out = lax.optimization_barrier(jnp.sum(partial_out, axis=0)).astype(jnp.bfloat16)
        scale = jnp.take(flat_weights, copies, mode='fill', fill_value=0.0)
        carried = carried.at[positions].add(scale[:, None] * expert_out.astype(jnp.float32), mode='drop')
        return (carried, None)
    start = jnp.zeros((length, normed.shape[1]), jnp.float32)
    total, _ = lax.scan(one_expert, start, (lookup, gate_weight, up_weight, down_weight))
    return total

def reference(residual, query_wide, key_wide, value_wide, query_narrow, key_narrow, value_narrow, gate_wide, gate_narrow, out_wide, out_narrow, norm_gain, routing, route_weight, gate_weight, up_weight, down_weight):
    att_wide = attend(query_wide, key_wide, value_wide, gate_wide, HW)
    att_narrow = attend(query_narrow, key_narrow, value_narrow, gate_narrow, HN)
    mixed = jnp.dot(att_wide, out_wide, preferred_element_type=jnp.float32)
    mixed = mixed + jnp.dot(att_narrow, out_narrow, preferred_element_type=jnp.float32)
    middle = (residual.astype(jnp.float32) + mixed).astype(jnp.bfloat16)
    middle_wide = middle.astype(jnp.float32)
    spread = lax.optimization_barrier(jnp.mean(middle_wide * middle_wide, axis=1, keepdims=True))
    normed = (middle_wide * lax.rsqrt(spread + epsilon) * norm_gain).astype(jnp.bfloat16)
    routed = experts_apply(normed, routing, route_weight, gate_weight, up_weight, down_weight)
    return (middle_wide + routed).astype(jnp.bfloat16)
```

```python
import functools
import math

import jax
import jax.numpy as jnp
from jax import lax
from jax.experimental import pallas as pl
from jax.experimental.pallas import tpu as pltpu
from jax.sharding import PartitionSpec as P

MESH = pl.DeviceIdType.MESH
F32, BF16 = jnp.float32, jnp.bfloat16
HW = 128
HN = 64
GROUPS = 4
LOG2E = math.log2(math.e)
NEG = -1e30
epsilon = 1e-06


def attention_kernel(
    dims, q_ref, kd_ref, v_ref, tot_ref, att_ref,
    qb, kb, vb, tt, drow, mb, acc, ob, sb, orv, srv, ab, ar,
    q_s, q_r, up_s, up_r, dn_s, dn_r, pr_s, pr_r, t1_s, t1_r, t2_s, t2_r, o_s, o_r, y_s, y_r, loc,
):
    nz, nx, ny = dims
    half = nz // 2
    sp, y = lax.axis_index("sp"), lax.axis_index("tp")
    c = lax.rem(sp, 2)
    x = lax.rem(sp // 2, nx)
    z = sp // (2 * nx)
    xc = x * 2 + c

    def at(z_, x_, c_, y_):
        return ((z_ * nx + x_) * 2 + c_, y_)

    def zup(i):
        return lax.rem(z + i, nz)

    def zdn(i):
        return lax.rem(z - i + nz, nz)

    def in_plane(i):
        other = lax.rem(xc + i, 2 * nx)
        return at(z, other // 2, lax.rem(other, 2), y)

    def remote(src, dst, send, recv, device):
        return pltpu.make_async_remote_copy(
            src_ref=src, dst_ref=dst, send_sem=send, recv_sem=recv, device_id=device, device_id_type=MESH
        )

    barrier = pltpu.get_barrier_semaphore()

    def greet(device):
        pl.semaphore_signal(barrier, inc=1, device_id=device, device_id_type=MESH)

    for i in range(1, nz):
        greet(at(zup(i), x, c, y))
    for i in range(1, 2 * nx):
        greet(in_plane(i))
    for i in range(1, ny):
        greet(at(z, x, c, lax.rem(y + i, ny)))
    pl.semaphore_wait(barrier, nz - 1 + 2 * nx - 1 + ny - 1)

    up_dev, dn_dev, pr_dev = at(zup(1), x, c, y), at(zdn(1), x, c, y), at(z, x, 1 - c, y)

    def up_copy(s, j):
        zb = zdn(s)
        src = (kb, vb)[j].at[zb, c]
        return remote(src, src, up_s.at[s, j], up_r.at[s, j], up_dev)

    def dn_copy(s, j):
        zb = zup(s)
        src = (kb, vb)[j].at[zb, c]
        return remote(src, src, dn_s.at[s, j], dn_r.at[s, j], dn_dev)

    def pr_copy(zb, j):
        src = (kb, vb)[j].at[zb, c]
        return remote(src, src, pr_s.at[zb, j], pr_r.at[zb, j], pr_dev)

    def pr_wait(zb, j):
        dst = (kb, vb)[j].at[zb, 1 - c]
        remote(dst, dst, pr_s.at[zb, j], pr_r.at[zb, j], pr_dev).wait_recv()

    def own_up(j):
        return remote((kd_ref, v_ref)[j], (kb, vb)[j].at[z, c], up_s.at[0, j], up_r.at[0, j], up_dev)

    def own_dn(j):
        return remote((kd_ref, v_ref)[j], (kb, vb)[j].at[z, c], dn_s.at[0, j], dn_r.at[0, j], dn_dev)

    def own_pr(j):
        return remote((kd_ref, v_ref)[j], (kb, vb)[j].at[z, c], pr_s.at[z, j], pr_r.at[z, j], pr_dev)

    def up_has(s, j):
        return s < half or (s == half and j == 0)

    def dn_has(s, j):
        return s < half or (s == half and j == 1)

    for j in range(2):
        if up_has(1, j):
            own_up(j).start()
        if dn_has(1, j):
            own_dn(j).start()

    def t1_copy(i):
        return remote(tot_ref, tt.at[z, xc], t1_s.at[i - 1], t1_r.at[i - 1], in_plane(i))

    def t2_copy(i):
        return remote(tt.at[z], tt.at[z], t2_s.at[i - 1], t2_r.at[i - 1], at(zup(i), x, c, y))

    def q_copy(i):
        return remote(q_ref, qb.at[x], q_s.at[i - 1], q_r.at[i - 1], at(z, lax.rem(x + i, nx), c, y))

    for i in range(1, 2 * nx):
        t1_copy(i).start()
    for i in range(1, nx):
        q_copy(i).start()
    for j in range(2):
        own_pr(j).start()
    local = [
        pltpu.make_async_copy(tot_ref, tt.at[z, xc], loc.at[0]),
        pltpu.make_async_copy(q_ref, qb.at[x], loc.at[1]),
        pltpu.make_async_copy(kd_ref, kb.at[z, c], loc.at[2]),
        pltpu.make_async_copy(v_ref, vb.at[z, c], loc.at[3]),
    ]
    for copy in local:
        copy.start()
    mb[...] = jnp.full(mb.shape, NEG, F32)
    acc[...] = jnp.zeros(acc.shape, F32)
    local[0].wait()
    for i in range(1, 2 * nx):
        other = lax.rem(xc - i + 2 * nx, 2 * nx)
        remote(tot_ref, tt.at[z, other], t1_s.at[i - 1], t1_r.at[i - 1], in_plane(i)).wait_recv()
    for i in range(1, nz):
        t2_copy(i).start()
    for copy in local[1:]:
        copy.wait()

    def relay(s):
        for j in range(2):
            if up_has(s, j):
                slot = (kb, vb)[j].at[zdn(s), c]
                remote(slot, slot, up_s.at[s - 1, j], up_r.at[s - 1, j], up_dev).wait_recv()
                if up_has(s + 1, j):
                    up_copy(s, j).start()
                pr_copy(zdn(s), j).start()
            if dn_has(s, j):
                slot = (kb, vb)[j].at[zup(s), c]
                remote(slot, slot, dn_s.at[s - 1, j], dn_r.at[s - 1, j], dn_dev).wait_recv()
                if dn_has(s + 1, j):
                    dn_copy(s, j).start()
                pr_copy(zup(s), j).start()

    lane = lax.broadcasted_iota(jnp.int32, (1, 128), 1)
    low = lane < HN

    def head_offsets(zb):
        def plane(p, run):
            whole = jnp.zeros((1, 128), F32)
            for k in range(2 * nx):
                whole = whole + tt[p, k]
            return run + jnp.where(p < zb, whole, 0.0)
        run = lax.fori_loop(0, nz, plane, jnp.zeros((1, 128), F32))
        for k in range(2 * nx):
            run = run + jnp.where(k < 2 * x, tt[zb, k], 0.0)
        return run, run + tt[zb, 2 * x]

    def make_drow(zb):
        offs = head_offsets(zb)
        parts = [kb[zb, k, pl.ds(256, 16), :].astype(F32) for k in range(2)]
        for h in range(3):
            pieces = []
            for k in range(2):
                off = jnp.sum(jnp.where(lane == h, offs[k], 0.0), axis=1, keepdims=True)
                p = parts[k]
                pieces.append(p[3 * h:3 * h + 1] + p[3 * h + 1:3 * h + 2] + p[3 * h + 2:3 * h + 3] + off)
            drow[h] = jnp.concatenate(pieces, axis=1)

    scales = (HW ** -0.5 * LOG2E, HN ** -0.5 * LOG2E, HN ** -0.5 * LOG2E)

    def tile(zb, xq, masked):
        q = qb[xq]
        qw, qn = q[:, :128], q[:, 128:]
        zero = jnp.zeros_like(qn)
        heads = (qw, jnp.where(low, qn, zero), jnp.where(low, zero, qn))
        keys = jnp.concatenate([kb[zb, 0, :256, :], kb[zb, 1, :256, :]], axis=0)
        vals = jnp.concatenate([vb[zb, 0], vb[zb, 1]], axis=0)
        ones = jnp.ones((512, 128), BF16)
        if masked:
            rows = lax.broadcasted_iota(jnp.int32, (256, 512), 0) + (xq * 512 + c * 256)
            cols = lax.broadcasted_iota(jnp.int32, (256, 512), 1) + x * 512
            seen = cols <= rows
        for h in range(3):
            side = slice(0, 128) if h == 0 else slice(128, 256)
            s = lax.dot_general(heads[h], keys[:, side], (((1,), (1,)), ((), ())), preferred_element_type=F32)
            r = s * scales[h] - drow[h]
            if masked:
                r = jnp.where(seen, r, NEG)
            old = mb[xq, h]
            new = jnp.maximum(old, jnp.max(r, axis=1, keepdims=True))
            p = jnp.exp2(r - jnp.concatenate([new] * 4, axis=1)).astype(BF16)
            shrink = jnp.exp2(old - new)
            mb[xq, h] = new
            right = jnp.concatenate([vals[:, side], ones], axis=1)
            pv = jnp.dot(p, right, preferred_element_type=F32)
            acc[xq, h] = acc[xq, h] * jnp.concatenate([shrink, shrink], axis=1) + pv

    def both(zb):
        make_drow(zb)

        def one(xq, carry):
            tile(zb, xq, False)
            return carry
        lax.fori_loop(0, nx, one, 0)

    relay(1)
    for i in range(1, nx):
        src = lax.rem(x - i + nx, nx)
        remote(q_ref, qb.at[src], q_s.at[i - 1], q_r.at[i - 1], at(z, src, c, y)).wait_recv()
    for i in range(1, nz):
        slot = tt.at[zdn(i)]
        remote(slot, slot, t2_s.at[i - 1], t2_r.at[i - 1], at(zdn(i), x, c, y)).wait_recv()
    for j in range(2):
        pr_wait(z, j)
    make_drow(z)

    def own(xq, carry):
        @pl.when(xq >= x)
        def _():
            tile(z, xq, True)
        return carry
    lax.fori_loop(0, nx, own, 0)

    for s in range(1, half):
        relay(s + 1)
        for j in range(2):
            pr_wait(zdn(s), j)
            pr_wait(zup(s), j)
        for zb, needed in ((zdn(s), z >= s), (zup(s), z + s >= nz)):
            @pl.when(needed)
            def _():
                both(zb)
    if half == 1:
        pass
    for j in range(2):
        pr_wait(zdn(half), j)

    @pl.when(z >= half)
    def _():
        make_drow(zdn(half))

    def o_copies(i):
        dev = at(z, lax.rem(x + i, nx), c, y)
        return (
            remote(ob.at[i], orv.at[i], o_s.at[i, 0], o_r.at[i, 0], dev),
            remote(sb.at[i], srv.at[i], o_s.at[i, 1], o_r.at[i, 1], dev),
        )

    def last(k, carry):
        i = lax.rem(k + 1, nx)
        xq = lax.rem(x + i, nx)

        @pl.when(z >= half)
        def _():
            tile(zdn(half), xq, False)

        outs, lses = [], []
        for h in range(3):
            total = acc[xq, h, :, 128:]
            some = total > 0.0
            safe = jnp.where(some, total, 1.0)
            outs.append(acc[xq, h, :, :128] / safe)
            lses.append(jnp.where(some, mb[xq, h] + jnp.log2(safe), NEG))
        wide, narrow = outs[0], jnp.where(low, outs[1], outs[2])
        ob[i] = jnp.concatenate([wide, narrow], axis=1).astype(BF16)
        packed = jnp.where(lane == 0, lses[0], jnp.where(lane == 1, lses[1], lses[2]))
        sb[i] = jnp.transpose(packed)[:8]

        @pl.when(i > 0)
        def _():
            for copy in o_copies(i):
                copy.start()
        return carry
    lax.fori_loop(0, nx, last, 0)

    for i in range(1, nx):
        src = lax.rem(x - i + nx, nx)
        for copy in o_copies(i):
            copy.wait_recv()
    stats = [sb[0]] + [srv[i] for i in range(1, nx)]
    outs = [ob[0]] + [orv[i] for i in range(1, nx)]
    top = functools.reduce(jnp.maximum, stats)
    shares = [jnp.exp2(t - top) for t in stats]
    whole = functools.reduce(jnp.add, shares)
    shares = [t / whole for t in shares]
    columns = jnp.transpose(jnp.concatenate(shares + [jnp.zeros((128 - 8 * nx, 256), F32)], axis=0))
    wide = jnp.zeros((256, 128), F32)
    narrow = jnp.zeros((256, 128), F32)
    for i in range(nx):
        o = outs[i].astype(F32)
        wide = wide + columns[:, 8 * i:8 * i + 1] * o[:, :128]
        narrow = narrow + jnp.where(low, columns[:, 8 * i + 1:8 * i + 2], columns[:, 8 * i + 2:8 * i + 3]) * o[:, 128:]
    ab[...] = jnp.concatenate([wide, narrow], axis=1).astype(BF16)

    share = 256 // ny

    def rows_of(y_):
        return ab.at[pl.ds(pl.multiple_of(y_ * share, share), share), :]

    def y_copy(i):
        other = lax.rem(y + i, ny)
        return remote(rows_of(other), ar.at[y], y_s.at[i - 1], y_r.at[i - 1], at(z, x, c, other))

    for i in range(1, ny):
        y_copy(i).start()
    att_ref[y] = ab[pl.ds(pl.multiple_of(y * share, share), share), :]
    for i in range(1, ny):
        src = lax.rem(y - i + ny, ny)
        remote(rows_of(src), ar.at[src], y_s.at[i - 1], y_r.at[i - 1], at(z, x, c, src)).wait_recv()
        att_ref[src] = ar[src]

    for j in range(2):
        if up_has(1, j):
            own_up(j).wait_send()
        if dn_has(1, j):
            own_dn(j).wait_send()
        own_pr(j).wait_send()
        for s in range(1, half + 1):
            if up_has(s, j):
                if up_has(s + 1, j):
                    up_copy(s, j).wait_send()
                pr_copy(zdn(s), j).wait_send()
            if dn_has(s, j):
                if dn_has(s + 1, j):
                    dn_copy(s, j).wait_send()
                pr_copy(zup(s), j).wait_send()
    for i in range(1, 2 * nx):
        t1_copy(i).wait_send()
    for i in range(1, nz):
        t2_copy(i).wait_send()
    for i in range(1, nx):
        q_copy(i).wait_send()
        for copy in o_copies(i):
            copy.wait_send()
    for i in range(1, ny):
        y_copy(i).wait_send()


def attend(dims, q, kd, v, tot):
    nz, nx, ny = dims
    half = nz // 2
    dma = pltpu.SemaphoreType.DMA
    vmem = pl.BlockSpec(memory_space=pltpu.VMEM)
    return pl.pallas_call(
        functools.partial(attention_kernel, dims),
        out_shape=jax.ShapeDtypeStruct((ny, 256 // ny, 256), BF16),
        in_specs=[vmem] * 4,
        out_specs=vmem,
        scratch_shapes=[
            pltpu.VMEM((nx, 256, 256), BF16),
            pltpu.VMEM((nz, 2, 272, 256), BF16),
            pltpu.VMEM((nz, 2, 256, 256), BF16),
            pltpu.VMEM((nz, 2 * nx, 1, 128), F32),
            pltpu.VMEM((3, 1, 512), F32),
            pltpu.VMEM((nx, 3, 256, 128), F32),
            pltpu.VMEM((nx, 3, 256, 256), F32),
            pltpu.VMEM((nx, 256, 256), BF16),
            pltpu.VMEM((nx, 8, 256), F32),
            pltpu.VMEM((nx, 256, 256), BF16),
            pltpu.VMEM((nx, 8, 256), F32),
            pltpu.VMEM((256, 256), BF16),
            pltpu.VMEM((ny, 256 // ny, 256), BF16),
            dma((nx,)), dma((nx,)),
            dma((half + 1, 2)), dma((half + 1, 2)), dma((half + 1, 2)), dma((half + 1, 2)),
            dma((nz, 2)), dma((nz, 2)),
            dma((2 * nx,)), dma((2 * nx,)), dma((nz,)), dma((nz,)),
            dma((nx, 2)), dma((nx, 2)), dma((ny,)), dma((ny,)), dma((4,)),
        ],
        compiler_params=pltpu.CompilerParams(collective_id=1, has_side_effects=True, vmem_limit_bytes=40 * 2**20),
        cost_estimate=pl.CostEstimate(flops=10**10, bytes_accessed=10**7, transcendentals=12 * 10**6),
        name="attend",
    )(q, kd, v, tot)


def prepare(query_wide, key_wide, value_wide, query_narrow, key_narrow, value_narrow, gate_wide, gate_narrow):
    gates = jnp.concatenate([gate_wide, gate_narrow], axis=1)
    run = jnp.cumsum(jax.nn.log_sigmoid(gates).T, axis=1) * LOG2E
    tot = jnp.pad(run[:, -1], (0, 125))[None, :]
    high = lax.reduce_precision(run, 8, 7)
    mid = lax.reduce_precision(run - high, 8, 7)
    parts = jnp.stack([high, mid, run - high - mid], axis=1).reshape(9, 256)
    parts = jnp.pad(parts, ((0, 7), (0, 0))).astype(BF16)
    q = jnp.concatenate([query_wide, query_narrow], axis=1)
    kd = jnp.concatenate([jnp.concatenate([key_wide, key_narrow], axis=1), parts], axis=0)
    v = jnp.concatenate([value_wide, value_narrow], axis=1)
    return q, kd, v, tot


def body(
    residual,
    query_wide,
    key_wide,
    value_wide,
    query_narrow,
    key_narrow,
    value_narrow,
    gate_wide,
    gate_narrow,
    out_wide,
    out_narrow,
    norm_gain,
    routing,
    route_weight,
    gate_weight,
    up_weight,
    down_weight,
):
    ny = lax.axis_size("tp")
    nx = 4
    dims = (lax.axis_size("sp") // (2 * nx), nx, ny)
    own_rows = residual.shape[0]
    full_gate = lax.all_gather(gate_weight[0], "tp", axis=0)
    full_up = lax.all_gather(up_weight[0], "tp", axis=0)
    full_down = lax.all_gather(down_weight[0], "tp", axis=0, tiled=True)
    att = attend(
        dims,
        *prepare(
            query_wide, key_wide, value_wide, query_narrow, key_narrow, value_narrow, gate_wide, gate_narrow
        ),
    )
    heads_wide = jnp.transpose(att[:, :, :128], (1, 0, 2)).reshape(own_rows, 128 * ny)
    heads_narrow = jnp.transpose(att[:, :, 128:], (1, 0, 2)).reshape(own_rows, 128 * ny)
    mixed = jnp.dot(heads_wide, out_wide, preferred_element_type=jnp.float32)
    mixed = mixed + jnp.dot(heads_narrow, out_narrow, preferred_element_type=jnp.float32)
    middle = (residual.astype(jnp.float32) + mixed).astype(jnp.bfloat16)
    middle_wide = middle.astype(jnp.float32)
    spread = jnp.mean(middle_wide * middle_wide, axis=1, keepdims=True)
    normed = (middle_wide * lax.rsqrt(spread + epsilon) * norm_gain).astype(jnp.bfloat16)
    features = normed.shape[1]
    chosen_count = routing.shape[1]
    expert_count = gate_weight.shape[0] * lax.axis_size("sp")
    capacity = own_rows * GROUPS // expert_count
    flat_routes = routing.reshape(-1)
    matches = (flat_routes[:, None] == jnp.arange(expert_count, dtype=jnp.int32)[None, :]).astype(
        jnp.int32
    )
    ranking = jnp.sum((jnp.cumsum(matches, axis=0) - matches) * matches, axis=1)
    placing = flat_routes * capacity + ranking
    picker = (
        placing[None, :] == jnp.arange(expert_count * capacity, dtype=jnp.int32)[:, None]
    ).astype(jnp.bfloat16)
    picker = jnp.sum(picker.reshape(expert_count * capacity, own_rows, chosen_count), axis=2)
    outgoing = jnp.dot(picker, normed, preferred_element_type=jnp.float32).astype(jnp.bfloat16)
    outgoing = outgoing.reshape(expert_count, capacity, features)
    arrived = lax.all_to_all(outgoing, "sp", split_axis=0, concat_axis=0, tiled=True)
    rows = arrived.reshape(-1, features)
    hidden = []
    for k in range(ny):
        gate_value = jnp.dot(rows, full_gate[k], preferred_element_type=jnp.float32)
        up_value = jnp.dot(rows, full_up[k], preferred_element_type=jnp.float32)
        hidden.append((jax.nn.silu(gate_value) * up_value).astype(jnp.bfloat16))
    hidden = jnp.concatenate(hidden, axis=1)
    answers = jnp.dot(hidden, full_down, preferred_element_type=jnp.float32).astype(jnp.bfloat16)
    returned = lax.all_to_all(
        answers.reshape(expert_count, capacity, features),
        "sp",
        split_axis=0,
        concat_axis=0,
        tiled=True,
    )
    picked = jnp.take(returned.reshape(expert_count * capacity, features), placing, axis=0)
    picked = picked.reshape(own_rows, chosen_count, features).astype(jnp.float32)
    combined = jnp.sum(route_weight[:, :, None] * picked, axis=1)
    return (middle_wide + combined).astype(jnp.bfloat16)


def solution(mesh):
    placed = (
        P(("sp", "tp"), None),
        P("sp", "tp"),
        P("sp", "tp"),
        P("sp", "tp"),
        P("sp", "tp"),
        P("sp", "tp"),
        P("sp", "tp"),
        P("sp", "tp"),
        P("sp", "tp"),
        P(),
        P(),
        P(),
        P(("sp", "tp"), None),
        P(("sp", "tp"), None),
        P("sp", None, "tp"),
        P("sp", None, "tp"),
        P("sp", "tp", None),
    )
    return jax.shard_map(
        body, mesh=mesh, in_specs=placed, out_specs=P(("sp", "tp"), None), check_vma=False
    )
```

```python
import functools
import math

import jax
import jax.numpy as jnp
from jax import lax
from jax.experimental import pallas as pl
from jax.experimental.pallas import tpu as pltpu
from jax.sharding import PartitionSpec as P

MESH = pl.DeviceIdType.MESH
F32, BF16 = jnp.float32, jnp.bfloat16
HW = 128
HN = 64
NX = 4
LOG2E = math.log2(math.e)
NEG = -1e30
epsilon = 1e-06


def attention_kernel(
    dims, q_ref, kd_ref, v_ref, tot_ref, gate_ref, up_ref, att_ref, peer_gate, peer_up,
    qb, kb, vb, tt, drow, mb, acc, ob, sb, orv, srv, ab, ar,
    q_s, q_r, up_s, up_r, dn_s, dn_r, pr_s, pr_r, t1_s, t1_r, t2_s, t2_r, o_s, o_r, y_s, y_r, loc, w_s, w_r,
):
    nz, nx, ny = dims
    half = nz // 2
    sp, y = lax.axis_index("sp"), lax.axis_index("tp")
    c = lax.rem(sp, 2)
    x = lax.rem(sp // 2, nx)
    z = sp // (2 * nx)
    xc = x * 2 + c

    def at(z_, x_, c_, y_):
        return ((z_ * nx + x_) * 2 + c_, y_)

    def zup(i):
        return lax.rem(z + i, nz)

    def zdn(i):
        return lax.rem(z - i + nz, nz)

    def in_plane(i):
        other = lax.rem(xc + i, 2 * nx)
        return at(z, other // 2, lax.rem(other, 2), y)

    def remote(src, dst, send, recv, device):
        return pltpu.make_async_remote_copy(
            src_ref=src, dst_ref=dst, send_sem=send, recv_sem=recv, device_id=device, device_id_type=MESH
        )

    barrier = pltpu.get_barrier_semaphore()

    def greet(device):
        pl.semaphore_signal(barrier, inc=1, device_id=device, device_id_type=MESH)

    for i in range(1, nz):
        greet(at(zup(i), x, c, y))
    for i in range(1, 2 * nx):
        greet(in_plane(i))
    for i in range(1, ny):
        greet(at(z, x, c, lax.rem(y + i, ny)))
    pl.semaphore_wait(barrier, nz - 1 + 2 * nx - 1 + ny - 1)

    up_dev, dn_dev, pr_dev = at(zup(1), x, c, y), at(zdn(1), x, c, y), at(z, x, 1 - c, y)

    def up_copy(s, j):
        zb = zdn(s)
        src = (kb, vb)[j].at[zb, c]
        return remote(src, src, up_s.at[s, j], up_r.at[s, j], up_dev)

    def dn_copy(s, j):
        zb = zup(s)
        src = (kb, vb)[j].at[zb, c]
        return remote(src, src, dn_s.at[s, j], dn_r.at[s, j], dn_dev)

    def pr_copy(zb, j):
        src = (kb, vb)[j].at[zb, c]
        return remote(src, src, pr_s.at[zb, j], pr_r.at[zb, j], pr_dev)

    def pr_wait(zb, j):
        dst = (kb, vb)[j].at[zb, 1 - c]
        remote(dst, dst, pr_s.at[zb, j], pr_r.at[zb, j], pr_dev).wait_recv()

    def own_up(j):
        return remote((kd_ref, v_ref)[j], (kb, vb)[j].at[z, c], up_s.at[0, j], up_r.at[0, j], up_dev)

    def own_dn(j):
        return remote((kd_ref, v_ref)[j], (kb, vb)[j].at[z, c], dn_s.at[0, j], dn_r.at[0, j], dn_dev)

    def own_pr(j):
        return remote((kd_ref, v_ref)[j], (kb, vb)[j].at[z, c], pr_s.at[z, j], pr_r.at[z, j], pr_dev)

    def up_has(s, j):
        return s < half or (s == half and j == 0)

    def dn_has(s, j):
        return s < half or (s == half and j == 1)

    for j in range(2):
        if up_has(1, j):
            own_up(j).start()
        if dn_has(1, j):
            own_dn(j).start()

    def t1_copy(i):
        return remote(tot_ref, tt.at[z, xc], t1_s.at[i - 1], t1_r.at[i - 1], in_plane(i))

    def t2_copy(i):
        return remote(tt.at[z], tt.at[z], t2_s.at[i - 1], t2_r.at[i - 1], at(zup(i), x, c, y))

    def q_copy(i):
        return remote(q_ref, qb.at[x], q_s.at[i - 1], q_r.at[i - 1], at(z, lax.rem(x + i, nx), c, y))

    for i in range(1, 2 * nx):
        t1_copy(i).start()
    for i in range(1, nx):
        q_copy(i).start()
    for j in range(2):
        own_pr(j).start()
    pair = at(z, x, c, lax.rem(y, 2) * (y - 1) + (1 - lax.rem(y, 2)) * (y + 1))
    first_rows = pl.ds(0, peer_up.shape[0])
    weights = [
        remote(gate_ref, peer_gate, w_s.at[0], w_r.at[0], pair),
        remote(up_ref.at[first_rows, :], peer_up, w_s.at[1], w_r.at[1], pair),
    ]
    for copy in weights:
        copy.start()
    local = [
        pltpu.make_async_copy(tot_ref, tt.at[z, xc], loc.at[0]),
        pltpu.make_async_copy(q_ref, qb.at[x], loc.at[1]),
        pltpu.make_async_copy(kd_ref, kb.at[z, c], loc.at[2]),
        pltpu.make_async_copy(v_ref, vb.at[z, c], loc.at[3]),
    ]
    for copy in local:
        copy.start()
    mb[...] = jnp.full(mb.shape, NEG, F32)
    acc[...] = jnp.zeros(acc.shape, F32)
    local[0].wait()
    for i in range(1, 2 * nx):
        other = lax.rem(xc - i + 2 * nx, 2 * nx)
        remote(tot_ref, tt.at[z, other], t1_s.at[i - 1], t1_r.at[i - 1], in_plane(i)).wait_recv()
    for i in range(1, nz):
        t2_copy(i).start()
    for copy in local[1:]:
        copy.wait()

    def relay(s):
        for j in range(2):
            if up_has(s, j):
                slot = (kb, vb)[j].at[zdn(s), c]
                remote(slot, slot, up_s.at[s - 1, j], up_r.at[s - 1, j], up_dev).wait_recv()
                if up_has(s + 1, j):
                    up_copy(s, j).start()
                pr_copy(zdn(s), j).start()
            if dn_has(s, j):
                slot = (kb, vb)[j].at[zup(s), c]
                remote(slot, slot, dn_s.at[s - 1, j], dn_r.at[s - 1, j], dn_dev).wait_recv()
                if dn_has(s + 1, j):
                    dn_copy(s, j).start()
                pr_copy(zup(s), j).start()

    lane = lax.broadcasted_iota(jnp.int32, (1, 128), 1)
    low = lane < HN

    def head_offsets(zb):
        def plane(p, run):
            whole = jnp.zeros((1, 128), F32)
            for k in range(2 * nx):
                whole = whole + tt[p, k]
            return run + jnp.where(p < zb, whole, 0.0)
        run = lax.fori_loop(0, nz, plane, jnp.zeros((1, 128), F32))
        for k in range(2 * nx):
            run = run + jnp.where(k < 2 * x, tt[zb, k], 0.0)
        return run, run + tt[zb, 2 * x]

    def make_drow(zb):
        offs = head_offsets(zb)
        parts = [kb[zb, k, pl.ds(256, 16), :].astype(F32) for k in range(2)]
        for h in range(3):
            pieces = []
            for k in range(2):
                off = jnp.sum(jnp.where(lane == h, offs[k], 0.0), axis=1, keepdims=True)
                p = parts[k]
                pieces.append(p[3 * h:3 * h + 1] + p[3 * h + 1:3 * h + 2] + p[3 * h + 2:3 * h + 3] + off)
            drow[h] = jnp.concatenate(pieces, axis=1)

    scales = (HW ** -0.5 * LOG2E, HN ** -0.5 * LOG2E, HN ** -0.5 * LOG2E)

    def tile(zb, xq, masked):
        q = qb[xq]
        qw, qn = q[:, :128], q[:, 128:]
        zero = jnp.zeros_like(qn)
        heads = (qw, jnp.where(low, qn, zero), jnp.where(low, zero, qn))
        keys = jnp.concatenate([kb[zb, 0, :256, :], kb[zb, 1, :256, :]], axis=0)
        vals = jnp.concatenate([vb[zb, 0], vb[zb, 1]], axis=0)
        ones = jnp.ones((512, 128), BF16)
        if masked:
            rows = lax.broadcasted_iota(jnp.int32, (256, 512), 0) + (xq * 512 + c * 256)
            cols = lax.broadcasted_iota(jnp.int32, (256, 512), 1) + x * 512
            seen = cols <= rows
        for h in range(3):
            side = slice(0, 128) if h == 0 else slice(128, 256)
            s = lax.dot_general(heads[h], keys[:, side], (((1,), (1,)), ((), ())), preferred_element_type=F32)
            r = s * scales[h] - drow[h]
            if masked:
                r = jnp.where(seen, r, NEG)
            old = mb[xq, h]
            new = jnp.maximum(old, jnp.max(r, axis=1, keepdims=True))
            p = jnp.exp2(r - jnp.concatenate([new] * 4, axis=1)).astype(BF16)
            shrink = jnp.exp2(old - new)
            mb[xq, h] = new
            right = jnp.concatenate([vals[:, side], ones], axis=1)
            pv = jnp.dot(p, right, preferred_element_type=F32)
            acc[xq, h] = acc[xq, h] * jnp.concatenate([shrink, shrink], axis=1) + pv

    def both(zb):
        make_drow(zb)

        def one(xq, carry):
            tile(zb, xq, False)
            return carry
        lax.fori_loop(0, nx, one, 0)

    relay(1)
    for i in range(1, nx):
        src = lax.rem(x - i + nx, nx)
        remote(q_ref, qb.at[src], q_s.at[i - 1], q_r.at[i - 1], at(z, src, c, y)).wait_recv()
    for i in range(1, nz):
        slot = tt.at[zdn(i)]
        remote(slot, slot, t2_s.at[i - 1], t2_r.at[i - 1], at(zdn(i), x, c, y)).wait_recv()
    for j in range(2):
        pr_wait(z, j)
    make_drow(z)

    def own(xq, carry):
        @pl.when(xq >= x)
        def _():
            tile(z, xq, True)
        return carry
    lax.fori_loop(0, nx, own, 0)

    for s in range(1, half):
        relay(s + 1)
        for j in range(2):
            pr_wait(zdn(s), j)
            pr_wait(zup(s), j)
        for zb, needed in ((zdn(s), z >= s), (zup(s), z + s >= nz)):
            @pl.when(needed)
            def _():
                both(zb)
    if half == 1:
        pass
    for j in range(2):
        pr_wait(zdn(half), j)

    @pl.when(z >= half)
    def _():
        make_drow(zdn(half))

    def o_copies(i):
        dev = at(z, lax.rem(x + i, nx), c, y)
        return (
            remote(ob.at[i], orv.at[i], o_s.at[i, 0], o_r.at[i, 0], dev),
            remote(sb.at[i], srv.at[i], o_s.at[i, 1], o_r.at[i, 1], dev),
        )

    def last(k, carry):
        i = lax.rem(k + 1, nx)
        xq = lax.rem(x + i, nx)

        @pl.when(z >= half)
        def _():
            tile(zdn(half), xq, False)

        outs, lses = [], []
        for h in range(3):
            total = acc[xq, h, :, 128:]
            some = total > 0.0
            safe = jnp.where(some, total, 1.0)
            outs.append(acc[xq, h, :, :128] / safe)
            lses.append(jnp.where(some, mb[xq, h] + jnp.log2(safe), NEG))
        wide, narrow = outs[0], jnp.where(low, outs[1], outs[2])
        ob[i] = jnp.concatenate([wide, narrow], axis=1).astype(BF16)
        packed = jnp.where(lane == 0, lses[0], jnp.where(lane == 1, lses[1], lses[2]))
        sb[i] = jnp.transpose(packed)[:8]

        @pl.when(i > 0)
        def _():
            for copy in o_copies(i):
                copy.start()
        return carry
    lax.fori_loop(0, nx, last, 0)

    for i in range(1, nx):
        src = lax.rem(x - i + nx, nx)
        for copy in o_copies(i):
            copy.wait_recv()
    stats = [sb[0]] + [srv[i] for i in range(1, nx)]
    outs = [ob[0]] + [orv[i] for i in range(1, nx)]
    top = functools.reduce(jnp.maximum, stats)
    shares = [jnp.exp2(t - top) for t in stats]
    whole = functools.reduce(jnp.add, shares)
    shares = [t / whole for t in shares]
    columns = jnp.transpose(jnp.concatenate(shares + [jnp.zeros((128 - 8 * nx, 256), F32)], axis=0))
    wide = jnp.zeros((256, 128), F32)
    narrow = jnp.zeros((256, 128), F32)
    for i in range(nx):
        o = outs[i].astype(F32)
        wide = wide + columns[:, 8 * i:8 * i + 1] * o[:, :128]
        narrow = narrow + jnp.where(low, columns[:, 8 * i + 1:8 * i + 2], columns[:, 8 * i + 2:8 * i + 3]) * o[:, 128:]
    ab[...] = jnp.concatenate([wide, narrow], axis=1).astype(BF16)

    share = 256 // ny

    def rows_of(y_):
        return ab.at[pl.ds(pl.multiple_of(y_ * share, share), share), :]

    def y_copy(i):
        other = lax.rem(y + i, ny)
        return remote(rows_of(other), ar.at[y], y_s.at[i - 1], y_r.at[i - 1], at(z, x, c, other))

    for i in range(1, ny):
        y_copy(i).start()
    att_ref[y] = ab[pl.ds(pl.multiple_of(y * share, share), share), :]
    for i in range(1, ny):
        src = lax.rem(y - i + ny, ny)
        remote(rows_of(src), ar.at[src], y_s.at[i - 1], y_r.at[i - 1], at(z, x, c, src)).wait_recv()
        att_ref[src] = ar[src]

    for copy in weights:
        copy.wait()
    for j in range(2):
        if up_has(1, j):
            own_up(j).wait_send()
        if dn_has(1, j):
            own_dn(j).wait_send()
        own_pr(j).wait_send()
        for s in range(1, half + 1):
            if up_has(s, j):
                if up_has(s + 1, j):
                    up_copy(s, j).wait_send()
                pr_copy(zdn(s), j).wait_send()
            if dn_has(s, j):
                if dn_has(s + 1, j):
                    dn_copy(s, j).wait_send()
                pr_copy(zup(s), j).wait_send()
    for i in range(1, 2 * nx):
        t1_copy(i).wait_send()
    for i in range(1, nz):
        t2_copy(i).wait_send()
    for i in range(1, nx):
        q_copy(i).wait_send()
        for copy in o_copies(i):
            copy.wait_send()
    for i in range(1, ny):
        y_copy(i).wait_send()


def attend(dims, q, kd, v, tot, gate, up):
    nz, nx, ny = dims
    half = nz // 2
    dma = pltpu.SemaphoreType.DMA
    vmem = pl.BlockSpec(memory_space=pltpu.VMEM)
    hbm = pl.BlockSpec(memory_space=pl.ANY)
    return pl.pallas_call(
        functools.partial(attention_kernel, dims),
        out_shape=[
            jax.ShapeDtypeStruct((ny, 256 // ny, 256), BF16),
            jax.ShapeDtypeStruct(gate.shape, BF16),
            jax.ShapeDtypeStruct((up.shape[0] // 2, up.shape[1]), BF16),
        ],
        in_specs=[vmem] * 4 + [hbm] * 2,
        out_specs=[vmem, hbm, hbm],
        scratch_shapes=[
            pltpu.VMEM((nx, 256, 256), BF16),
            pltpu.VMEM((nz, 2, 272, 256), BF16),
            pltpu.VMEM((nz, 2, 256, 256), BF16),
            pltpu.VMEM((nz, 2 * nx, 1, 128), F32),
            pltpu.VMEM((3, 1, 512), F32),
            pltpu.VMEM((nx, 3, 256, 128), F32),
            pltpu.VMEM((nx, 3, 256, 256), F32),
            pltpu.VMEM((nx, 256, 256), BF16),
            pltpu.VMEM((nx, 8, 256), F32),
            pltpu.VMEM((nx, 256, 256), BF16),
            pltpu.VMEM((nx, 8, 256), F32),
            pltpu.VMEM((256, 256), BF16),
            pltpu.VMEM((ny, 256 // ny, 256), BF16),
            dma((nx,)), dma((nx,)),
            dma((half + 1, 2)), dma((half + 1, 2)), dma((half + 1, 2)), dma((half + 1, 2)),
            dma((nz, 2)), dma((nz, 2)),
            dma((2 * nx,)), dma((2 * nx,)), dma((nz,)), dma((nz,)),
            dma((nx, 2)), dma((nx, 2)), dma((ny,)), dma((ny,)), dma((4,)), dma((2,)), dma((2,)),
        ],
        compiler_params=pltpu.CompilerParams(collective_id=1, has_side_effects=True, vmem_limit_bytes=40 * 2**20),
        cost_estimate=pl.CostEstimate(flops=10**10, bytes_accessed=10**7, transcendentals=12 * 10**6),
        name="attend",
    )(q, kd, v, tot, gate, up)


def prepare(query_wide, key_wide, value_wide, query_narrow, key_narrow, value_narrow, gate_wide, gate_narrow):
    gates = jnp.concatenate([gate_wide, gate_narrow], axis=1)
    run = jnp.cumsum(jax.nn.log_sigmoid(gates).T, axis=1) * LOG2E
    tot = jnp.pad(run[:, -1], (0, 125))[None, :]
    high = lax.reduce_precision(run, 8, 7)
    mid = lax.reduce_precision(run - high, 8, 7)
    parts = jnp.stack([high, mid, run - high - mid], axis=1).reshape(9, 256)
    parts = jnp.pad(parts, ((0, 7), (0, 0))).astype(BF16)
    q = jnp.concatenate([query_wide, query_narrow], axis=1)
    kd = jnp.concatenate([jnp.concatenate([key_wide, key_narrow], axis=1), parts], axis=0)
    v = jnp.concatenate([value_wide, value_narrow], axis=1)
    return q, kd, v, tot


def paired(y):
    return lax.rem(y, 2) * (y - 1) + (1 - lax.rem(y, 2)) * (y + 1)


def plane_at(t, z, nz):
    d = jnp.where(lax.rem(t, 2) == 1, (t + 1) // 2, nz - t // 2)
    return lax.rem(z + d, nz)


def to_rows(take, tmp, plane):
    for k in range(plane // 2):
        tmp[8 * k:8 * k + 8, :] = jnp.concatenate([take(2 * k).astype(F32), take(2 * k + 1).astype(F32)], axis=0)


def dispatch_kernel(
    dims, att_ref, res_ref, wide_ref, narrow_ref, gain_ref, picker_ref, up_ref, down_ref,
    own_ref, cross_ref, mid_ref, peer_up, peer_down,
    ow, on, perm, tmp, snd, arr, arc, a_s, a_r, c_s, c_r, w_s, w_r, loc,
):
    nz, nx, ny = dims
    plane = 2 * nx
    count = nz * plane
    sp, y = lax.axis_index("sp"), lax.axis_index("tp")
    z = sp // plane
    fetch = [pltpu.make_async_copy(wide_ref, ow, loc.at[0]), pltpu.make_async_copy(narrow_ref, on, loc.at[1])]
    for copy in fetch:
        copy.start()

    def remote(src, dst, send, recv, device):
        return pltpu.make_async_remote_copy(
            src_ref=src, dst_ref=dst, send_sem=send, recv_sem=recv, device_id=device, device_id_type=MESH
        )

    barrier = pltpu.get_barrier_semaphore()
    pair, across = (sp, paired(y)), (sp, ny - 1 - y)

    def greet(i, carry):
        pl.semaphore_signal(barrier, inc=1, device_id=(lax.rem(sp + i, count), y), device_id_type=MESH)
        return carry
    lax.fori_loop(1, count, greet, 0)
    pl.semaphore_signal(barrier, inc=1, device_id=pair, device_id_type=MESH)
    pl.semaphore_signal(barrier, inc=1, device_id=across, device_id_type=MESH)

    done = up_ref.shape[0] - peer_up.shape[0]
    for copy in fetch:
        copy.wait()
    a_wide = jnp.concatenate([att_ref[k, :, :128] for k in range(ny)], axis=1)
    a_narrow = jnp.concatenate([att_ref[k, :, 128:] for k in range(ny)], axis=1)
    mixed = jnp.dot(a_wide, ow[...], preferred_element_type=F32) + jnp.dot(a_narrow, on[...], preferred_element_type=F32)
    middle = (res_ref[...].astype(F32) + mixed).astype(BF16)
    mid_ref[...] = middle
    middle = middle.astype(F32)
    spread = jnp.mean(middle * middle, axis=1, keepdims=True)
    normed = (middle * lax.rsqrt(spread + epsilon) * gain_ref[...]).astype(BF16)
    perm[...] = jnp.dot(picker_ref[...], normed, preferred_element_type=F32)

    def cut(k, carry):
        v = perm[pl.ds(pl.multiple_of(8 * k, 8), 8), :]
        snd[2 * k] = v[:4].astype(BF16)
        snd[2 * k + 1] = v[4:].astype(BF16)
        return carry
    lax.fori_loop(0, count // 2, cut, 0)

    pl.semaphore_wait(barrier, count - 1 + 2)
    weights = [
        remote(up_ref.at[pl.ds(done, peer_up.shape[0]), :], peer_up, w_s.at[0], w_r.at[0], pair),
        remote(down_ref, peer_down, w_s.at[1], w_r.at[1], pair),
    ]
    for copy in weights:
        copy.start()

    def out_copy(e):
        return remote(snd.at[e], arr.at[sp], a_s.at[e], a_r.at[sp], (e, y))

    keep = pltpu.make_async_copy(snd.at[sp], arr.at[sp], loc.at[2])
    keep.start()

    def send(t, carry):
        first = plane_at(t, z, nz) * plane

        def one(k, inner):
            e = first + k

            @pl.when(e != sp)
            def _():
                out_copy(e).start()
            return inner
        return lax.fori_loop(0, plane, one, carry)
    lax.fori_loop(0, nz, send, 0)
    keep.wait()

    def cross_copy(p):
        part = pl.ds(p * plane, plane)
        return remote(arr.at[part], arc.at[part], c_s.at[p], c_r.at[p], across)

    def arrive(t, carry):
        p = plane_at(t, z, nz)
        first = p * plane

        def one(k, inner):
            s = first + k

            @pl.when(s != sp)
            def _():
                remote(snd.at[s], arr.at[s], a_s.at[s], a_r.at[s], (s, y)).wait_recv()
            return inner
        lax.fori_loop(0, plane, one, 0)
        cross_copy(p).start()
        to_rows(lambda k: arr[first + k], tmp, plane)
        own_ref[pl.ds(pl.multiple_of(first * 4, 4 * plane), 4 * plane), :] = tmp[...].astype(BF16)
        return carry
    lax.fori_loop(0, nz, arrive, 0)

    def arrive_cross(t, carry):
        p = plane_at(t, z, nz)
        first = p * plane
        cross_copy(p).wait_recv()
        to_rows(lambda k: arc[first + k], tmp, plane)
        cross_ref[pl.ds(pl.multiple_of(first * 4, 4 * plane), 4 * plane), :] = tmp[...].astype(BF16)
        return carry
    lax.fori_loop(0, nz, arrive_cross, 0)

    def drain(e, carry):
        @pl.when(e != sp)
        def _():
            out_copy(e).wait_send()
        return carry
    lax.fori_loop(0, count, drain, 0)

    def drain_cross(p, carry):
        cross_copy(p).wait_send()
        return carry
    lax.fori_loop(0, nz, drain_cross, 0)
    for copy in weights:
        copy.wait()


def dispatch(dims, att, residual, wide, narrow, gain, picker, up, down):
    nz, nx, ny = dims
    count, features = nz * nx * 2, residual.shape[1]
    dma = pltpu.SemaphoreType.DMA
    vmem = pl.BlockSpec(memory_space=pltpu.VMEM)
    hbm = pl.BlockSpec(memory_space=pl.ANY)
    shape = jax.ShapeDtypeStruct
    return pl.pallas_call(
        functools.partial(dispatch_kernel, dims),
        out_shape=[
            shape((4 * count, features), BF16),
            shape((4 * count, features), BF16),
            shape(residual.shape, BF16),
            shape((up.shape[0] // 2, up.shape[1]), BF16),
            shape(down.shape, BF16),
        ],
        in_specs=[vmem, vmem, hbm, hbm, vmem, vmem, hbm, hbm],
        out_specs=[vmem, vmem, vmem, hbm, hbm],
        scratch_shapes=[
            pltpu.VMEM(wide.shape, BF16),
            pltpu.VMEM(narrow.shape, BF16),
            pltpu.VMEM((4 * count, features), F32),
            pltpu.VMEM((8 * nx, features), F32),
            pltpu.VMEM((count, 4, features), BF16),
            pltpu.VMEM((count, 4, features), BF16),
            pltpu.VMEM((count, 4, features), BF16),
            dma((count,)), dma((count,)), dma((nz,)), dma((nz,)), dma((2,)), dma((2,)), dma((3,)),
        ],
        compiler_params=pltpu.CompilerParams(collective_id=2, has_side_effects=True, vmem_limit_bytes=40 * 2**20),
        cost_estimate=pl.CostEstimate(flops=10**9, bytes_accessed=10**7, transcendentals=1000),
        name="dispatch",
    )(att, residual, wide, narrow, gain, picker, up, down)


def expert_kernel(
    dims, own_ref, cross_ref, gate_ref, up_ref, down_ref, peer_gate, peer_up0, peer_up1, peer_down, mid_ref, share_ref,
    out_ref,
    wg, wu, wd, total, part, back, tmp, snd, ret, rows, p_s, p_r, b_s, b_r, loc,
):
    nz, nx, ny = dims
    plane = 2 * nx
    count = nz * plane
    sp, y = lax.axis_index("sp"), lax.axis_index("tp")
    z = sp // plane
    half = peer_up0.shape[0]
    fetch = [
        pltpu.make_async_copy(gate_ref, wg.at[0], loc.at[0]),
        pltpu.make_async_copy(peer_gate, wg.at[1], loc.at[1]),
        pltpu.make_async_copy(up_ref, wu.at[0], loc.at[2]),
        pltpu.make_async_copy(peer_up0, wu.at[1, pl.ds(0, half), :], loc.at[3]),
        pltpu.make_async_copy(peer_up1, wu.at[1, pl.ds(half, half), :], loc.at[4]),
        pltpu.make_async_copy(down_ref, wd.at[0], loc.at[5]),
        pltpu.make_async_copy(peer_down, wd.at[1], loc.at[6]),
    ]
    for copy in fetch:
        copy.start()

    def remote(src, dst, send, recv, device):
        return pltpu.make_async_remote_copy(
            src_ref=src, dst_ref=dst, send_sem=send, recv_sem=recv, device_id=device, device_id_type=MESH
        )

    barrier = pltpu.get_barrier_semaphore()
    across = (sp, ny - 1 - y)

    def greet(i, carry):
        pl.semaphore_signal(barrier, inc=1, device_id=(lax.rem(sp + i, count), y), device_id_type=MESH)
        return carry
    lax.fori_loop(1, count, greet, 0)
    pl.semaphore_signal(barrier, inc=1, device_id=across, device_id_type=MESH)
    for copy in fetch[:5]:
        copy.wait()

    def hidden(x):
        both = []
        for k in range(2):
            g = jnp.dot(x, wg[k], preferred_element_type=F32)
            u = jnp.dot(x, wu[k], preferred_element_type=F32)
            both.append((jax.nn.silu(g) * u).astype(BF16))
        return both

    def down(h, put):
        step = 512
        for q in range(wd.shape[2] // step):
            cols = slice(q * step, (q + 1) * step)
            put(
                cols,
                jnp.dot(h[0], wd[0, :, cols], preferred_element_type=F32)
                + jnp.dot(h[1], wd[1, :, cols], preferred_element_type=F32),
            )

    h = hidden(cross_ref[...])
    for copy in fetch[5:]:
        copy.wait()

    def put_part(cols, value):
        part[:, cols] = value.astype(BF16)
    down(h, put_part)
    pl.semaphore_wait(barrier, count)

    def rows_of(ref, p):
        return ref.at[pl.ds(pl.multiple_of(p * 4 * plane, 4 * plane), 4 * plane), :]

    def part_copy(p):
        return remote(rows_of(part, p), rows_of(back, p), p_s.at[p], p_r.at[p], across)

    def send_part(t, carry):
        part_copy(plane_at(t, z, nz)).start()
        return carry
    lax.fori_loop(0, nz, send_part, 0)

    h = hidden(own_ref[...])

    def put_total(cols, value):
        total[:, cols] = value
    down(h, put_total)

    def back_copy(e):
        return remote(snd.at[e], ret.at[sp], b_s.at[e], b_r.at[sp], (e, y))

    def finish(t, carry):
        p = plane_at(t, z, nz)
        first = p * plane
        part_copy(p).wait_recv()
        some = pl.ds(pl.multiple_of(first * 4, 4 * plane), 4 * plane)
        tmp[...] = total[some, :] + back[some, :].astype(F32)
        for k in range(plane // 2):
            v = tmp[8 * k:8 * k + 8, :]
            snd[first + 2 * k] = v[:4].astype(BF16)
            snd[first + 2 * k + 1] = v[4:].astype(BF16)

        def one(k, inner):
            e = first + k

            @pl.when(e != sp)
            def _():
                back_copy(e).start()
            return inner
        return lax.fori_loop(0, plane, one, carry)
    lax.fori_loop(0, nz, finish, 0)
    keep = pltpu.make_async_copy(snd.at[sp], ret.at[sp], loc.at[7])
    keep.start()
    keep.wait()

    def arrive(t, carry):
        first = plane_at(t, z, nz) * plane

        def one(k, inner):
            e = first + k

            @pl.when(e != sp)
            def _():
                remote(snd.at[e], ret.at[e], b_s.at[e], b_r.at[e], (e, y)).wait_recv()
            return inner
        lax.fori_loop(0, plane, one, 0)
        to_rows(lambda k: ret[first + k], tmp, plane)
        rows[pl.ds(pl.multiple_of(first * 4, 4 * plane), 4 * plane), :] = tmp[...].astype(BF16)
        return carry
    lax.fori_loop(0, nz, arrive, 0)
    combined = mid_ref[...].astype(F32)
    for k in range(3):
        combined = combined + jnp.dot(share_ref[k], rows[...], preferred_element_type=F32)
    out_ref[...] = combined.astype(BF16)

    def drain(e, carry):
        @pl.when(e != sp)
        def _():
            back_copy(e).wait_send()
        return carry
    lax.fori_loop(0, count, drain, 0)

    def drain_part(p, carry):
        part_copy(p).wait_send()
        return carry
    lax.fori_loop(0, nz, drain_part, 0)


def experts(dims, own, cross, gate, up, down, peer_gate, peer_up0, peer_up1, peer_down, middle, shares):
    nz, nx, ny = dims
    count, features = nz * nx * 2, middle.shape[1]
    dma = pltpu.SemaphoreType.DMA
    vmem = pl.BlockSpec(memory_space=pltpu.VMEM)
    hbm = pl.BlockSpec(memory_space=pl.ANY)
    return pl.pallas_call(
        functools.partial(expert_kernel, dims),
        out_shape=jax.ShapeDtypeStruct(middle.shape, BF16),
        in_specs=[vmem] * 2 + [hbm] * 7 + [vmem] * 2,
        out_specs=vmem,
        scratch_shapes=[
            pltpu.VMEM((2, *gate.shape), BF16),
            pltpu.VMEM((2, *up.shape), BF16),
            pltpu.VMEM((2, *down.shape), BF16),
            pltpu.VMEM((4 * count, features), F32),
            pltpu.VMEM((4 * count, features), BF16),
            pltpu.VMEM((4 * count, features), BF16),
            pltpu.VMEM((8 * nx, features), F32),
            pltpu.VMEM((count, 4, features), BF16),
            pltpu.VMEM((count, 4, features), BF16),
            pltpu.VMEM((4 * count, features), BF16),
            dma((nz,)), dma((nz,)), dma((count,)), dma((count,)), dma((8,)),
        ],
        compiler_params=pltpu.CompilerParams(collective_id=3, has_side_effects=True, vmem_limit_bytes=48 * 2**20),
        cost_estimate=pl.CostEstimate(flops=10**9, bytes_accessed=10**7, transcendentals=1000),
        name="experts",
    )(own, cross, gate, up, down, peer_gate, peer_up0, peer_up1, peer_down, middle, shares)


def tables(routing, route_weight, slots):
    flat = routing.reshape(-1)
    experts_here = jnp.arange(slots // 4, dtype=jnp.int32)
    matches = (flat[:, None] == experts_here[None, :]).astype(jnp.int32)
    ranking = jnp.sum((jnp.cumsum(matches, axis=0) - matches) * matches, axis=1)
    placing = (flat * 4 + ranking).reshape(routing.shape)
    hits = placing[:, :, None] == jnp.arange(slots, dtype=jnp.int32)[None, None, :]
    picker = jnp.sum(hits.astype(F32), axis=1).T.astype(BF16)
    shares = jnp.sum(jnp.where(hits, route_weight[:, :, None], 0.0), axis=1)
    high = lax.reduce_precision(shares, 8, 7)
    mid = lax.reduce_precision(shares - high, 8, 7)
    return picker, jnp.stack([high, mid, shares - high - mid]).astype(BF16)


def body(
    residual,
    query_wide,
    key_wide,
    value_wide,
    query_narrow,
    key_narrow,
    value_narrow,
    gate_wide,
    gate_narrow,
    out_wide,
    out_narrow,
    norm_gain,
    routing,
    route_weight,
    gate_weight,
    up_weight,
    down_weight,
):
    ny = lax.axis_size("tp")
    nx = NX
    dims = (lax.axis_size("sp") // (2 * nx), nx, ny)
    gate, up, down = gate_weight[0], up_weight[0], down_weight[0]
    picker, shares = tables(routing, route_weight, 4 * lax.axis_size("sp"))
    ready = prepare(
        query_wide, key_wide, value_wide, query_narrow, key_narrow, value_narrow, gate_wide, gate_narrow
    )
    att, peer_gate, peer_up0 = attend(dims, *ready, gate, up)
    own, cross, middle, peer_up1, peer_down = dispatch(
        dims, att, residual, out_wide, out_narrow, norm_gain[None, :], picker, up, down
    )
    return experts(dims, own, cross, gate, up, down, peer_gate, peer_up0, peer_up1, peer_down, middle, shares)


def solution(mesh):
    placed = (
        P(("sp", "tp"), None),
        P("sp", "tp"),
        P("sp", "tp"),
        P("sp", "tp"),
        P("sp", "tp"),
        P("sp", "tp"),
        P("sp", "tp"),
        P("sp", "tp"),
        P("sp", "tp"),
        P(),
        P(),
        P(),
        P(("sp", "tp"), None),
        P(("sp", "tp"), None),
        P("sp", None, "tp"),
        P("sp", None, "tp"),
        P("sp", "tp", None),
    )
    return jax.shard_map(
        body, mesh=mesh, in_specs=placed, out_specs=P(("sp", "tp"), None), check_vma=False
    )
```

```python
import functools
import math

import jax
import jax.numpy as jnp
from jax import lax
from jax.experimental import pallas as pl
from jax.experimental.pallas import tpu as pltpu
from jax.sharding import PartitionSpec as P

MESH = pl.DeviceIdType.MESH
F32, BF16 = jnp.float32, jnp.bfloat16
HW = 128
HN = 64
NX = 4
LOG2E = math.log2(math.e)
NEG = -1e30
epsilon = 1e-06


def attention_kernel(
    dims, q_ref, kd_ref, v_ref, tot_ref, gate_ref, up_ref, att_ref, peer_gate, peer_up,
    qb, kb, vb, tt, drow, mb, acc, ob, sb, orv, srv, ab, ar,
    q_s, q_r, up_s, up_r, dn_s, dn_r, pr_s, pr_r, t1_s, t1_r, t2_s, t2_r, o_s, o_r, y_s, y_r, loc, w_s, w_r,
):
    nz, nx, ny = dims
    half = nz // 2
    sp, y = lax.axis_index("sp"), lax.axis_index("tp")
    c = lax.rem(sp, 2)
    x = lax.rem(sp // 2, nx)
    z = sp // (2 * nx)
    xc = x * 2 + c

    def at(z_, x_, c_, y_):
        return ((z_ * nx + x_) * 2 + c_, y_)

    def zup(i):
        return lax.rem(z + i, nz)

    def zdn(i):
        return lax.rem(z - i + nz, nz)

    def in_plane(i):
        other = lax.rem(xc + i, 2 * nx)
        return at(z, other // 2, lax.rem(other, 2), y)

    def remote(src, dst, send, recv, device):
        return pltpu.make_async_remote_copy(
            src_ref=src, dst_ref=dst, send_sem=send, recv_sem=recv, device_id=device, device_id_type=MESH
        )

    barrier = pltpu.get_barrier_semaphore()

    def greet(device):
        pl.semaphore_signal(barrier, inc=1, device_id=device, device_id_type=MESH)

    for i in range(1, nz):
        greet(at(zup(i), x, c, y))
    for i in range(1, 2 * nx):
        greet(in_plane(i))
    for i in range(1, ny):
        greet(at(z, x, c, lax.rem(y + i, ny)))
    pl.semaphore_wait(barrier, nz - 1 + 2 * nx - 1 + ny - 1)

    up_dev, dn_dev, pr_dev = at(zup(1), x, c, y), at(zdn(1), x, c, y), at(z, x, 1 - c, y)

    def up_copy(s, j):
        zb = zdn(s)
        src = (kb, vb)[j].at[zb, c]
        return remote(src, src, up_s.at[s, j], up_r.at[s, j], up_dev)

    def dn_copy(s, j):
        zb = zup(s)
        src = (kb, vb)[j].at[zb, c]
        return remote(src, src, dn_s.at[s, j], dn_r.at[s, j], dn_dev)

    def pr_copy(zb, j):
        src = (kb, vb)[j].at[zb, c]
        return remote(src, src, pr_s.at[zb, j], pr_r.at[zb, j], pr_dev)

    def pr_wait(zb, j):
        dst = (kb, vb)[j].at[zb, 1 - c]
        remote(dst, dst, pr_s.at[zb, j], pr_r.at[zb, j], pr_dev).wait_recv()

    def own_up(j):
        return remote((kd_ref, v_ref)[j], (kb, vb)[j].at[z, c], up_s.at[0, j], up_r.at[0, j], up_dev)

    def own_dn(j):
        return remote((kd_ref, v_ref)[j], (kb, vb)[j].at[z, c], dn_s.at[0, j], dn_r.at[0, j], dn_dev)

    def own_pr(j):
        return remote((kd_ref, v_ref)[j], (kb, vb)[j].at[z, c], pr_s.at[z, j], pr_r.at[z, j], pr_dev)

    def up_has(s, j):
        return s < half or (s == half and j == 0)

    def dn_has(s, j):
        return s < half or (s == half and j == 1)

    for j in range(2):
        if up_has(1, j):
            own_up(j).start()
        if dn_has(1, j):
            own_dn(j).start()

    def t1_copy(i):
        return remote(tot_ref, tt.at[z, xc], t1_s.at[i - 1], t1_r.at[i - 1], in_plane(i))

    def t2_copy(i):
        return remote(tt.at[z], tt.at[z], t2_s.at[i - 1], t2_r.at[i - 1], at(zup(i), x, c, y))

    def q_copy(i):
        return remote(q_ref, qb.at[x], q_s.at[i - 1], q_r.at[i - 1], at(z, lax.rem(x + i, nx), c, y))

    for i in range(1, 2 * nx):
        t1_copy(i).start()
    for i in range(1, nx):
        q_copy(i).start()
    for j in range(2):
        own_pr(j).start()
    pair = at(z, x, c, lax.rem(y, 2) * (y - 1) + (1 - lax.rem(y, 2)) * (y + 1))
    first_rows = pl.ds(0, peer_up.shape[0])
    weights = [
        remote(gate_ref, peer_gate, w_s.at[0], w_r.at[0], pair),
        remote(up_ref.at[first_rows, :], peer_up, w_s.at[1], w_r.at[1], pair),
    ]
    for copy in weights:
        copy.start()
    local = [
        pltpu.make_async_copy(tot_ref, tt.at[z, xc], loc.at[0]),
        pltpu.make_async_copy(q_ref, qb.at[x], loc.at[1]),
        pltpu.make_async_copy(kd_ref, kb.at[z, c], loc.at[2]),
        pltpu.make_async_copy(v_ref, vb.at[z, c], loc.at[3]),
    ]
    for copy in local:
        copy.start()
    mb[...] = jnp.full(mb.shape, NEG, F32)
    acc[...] = jnp.zeros(acc.shape, F32)
    local[0].wait()
    for i in range(1, 2 * nx):
        other = lax.rem(xc - i + 2 * nx, 2 * nx)
        remote(tot_ref, tt.at[z, other], t1_s.at[i - 1], t1_r.at[i - 1], in_plane(i)).wait_recv()
    for i in range(1, nz):
        t2_copy(i).start()
    for copy in local[1:]:
        copy.wait()

    def relay(s):
        for j in range(2):
            if up_has(s, j):
                slot = (kb, vb)[j].at[zdn(s), c]
                remote(slot, slot, up_s.at[s - 1, j], up_r.at[s - 1, j], up_dev).wait_recv()
                if up_has(s + 1, j):
                    up_copy(s, j).start()
                pr_copy(zdn(s), j).start()
            if dn_has(s, j):
                slot = (kb, vb)[j].at[zup(s), c]
                remote(slot, slot, dn_s.at[s - 1, j], dn_r.at[s - 1, j], dn_dev).wait_recv()
                if dn_has(s + 1, j):
                    dn_copy(s, j).start()
                pr_copy(zup(s), j).start()

    lane = lax.broadcasted_iota(jnp.int32, (1, 128), 1)
    low = lane < HN

    def head_offsets(zb):
        def plane(p, run):
            whole = jnp.zeros((1, 128), F32)
            for k in range(2 * nx):
                whole = whole + tt[p, k]
            return run + jnp.where(p < zb, whole, 0.0)
        run = lax.fori_loop(0, nz, plane, jnp.zeros((1, 128), F32))
        for k in range(2 * nx):
            run = run + jnp.where(k < 2 * x, tt[zb, k], 0.0)
        return run, run + tt[zb, 2 * x]

    def make_drow(zb):
        offs = head_offsets(zb)
        parts = [kb[zb, k, pl.ds(256, 16), :].astype(F32) for k in range(2)]
        for h in range(3):
            pieces = []
            for k in range(2):
                off = jnp.sum(jnp.where(lane == h, offs[k], 0.0), axis=1, keepdims=True)
                p = parts[k]
                pieces.append(p[3 * h:3 * h + 1] + p[3 * h + 1:3 * h + 2] + p[3 * h + 2:3 * h + 3] + off)
            drow[h] = jnp.concatenate(pieces, axis=1)

    scales = (HW ** -0.5 * LOG2E, HN ** -0.5 * LOG2E, HN ** -0.5 * LOG2E)

    def tile(zb, xq, masked):
        q = qb[xq]
        qw, qn = q[:, :128], q[:, 128:]
        zero = jnp.zeros_like(qn)
        heads = (qw, jnp.where(low, qn, zero), jnp.where(low, zero, qn))
        keys = jnp.concatenate([kb[zb, 0, :256, :], kb[zb, 1, :256, :]], axis=0)
        vals = jnp.concatenate([vb[zb, 0], vb[zb, 1]], axis=0)
        ones = jnp.ones((512, 128), BF16)
        if masked:
            rows = lax.broadcasted_iota(jnp.int32, (256, 512), 0) + (xq * 512 + c * 256)
            cols = lax.broadcasted_iota(jnp.int32, (256, 512), 1) + x * 512
            seen = cols <= rows
        for h in range(3):
            side = slice(0, 128) if h == 0 else slice(128, 256)
            s = lax.dot_general(heads[h], keys[:, side], (((1,), (1,)), ((), ())), preferred_element_type=F32)
            r = s * scales[h] - drow[h]
            if masked:
                r = jnp.where(seen, r, NEG)
            old = mb[xq, h]
            new = jnp.maximum(old, jnp.max(r, axis=1, keepdims=True))
            p = jnp.exp2(r - jnp.concatenate([new] * 4, axis=1)).astype(BF16)
            shrink = jnp.exp2(old - new)
            mb[xq, h] = new
            right = jnp.concatenate([vals[:, side], ones], axis=1)
            pv = jnp.dot(p, right, preferred_element_type=F32)
            acc[xq, h] = acc[xq, h] * jnp.concatenate([shrink, shrink], axis=1) + pv

    def both(zb):
        make_drow(zb)

        def one(xq, carry):
            tile(zb, xq, False)
            return carry
        lax.fori_loop(0, nx, one, 0)

    relay(1)
    for i in range(1, nx):
        src = lax.rem(x - i + nx, nx)
        remote(q_ref, qb.at[src], q_s.at[i - 1], q_r.at[i - 1], at(z, src, c, y)).wait_recv()
    for i in range(1, nz):
        slot = tt.at[zdn(i)]
        remote(slot, slot, t2_s.at[i - 1], t2_r.at[i - 1], at(zdn(i), x, c, y)).wait_recv()
    for j in range(2):
        pr_wait(z, j)
    make_drow(z)

    def own(xq, carry):
        @pl.when(xq >= x)
        def _():
            tile(z, xq, True)
        return carry
    lax.fori_loop(0, nx, own, 0)

    for s in range(1, half):
        relay(s + 1)
        for j in range(2):
            pr_wait(zdn(s), j)
            pr_wait(zup(s), j)
        for zb, needed in ((zdn(s), z >= s), (zup(s), z + s >= nz)):
            @pl.when(needed)
            def _():
                both(zb)
    if half == 1:
        pass
    for j in range(2):
        pr_wait(zdn(half), j)

    @pl.when(z >= half)
    def _():
        make_drow(zdn(half))

    def o_copies(i):
        dev = at(z, lax.rem(x + i, nx), c, y)
        return (
            remote(ob.at[i], orv.at[i], o_s.at[i, 0], o_r.at[i, 0], dev),
            remote(sb.at[i], srv.at[i], o_s.at[i, 1], o_r.at[i, 1], dev),
        )

    def last(k, carry):
        i = lax.rem(k + 1, nx)
        xq = lax.rem(x + i, nx)

        @pl.when(z >= half)
        def _():
            tile(zdn(half), xq, False)

        outs, lses = [], []
        for h in range(3):
            total = acc[xq, h, :, 128:]
            some = total > 0.0
            safe = jnp.where(some, total, 1.0)
            outs.append(acc[xq, h, :, :128] / safe)
            lses.append(jnp.where(some, mb[xq, h] + jnp.log2(safe), NEG))
        wide, narrow = outs[0], jnp.where(low, outs[1], outs[2])
        ob[i] = jnp.concatenate([wide, narrow], axis=1).astype(BF16)
        packed = jnp.where(lane == 0, lses[0], jnp.where(lane == 1, lses[1], lses[2]))
        sb[i] = jnp.transpose(packed)[:8]

        @pl.when(i > 0)
        def _():
            for copy in o_copies(i):
                copy.start()
        return carry
    lax.fori_loop(0, nx, last, 0)

    for i in range(1, nx):
        src = lax.rem(x - i + nx, nx)
        for copy in o_copies(i):
            copy.wait_recv()
    stats = [sb[0]] + [srv[i] for i in range(1, nx)]
    outs = [ob[0]] + [orv[i] for i in range(1, nx)]
    top = functools.reduce(jnp.maximum, stats)
    shares = [jnp.exp2(t - top) for t in stats]
    whole = functools.reduce(jnp.add, shares)
    shares = [t / whole for t in shares]
    columns = jnp.transpose(jnp.concatenate(shares + [jnp.zeros((128 - 8 * nx, 256), F32)], axis=0))
    wide = jnp.zeros((256, 128), F32)
    narrow = jnp.zeros((256, 128), F32)
    for i in range(nx):
        o = outs[i].astype(F32)
        wide = wide + columns[:, 8 * i:8 * i + 1] * o[:, :128]
        narrow = narrow + jnp.where(low, columns[:, 8 * i + 1:8 * i + 2], columns[:, 8 * i + 2:8 * i + 3]) * o[:, 128:]
    ab[...] = jnp.concatenate([wide, narrow], axis=1).astype(BF16)

    share = 256 // ny

    def rows_of(y_):
        return ab.at[pl.ds(pl.multiple_of(y_ * share, share), share), :]

    def y_copy(i):
        other = lax.rem(y + i, ny)
        return remote(rows_of(other), ar.at[y], y_s.at[i - 1], y_r.at[i - 1], at(z, x, c, other))

    for i in range(1, ny):
        y_copy(i).start()
    att_ref[y] = ab[pl.ds(pl.multiple_of(y * share, share), share), :]
    for i in range(1, ny):
        src = lax.rem(y - i + ny, ny)
        remote(rows_of(src), ar.at[src], y_s.at[i - 1], y_r.at[i - 1], at(z, x, c, src)).wait_recv()
        att_ref[src] = ar[src]

    for copy in weights:
        copy.wait()
    for j in range(2):
        if up_has(1, j):
            own_up(j).wait_send()
        if dn_has(1, j):
            own_dn(j).wait_send()
        own_pr(j).wait_send()
        for s in range(1, half + 1):
            if up_has(s, j):
                if up_has(s + 1, j):
                    up_copy(s, j).wait_send()
                pr_copy(zdn(s), j).wait_send()
            if dn_has(s, j):
                if dn_has(s + 1, j):
                    dn_copy(s, j).wait_send()
                pr_copy(zup(s), j).wait_send()
    for i in range(1, 2 * nx):
        t1_copy(i).wait_send()
    for i in range(1, nz):
        t2_copy(i).wait_send()
    for i in range(1, nx):
        q_copy(i).wait_send()
        for copy in o_copies(i):
            copy.wait_send()
    for i in range(1, ny):
        y_copy(i).wait_send()


def attend(dims, q, kd, v, tot, gate, up):
    nz, nx, ny = dims
    half = nz // 2
    dma = pltpu.SemaphoreType.DMA
    vmem = pl.BlockSpec(memory_space=pltpu.VMEM)
    hbm = pl.BlockSpec(memory_space=pl.ANY)
    return pl.pallas_call(
        functools.partial(attention_kernel, dims),
        out_shape=[
            jax.ShapeDtypeStruct((ny, 256 // ny, 256), BF16),
            jax.ShapeDtypeStruct(gate.shape, BF16),
            jax.ShapeDtypeStruct((up.shape[0] // 2, up.shape[1]), BF16),
        ],
        in_specs=[vmem] * 4 + [hbm] * 2,
        out_specs=[vmem, hbm, hbm],
        scratch_shapes=[
            pltpu.VMEM((nx, 256, 256), BF16),
            pltpu.VMEM((nz, 2, 272, 256), BF16),
            pltpu.VMEM((nz, 2, 256, 256), BF16),
            pltpu.VMEM((nz, 2 * nx, 1, 128), F32),
            pltpu.VMEM((3, 1, 512), F32),
            pltpu.VMEM((nx, 3, 256, 128), F32),
            pltpu.VMEM((nx, 3, 256, 256), F32),
            pltpu.VMEM((nx, 256, 256), BF16),
            pltpu.VMEM((nx, 8, 256), F32),
            pltpu.VMEM((nx, 256, 256), BF16),
            pltpu.VMEM((nx, 8, 256), F32),
            pltpu.VMEM((256, 256), BF16),
            pltpu.VMEM((ny, 256 // ny, 256), BF16),
            dma((nx,)), dma((nx,)),
            dma((half + 1, 2)), dma((half + 1, 2)), dma((half + 1, 2)), dma((half + 1, 2)),
            dma((nz, 2)), dma((nz, 2)),
            dma((2 * nx,)), dma((2 * nx,)), dma((nz,)), dma((nz,)),
            dma((nx, 2)), dma((nx, 2)), dma((ny,)), dma((ny,)), dma((4,)), dma((2,)), dma((2,)),
        ],
        compiler_params=pltpu.CompilerParams(collective_id=1, has_side_effects=True, vmem_limit_bytes=40 * 2**20),
        cost_estimate=pl.CostEstimate(flops=10**10, bytes_accessed=10**7, transcendentals=12 * 10**6),
        name="attend",
    )(q, kd, v, tot, gate, up)


def prepare(query_wide, key_wide, value_wide, query_narrow, key_narrow, value_narrow, gate_wide, gate_narrow):
    gates = jnp.concatenate([gate_wide, gate_narrow], axis=1)
    run = jnp.cumsum(jax.nn.log_sigmoid(gates).T, axis=1) * LOG2E
    tot = jnp.pad(run[:, -1], (0, 125))[None, :]
    high = lax.reduce_precision(run, 8, 7)
    mid = lax.reduce_precision(run - high, 8, 7)
    parts = jnp.stack([high, mid, run - high - mid], axis=1).reshape(9, 256)
    parts = jnp.pad(parts, ((0, 7), (0, 0))).astype(BF16)
    q = jnp.concatenate([query_wide, query_narrow], axis=1)
    kd = jnp.concatenate([jnp.concatenate([key_wide, key_narrow], axis=1), parts], axis=0)
    v = jnp.concatenate([value_wide, value_narrow], axis=1)
    return q, kd, v, tot


def paired(y):
    return lax.rem(y, 2) * (y - 1) + (1 - lax.rem(y, 2)) * (y + 1)


def far_first(t, nz):
    m = nz // 2 - (t + 1) // 2
    return jnp.where((lax.rem(t, 2) == 0) & (t > 0), -m, m)


def moe_kernel(
    dims, att_ref, res_ref, wide_ref, narrow_ref, gain_ref, routing_ref, weight_ref,
    gate_ref, up_ref, down_ref, peer_gate, peer_up, out_ref,
    ow, on, perm, tmp, snd, arr, arc, xo, xc, mid, wg, wu, wd, total, part, back, bsd, ret, rows,
    a_s, a_r, c_s, c_r, p_s, p_r, b_s, b_r, w_s, w_r, loc,
):
    nz, nx, ny = dims
    plane = 2 * nx
    count = nz * plane
    step = 4 * plane
    sp, y = lax.axis_index("sp"), lax.axis_index("tp")
    z = sp // plane
    half = peer_up.shape[0]
    fetch = [
        pltpu.make_async_copy(wide_ref, ow, loc.at[0]),
        pltpu.make_async_copy(narrow_ref, on, loc.at[1]),
        pltpu.make_async_copy(gate_ref, wg.at[0], loc.at[2]),
        pltpu.make_async_copy(peer_gate, wg.at[1], loc.at[3]),
        pltpu.make_async_copy(up_ref, wu.at[0], loc.at[4]),
        pltpu.make_async_copy(peer_up, wu.at[1, pl.ds(0, half), :], loc.at[5]),
        pltpu.make_async_copy(down_ref, wd.at[0], loc.at[6]),
    ]
    for copy in fetch:
        copy.start()

    def remote(src, dst, send, recv, device):
        return pltpu.make_async_remote_copy(
            src_ref=src, dst_ref=dst, send_sem=send, recv_sem=recv, device_id=device, device_id_type=MESH
        )

    barrier = pltpu.get_barrier_semaphore()
    pair, across = (sp, paired(y)), (sp, ny - 1 - y)

    def greet(i, carry):
        pl.semaphore_signal(barrier, inc=1, device_id=(lax.rem(sp + i, count), y), device_id_type=MESH)
        return carry
    lax.fori_loop(1, count, greet, 0)
    pl.semaphore_signal(barrier, inc=1, device_id=pair, device_id_type=MESH)
    pl.semaphore_signal(barrier, inc=1, device_id=across, device_id_type=MESH)

    own_rows = routing_ref.shape[0]
    names = [routing_ref[:, k:k + 1].astype(F32) for k in range(2)]
    expert = lax.broadcasted_iota(jnp.int32, (own_rows, count), 1).astype(F32)
    hits = [jnp.where(name == expert, 1.0, 0.0) for name in names]
    earlier = lax.broadcasted_iota(jnp.int32, (own_rows, own_rows), 1) < lax.broadcasted_iota(
        jnp.int32, (own_rows, own_rows), 0
    )
    before = jnp.dot(
        jnp.where(earlier, 1.0, 0.0).astype(BF16), (hits[0] + hits[1]).astype(BF16), preferred_element_type=F32
    )
    slot = lax.broadcasted_iota(jnp.int32, (own_rows, 4 * count), 1).astype(F32)
    chosen = [
        slot == names[k] * 4.0 + jnp.sum(before * hits[k], axis=1, keepdims=True) for k in range(2)
    ]

    for copy in fetch[:2]:
        copy.wait()
    a_wide = jnp.concatenate([att_ref[k, :, :128] for k in range(ny)], axis=1)
    a_narrow = jnp.concatenate([att_ref[k, :, 128:] for k in range(ny)], axis=1)
    mixed = jnp.dot(a_wide, ow[...], preferred_element_type=F32) + jnp.dot(a_narrow, on[...], preferred_element_type=F32)
    middle = (res_ref[...].astype(F32) + mixed).astype(BF16)
    mid[...] = middle
    middle = middle.astype(F32)
    spread = jnp.mean(middle * middle, axis=1, keepdims=True)
    normed = (middle * lax.rsqrt(spread + epsilon) * gain_ref[...]).astype(BF16)
    picker = jnp.where(chosen[0] | chosen[1], 1.0, 0.0).astype(BF16)
    perm[...] = lax.dot_general(picker, normed, (((0,), (0,)), ((), ())), preferred_element_type=F32)

    def cut(k, carry):
        v = perm[pl.ds(pl.multiple_of(8 * k, 8), 8), :]
        snd[2 * k] = v[:4].astype(BF16)
        snd[2 * k + 1] = v[4:].astype(BF16)
        return carry
    lax.fori_loop(0, count // 2, cut, 0)
    pl.semaphore_wait(barrier, count - 1 + 2)

    def to_plane(t):
        return lax.rem(z + far_first(t, nz) + nz, nz)

    def from_plane(t):
        return lax.rem(z - far_first(t, nz) + nz, nz)

    def out_copy(e):
        return remote(snd.at[e], arr.at[sp], a_s.at[e], a_r.at[sp], (e, y))

    def each_other(p, act):
        def one(k, carry):
            e = p * plane + k

            @pl.when(e != sp)
            def _():
                act(e)
            return carry
        lax.fori_loop(0, plane, one, 0)

    def send(t, carry):
        each_other(to_plane(t), lambda e: out_copy(e).start())
        return carry
    lax.fori_loop(0, nz, send, 0)
    weights = [
        remote(up_ref.at[pl.ds(half, half), :], wu.at[1, pl.ds(half, half), :], w_s.at[0], w_r.at[0], pair),
        remote(down_ref, wd.at[1], w_s.at[1], w_r.at[1], pair),
    ]
    for copy in weights:
        copy.start()
    keep = pltpu.make_async_copy(snd.at[sp], arr.at[sp], loc.at[7])
    keep.start()
    keep.wait()

    def to_rows(take):
        for k in range(plane // 2):
            tmp[8 * k:8 * k + 8, :] = jnp.concatenate([take(2 * k).astype(F32), take(2 * k + 1).astype(F32)], axis=0)

    def rows_at(t):
        return pl.ds(pl.multiple_of(t * step, step), step)

    def cross_copy(p):
        some = pl.ds(p * plane, plane)
        return remote(arr.at[some], arc.at[some], c_s.at[p], c_r.at[p], across)

    def arrive_cross(t):
        p = from_plane(t)
        cross_copy(p).wait_recv()
        to_rows(lambda k: arc[p * plane + k])
        xc[rows_at(t), :] = tmp[...].astype(BF16)

    def arrive(t, carry):
        p = from_plane(t)
        each_other(p, lambda s: remote(snd.at[s], arr.at[s], a_s.at[s], a_r.at[s], (s, y)).wait_recv())
        cross_copy(p).start()
        to_rows(lambda k: arr[p * plane + k])
        xo[rows_at(t), :] = tmp[...].astype(BF16)

        @pl.when(t >= nz // 2)
        def _():
            arrive_cross(t - nz // 2)
        return carry
    lax.fori_loop(0, nz, arrive, 0)
    for copy in fetch[2:]:
        copy.wait()
    for copy in weights:
        copy.wait_recv()

    def hidden(x):
        both = []
        for k in range(2):
            g = jnp.dot(x, wg[k], preferred_element_type=F32)
            u = jnp.dot(x, wu[k], preferred_element_type=F32)
            both.append((jax.nn.silu(g) * u).astype(BF16))
        return both

    def down(h, put):
        width = 512
        for q in range(wd.shape[2] // width):
            cols = slice(q * width, (q + 1) * width)
            put(
                cols,
                jnp.dot(h[0], wd[0, :, cols], preferred_element_type=F32)
                + jnp.dot(h[1], wd[1, :, cols], preferred_element_type=F32),
            )

    def part_copy(t):
        some = rows_at(t)
        return remote(part.at[some, :], back.at[some, :], p_s.at[t], p_r.at[t], across)

    def send_part(t, carry):
        part_copy(t).start()
        return carry

    def cross_half(k):
        some = slice(k * step * nz // 2, (k + 1) * step * nz // 2)

        def put(cols, value):
            part[some, cols] = value.astype(BF16)
        down(hidden(xc[some, :]), put)
        lax.fori_loop(k * nz // 2, (k + 1) * nz // 2, send_part, 0)

    cross_half(0)

    def put_total(cols, value):
        total[:, cols] = value
    down(hidden(xo[...]), put_total)

    def late(t, carry):
        arrive_cross(t)
        return carry
    lax.fori_loop(nz // 2, nz, late, 0)
    cross_half(1)

    def back_copy(e):
        return remote(bsd.at[e], ret.at[sp], b_s.at[e], b_r.at[sp], (e, y))

    def finish(t, carry):
        p = from_plane(t)
        part_copy(t).wait_recv()
        some = rows_at(t)
        tmp[...] = total[some, :] + back[some, :].astype(F32)
        for k in range(plane // 2):
            v = tmp[8 * k:8 * k + 8, :]
            bsd[p * plane + 2 * k] = v[:4].astype(BF16)
            bsd[p * plane + 2 * k + 1] = v[4:].astype(BF16)
        each_other(p, lambda e: back_copy(e).start())
        return carry
    lax.fori_loop(0, nz, finish, 0)
    last = pltpu.make_async_copy(bsd.at[sp], ret.at[sp], loc.at[8])
    last.start()
    last.wait()

    def returned(t, carry):
        p = to_plane(t)
        each_other(p, lambda e: remote(bsd.at[e], ret.at[e], b_s.at[e], b_r.at[e], (e, y)).wait_recv())
        to_rows(lambda k: ret[p * plane + k])
        rows[rows_at(p), :] = tmp[...].astype(BF16)
        return carry
    lax.fori_loop(0, nz, returned, 0)
    share = jnp.where(chosen[0], weight_ref[:, 0:1], 0.0) + jnp.where(chosen[1], weight_ref[:, 1:2], 0.0)
    combined = mid[...].astype(F32)
    for _ in range(3):
        term = share.astype(BF16)
        share = share - term.astype(F32)
        combined = combined + jnp.dot(term, rows[...], preferred_element_type=F32)
    out_ref[...] = combined.astype(BF16)

    for copy in weights:
        copy.wait_send()

    def drain(t, carry):
        each_other(t, lambda e: out_copy(e).wait_send())
        each_other(t, lambda e: back_copy(e).wait_send())
        cross_copy(t).wait_send()
        part_copy(t).wait_send()
        return carry
    lax.fori_loop(0, nz, drain, 0)


def experts(dims, att, residual, wide, narrow, gain, routing, route_weight, gate, up, down, peer_gate, peer_up):
    nz, nx, ny = dims
    count, features = nz * nx * 2, residual.shape[1]
    dma = pltpu.SemaphoreType.DMA
    vmem = pl.BlockSpec(memory_space=pltpu.VMEM)
    hbm = pl.BlockSpec(memory_space=pl.ANY)
    blocks = pltpu.VMEM((count, 4, features), BF16)
    table = pltpu.VMEM((4 * count, features), BF16)
    return pl.pallas_call(
        functools.partial(moe_kernel, dims),
        out_shape=jax.ShapeDtypeStruct(residual.shape, BF16),
        in_specs=[vmem, vmem, hbm, hbm, vmem, vmem, vmem] + [hbm] * 5,
        out_specs=vmem,
        scratch_shapes=[
            pltpu.VMEM(wide.shape, BF16),
            pltpu.VMEM(narrow.shape, BF16),
            pltpu.VMEM((4 * count, features), F32),
            pltpu.VMEM((8 * nx, features), F32),
            blocks, blocks, blocks, table, table,
            pltpu.VMEM(residual.shape, BF16),
            pltpu.VMEM((2, *gate.shape), BF16),
            pltpu.VMEM((2, *up.shape), BF16),
            pltpu.VMEM((2, *down.shape), BF16),
            pltpu.VMEM((4 * count, features), F32),
            table, table, blocks, blocks, table,
            dma((count,)), dma((count,)), dma((nz,)), dma((nz,)), dma((nz,)), dma((nz,)),
            dma((count,)), dma((count,)), dma((2,)), dma((2,)), dma((9,)),
        ],
        compiler_params=pltpu.CompilerParams(collective_id=2, has_side_effects=True, vmem_limit_bytes=48 * 2**20),
        cost_estimate=pl.CostEstimate(flops=10**9, bytes_accessed=10**7, transcendentals=1000),
        name="experts",
    )(att, residual, wide, narrow, gain, routing, route_weight, gate, up, down, peer_gate, peer_up)


def body(
    residual,
    query_wide,
    key_wide,
    value_wide,
    query_narrow,
    key_narrow,
    value_narrow,
    gate_wide,
    gate_narrow,
    out_wide,
    out_narrow,
    norm_gain,
    routing,
    route_weight,
    gate_weight,
    up_weight,
    down_weight,
):
    ny = lax.axis_size("tp")
    nx = NX
    dims = (lax.axis_size("sp") // (2 * nx), nx, ny)
    gate, up, down = gate_weight[0], up_weight[0], down_weight[0]
    ready = prepare(
        query_wide, key_wide, value_wide, query_narrow, key_narrow, value_narrow, gate_wide, gate_narrow
    )
    att, peer_gate, peer_up = attend(dims, *ready, gate, up)
    return experts(
        dims, att, residual, out_wide, out_narrow, norm_gain[None, :], routing, route_weight,
        gate, up, down, peer_gate, peer_up,
    )


def solution(mesh):
    placed = (
        P(("sp", "tp"), None),
        P("sp", "tp"),
        P("sp", "tp"),
        P("sp", "tp"),
        P("sp", "tp"),
        P("sp", "tp"),
        P("sp", "tp"),
        P("sp", "tp"),
        P("sp", "tp"),
        P(),
        P(),
        P(),
        P(("sp", "tp"), None),
        P(("sp", "tp"), None),
        P("sp", None, "tp"),
        P("sp", None, "tp"),
        P("sp", "tp", None),
    )
    return jax.shard_map(
        body, mesh=mesh, in_specs=placed, out_specs=P(("sp", "tp"), None), check_vma=False
    )
```

```python
import functools
import math

import jax
import jax.numpy as jnp
from jax import lax
from jax.experimental import pallas as pl
from jax.experimental.pallas import tpu as pltpu
from jax.sharding import PartitionSpec as P

MESH = pl.DeviceIdType.MESH
F32, BF16 = jnp.float32, jnp.bfloat16
HW = 128
HN = 64
NX = 4
LOG2E = math.log2(math.e)
NEG = -1e30
LOWEST = -1e20
epsilon = 1e-06


def paired(y):
    return lax.rem(y, 2) * (y - 1) + (1 - lax.rem(y, 2)) * (y + 1)


def far_first(t, nz):
    m = nz // 2 - (t + 1) // 2
    return jnp.where((lax.rem(t, 2) == 0) & (t > 0), -m, m)


def layer_kernel(
    dims, res_ref, qw_ref, kw_ref, vw_ref, qn_ref, kn_ref, vn_ref, gw_ref, gn_ref, wide_ref, narrow_ref, gain_ref,
    routing_ref, weight_ref, gate_ref, up_ref, down_ref, out_ref,
    q_ref, kd_ref, v_ref, tot_ref, qb, kb, vb, tt, kaug, mb, acc, ob, sb, orv, srv, ab, ar,
    q_s, q_r, up_s, up_r, dn_s, dn_r, pr_s, pr_r, t1_s, t1_r, t2_s, t2_r, o_s, o_r, y_s, y_r, loc,
    ow, on, perm, tmp, snd, arr, arc, xo, xs, mid, wg, wu, wd, total, part, back, bsd, ret, rows,
    a_s, a_r, c_s, c_r, p_s, p_r, b_s, b_r, w_s, w_r, loc2,
):
    nz, nx, ny = dims
    half = nz // 2
    plane = 2 * nx
    count = nz * plane
    step = 4 * plane
    sp, y = lax.axis_index("sp"), lax.axis_index("tp")
    fetch = [
        pltpu.make_async_copy(wide_ref, ow, loc2.at[0]),
        pltpu.make_async_copy(narrow_ref, on, loc2.at[1]),
        pltpu.make_async_copy(gate_ref, wg.at[0], loc2.at[2]),
        pltpu.make_async_copy(up_ref, wu.at[0], loc2.at[3]),
        pltpu.make_async_copy(down_ref, wd.at[0], loc2.at[4]),
    ]
    for copy in fetch:
        copy.start()
    c = lax.rem(sp, 2)
    x = lax.rem(sp // 2, nx)
    z = sp // (2 * nx)
    xc = x * 2 + c

    def at(z_, x_, c_, y_):
        return ((z_ * nx + x_) * 2 + c_, y_)

    def zup(i):
        return lax.rem(z + i, nz)

    def zdn(i):
        return lax.rem(z - i + nz, nz)

    def in_plane(i):
        other = lax.rem(xc + i, 2 * nx)
        return at(z, other // 2, lax.rem(other, 2), y)

    def remote(src, dst, send, recv, device):
        return pltpu.make_async_remote_copy(
            src_ref=src, dst_ref=dst, send_sem=send, recv_sem=recv, device_id=device, device_id_type=MESH
        )

    barrier = pltpu.get_barrier_semaphore()

    def greet(device):
        pl.semaphore_signal(barrier, inc=1, device_id=device, device_id_type=MESH)

    def greet_along(i, carry):
        greet((lax.rem(sp + i, count), y))
        return carry
    lax.fori_loop(1, count, greet_along, 0)
    for i in range(1, ny):
        greet((sp, lax.rem(y + i, ny)))
    lane = lax.broadcasted_iota(jnp.int32, (1, 128), 1)
    gates = jnp.where(lane == 0, gw_ref[...], jnp.where(lane == 1, gn_ref[:, 0:1], gn_ref[:, 1:2]))
    logs = jnp.minimum(gates, 0.0) - jnp.log1p(jnp.exp(-jnp.abs(gates)))
    logs = jnp.where(lane < 3, logs, 0.0)
    until = lax.broadcasted_iota(jnp.int32, (256, 256), 1) <= lax.broadcasted_iota(jnp.int32, (256, 256), 0)
    until = jnp.where(until, 1.0, 0.0).astype(BF16)
    run = jnp.zeros((256, 128), F32)
    for _ in range(3):
        term = logs.astype(BF16)
        logs = logs - term.astype(F32)
        run = run + jnp.dot(until, term, preferred_element_type=F32)
    run = run * LOG2E
    tot_ref[...] = run[255:256]
    left = jnp.transpose(run)[:8]
    terms = []
    for _ in range(3):
        term = left.astype(BF16).astype(F32)
        left = left - term
        terms.append(term)
    kd_ref[256:288, :] = jnp.concatenate(terms + [jnp.zeros((8, 256), F32)], axis=0).astype(BF16)
    kd_ref[0:256, :128] = kw_ref[...]
    kd_ref[0:256, 128:] = kn_ref[...]
    v_ref[0:128, :] = jnp.transpose(vw_ref[...].astype(F32)).astype(BF16)
    v_ref[128:256, :] = jnp.transpose(vn_ref[...].astype(F32)).astype(BF16)
    q_ref[0:128, :] = jnp.transpose(qw_ref[...].astype(F32) * (HW ** -0.5 * LOG2E)).astype(BF16)
    q_ref[128:256, :] = jnp.transpose(qn_ref[...].astype(F32) * (HN ** -0.5 * LOG2E)).astype(BF16)
    own_rows = routing_ref.shape[0]
    names = [routing_ref[:, k:k + 1].astype(F32) for k in range(2)]
    expert = lax.broadcasted_iota(jnp.int32, (own_rows, count), 1).astype(F32)
    hits = [jnp.where(name == expert, 1.0, 0.0) for name in names]
    earlier = lax.broadcasted_iota(jnp.int32, (own_rows, own_rows), 1) < lax.broadcasted_iota(
        jnp.int32, (own_rows, own_rows), 0
    )
    before = jnp.dot(
        jnp.where(earlier, 1.0, 0.0).astype(BF16), (hits[0] + hits[1]).astype(BF16), preferred_element_type=F32
    )
    slot = lax.broadcasted_iota(jnp.int32, (own_rows, 4 * count), 1).astype(F32)
    chosen = [
        slot == names[k] * 4.0 + jnp.sum(before * hits[k], axis=1, keepdims=True) for k in range(2)
    ]
    pl.semaphore_wait(barrier, count - 1 + ny - 1)

    up_dev, dn_dev, pr_dev = at(zup(1), x, c, y), at(zdn(1), x, c, y), at(z, x, 1 - c, y)

    def up_copy(s, j):
        zb = zdn(s)
        src = (kb, vb)[j].at[zb, c]
        return remote(src, src, up_s.at[s, j], up_r.at[s, j], up_dev)

    def dn_copy(s, j):
        zb = zup(s)
        src = (kb, vb)[j].at[zb, c]
        return remote(src, src, dn_s.at[s, j], dn_r.at[s, j], dn_dev)

    def pr_copy(zb, j):
        src = (kb, vb)[j].at[zb, c]
        return remote(src, src, pr_s.at[zb, j], pr_r.at[zb, j], pr_dev)

    def pr_wait(zb, j):
        dst = (kb, vb)[j].at[zb, 1 - c]
        remote(dst, dst, pr_s.at[zb, j], pr_r.at[zb, j], pr_dev).wait_recv()

    def own_up(j):
        return remote((kd_ref, v_ref)[j], (kb, vb)[j].at[z, c], up_s.at[0, j], up_r.at[0, j], up_dev)

    def own_dn(j):
        return remote((kd_ref, v_ref)[j], (kb, vb)[j].at[z, c], dn_s.at[0, j], dn_r.at[0, j], dn_dev)

    def own_pr(j):
        return remote((kd_ref, v_ref)[j], (kb, vb)[j].at[z, c], pr_s.at[z, j], pr_r.at[z, j], pr_dev)

    def up_has(s, j):
        return s < half or (s == half and j == 0)

    def dn_has(s, j):
        return s < half or (s == half and j == 1)

    for j in range(2):
        if up_has(1, j):
            own_up(j).start()
        if dn_has(1, j):
            own_dn(j).start()

    def t1_copy(i):
        return remote(tot_ref, tt.at[z, xc], t1_s.at[i - 1], t1_r.at[i - 1], in_plane(i))

    def t2_copy(i):
        return remote(tt.at[z], tt.at[z], t2_s.at[i - 1], t2_r.at[i - 1], at(zup(i), x, c, y))

    def q_copy(i):
        return remote(q_ref, qb.at[x], q_s.at[i - 1], q_r.at[i - 1], at(z, lax.rem(x + i, nx), c, y))

    for i in range(1, 2 * nx):
        t1_copy(i).start()
    for i in range(1, nx):
        q_copy(i).start()
    for j in range(2):
        own_pr(j).start()
    pair, across = (sp, paired(y)), (sp, ny - 1 - y)
    cut_at = up_ref.shape[0] * 3 // 4
    early, rest = pl.ds(0, cut_at), pl.ds(cut_at, up_ref.shape[0] - cut_at)
    weights = [
        remote(gate_ref, wg.at[1], w_s.at[0], w_r.at[0], pair),
        remote(up_ref.at[early, :], wu.at[1, early, :], w_s.at[1], w_r.at[1], pair),
        remote(up_ref.at[rest, :], wu.at[1, rest, :], w_s.at[2], w_r.at[2], pair),
        remote(down_ref, wd.at[1], w_s.at[3], w_r.at[3], pair),
    ]
    for copy in weights[:2]:
        copy.start()
    local = [
        pltpu.make_async_copy(tot_ref, tt.at[z, xc], loc.at[0]),
        pltpu.make_async_copy(q_ref, qb.at[x], loc.at[1]),
        pltpu.make_async_copy(kd_ref, kb.at[z, c], loc.at[2]),
        pltpu.make_async_copy(v_ref, vb.at[z, c], loc.at[3]),
    ]
    for copy in local:
        copy.start()
    mb[...] = jnp.full(mb.shape, LOWEST, F32)
    acc[...] = jnp.zeros(acc.shape, F32)
    local[0].wait()
    for i in range(1, 2 * nx):
        other = lax.rem(xc - i + 2 * nx, 2 * nx)
        remote(tot_ref, tt.at[z, other], t1_s.at[i - 1], t1_r.at[i - 1], in_plane(i)).wait_recv()
    for i in range(1, nz):
        t2_copy(i).start()
    for copy in local[1:]:
        copy.wait()

    def relay(s):
        for j in range(2):
            @pl.when(s <= (half if j == 0 else half - 1))
            def _():
                slot = (kb, vb)[j].at[zdn(s), c]
                remote(slot, slot, up_s.at[s - 1, j], up_r.at[s - 1, j], up_dev).wait_recv()

                @pl.when(s + 1 <= (half if j == 0 else half - 1))
                def _():
                    up_copy(s, j).start()
                pr_copy(zdn(s), j).start()

            @pl.when(s <= (half if j == 1 else half - 1))
            def _():
                slot = (kb, vb)[j].at[zup(s), c]
                remote(slot, slot, dn_s.at[s - 1, j], dn_r.at[s - 1, j], dn_dev).wait_recv()

                @pl.when(s + 1 <= (half if j == 1 else half - 1))
                def _():
                    dn_copy(s, j).start()
                pr_copy(zup(s), j).start()

    low = lax.broadcasted_iota(jnp.int32, (128, 1), 0) < HN

    def head_offsets(zb):
        def plane(p, run):
            whole = jnp.zeros((1, 128), F32)
            for k in range(2 * nx):
                whole = whole + tt[p, k]
            return run + jnp.where(p < zb, whole, 0.0)
        run = lax.fori_loop(0, nz, plane, jnp.zeros((1, 128), F32))
        for k in range(2 * nx):
            run = run + jnp.where(k < 2 * x, tt[zb, k], 0.0)
        return run, run + tt[zb, 2 * x]

    def offsets(zb):
        return [
            [jnp.sum(jnp.where(lane == h, row, 0.0), axis=1, keepdims=True) for h in range(3)]
            for row in head_offsets(zb)
        ]

    def make_kaug(zb):
        for k in range(2):
            part = jnp.concatenate([kb[zb, k, 256:288, :].astype(F32), jnp.zeros((96, 256), F32)], axis=0)
            kaug[256 * k:256 * k + 256, :] = jnp.transpose(part).astype(BF16)

    spans = ((0, 128), (144, 64), (224, 64))
    row_of = lax.broadcasted_iota(jnp.int32, (128, 256), 0)
    minus = [jnp.where((lax.rem(row_of, 8) == h) & (row_of < 24), -1.0, 0.0).astype(BF16) for h in range(3)]

    def tiles(zb, offs, masked):
        keys = jnp.concatenate([kb[zb, 0, 0:256, :], kb[zb, 1, 0:256, :]], axis=0)
        vals = jnp.concatenate([vb[zb, 0], vb[zb, 1]], axis=1)
        more = kaug[...]
        ones = jnp.ones((16, 512), BF16)
        work = [(xq, h) for xq in range(nx) for h in range(3)]
        scores, weights_, shrinks = [], [], []
        for xq, h in work:
            side = slice(0, 128) if h == 0 else slice(128, 256)
            q = qb[xq, side, :]
            if h > 0:
                q = jnp.where(low if h == 1 else jnp.logical_not(low), q, jnp.zeros_like(q))
            scores.append(
                jnp.dot(
                    jnp.concatenate([keys[:, side], more], axis=1),
                    jnp.concatenate([q, minus[h]], axis=0),
                    preferred_element_type=F32,
                )
            )
        for (xq, h), r in zip(work, scores):
            if masked:
                places = lax.broadcasted_iota(jnp.int32, (512, 256), 0) + x * 512
                wanted = lax.broadcasted_iota(jnp.int32, (512, 256), 1) + (xq * 512 + c * 256)
                r = jnp.where(places <= wanted, r, NEG)
            old = mb[xq, h]
            new = old
            for k in range(2):
                new = jnp.maximum(new, jnp.max(r[256 * k:256 * k + 256], axis=0, keepdims=True) - offs[k][h])
            weights_.append(
                jnp.concatenate(
                    [jnp.exp2(r[256 * k:256 * k + 256] - (new + offs[k][h])).astype(BF16) for k in range(2)], axis=0
                )
            )
            shrinks.append(jnp.exp2(old - new))
            mb[xq, h] = new
        for (xq, h), p, shrink in zip(work, weights_, shrinks):
            first, size = ((0, 128), (128, 64), (192, 64))[h]
            pv = jnp.dot(jnp.concatenate([vals[first:first + size], ones], axis=0), p, preferred_element_type=F32)
            some = slice(spans[h][0], spans[h][0] + size + 16)
            acc[xq, some, :] = acc[xq, some, :] * shrink + pv

    def both(zb):
        make_kaug(zb)
        tiles(zb, offsets(zb), False)

    relay(jnp.int32(1))
    for i in range(1, nx):
        src = lax.rem(x - i + nx, nx)
        remote(q_ref, qb.at[src], q_s.at[i - 1], q_r.at[i - 1], at(z, src, c, y)).wait_recv()
    for i in range(1, nz):
        slot = tt.at[zdn(i)]
        remote(slot, slot, t2_s.at[i - 1], t2_r.at[i - 1], at(zdn(i), x, c, y)).wait_recv()
    for j in range(2):
        pr_wait(z, j)
    make_kaug(z)
    tiles(z, offsets(z), True)

    def one_step(s, carry):
        @pl.when(s < half)
        def _():
            relay(s + 1)
        for j in range(2):
            pr_wait(zdn(s), j)

            @pl.when(s < half)
            def _():
                pr_wait(zup(s), j)

        def side(w, inner):
            zb = jnp.where(w == 0, zdn(s), zup(s))

            @pl.when(((w == 0) & (z >= s)) | ((w == 1) & (z + s >= nz) & (s < half)))
            def _():
                both(zb)
            return inner
        return lax.fori_loop(0, 2, side, carry)
    lax.fori_loop(1, half + 1, one_step, 0)

    def o_copies(i):
        dev = at(z, lax.rem(x + i, nx), c, y)
        return (
            remote(ob.at[i], orv.at[i], o_s.at[i, 0], o_r.at[i, 0], dev),
            remote(sb.at[i], srv.at[i], o_s.at[i, 1], o_r.at[i, 1], dev),
        )

    def last(k, carry):
        i = lax.rem(k + 1, nx)
        xq = lax.rem(x + i, nx)

        outs, lses = [], []
        for h in range(3):
            first, size = spans[h]
            total = acc[xq, pl.ds(first + size, 1), :]
            some = total > 0.0
            safe = jnp.where(some, total, 1.0)
            outs.append(acc[xq, pl.ds(first, size), :] / safe)
            lses.append(jnp.where(some, mb[xq, h] + jnp.log2(safe), NEG))
        ob[i] = jnp.concatenate(outs, axis=0).astype(BF16)
        place = lax.broadcasted_iota(jnp.int32, (8, 256), 0)
        sb[i] = jnp.where(place == 0, lses[0], jnp.where(place == 1, lses[1], lses[2]))

        @pl.when(i > 0)
        def _():
            for copy in o_copies(i):
                copy.start()
        return carry
    lax.fori_loop(0, nx, last, 0)

    for i in range(1, nx):
        src = lax.rem(x - i + nx, nx)
        for copy in o_copies(i):
            copy.wait_recv()
    stats = [sb[0]] + [srv[i] for i in range(1, nx)]
    outs = [ob[0]] + [orv[i] for i in range(1, nx)]
    top = functools.reduce(jnp.maximum, stats)
    shares = [jnp.exp2(t - top) for t in stats]
    whole = functools.reduce(jnp.add, shares)
    shares = [t / whole for t in shares]
    merged = [jnp.zeros((128, 256), F32), jnp.zeros((64, 256), F32), jnp.zeros((64, 256), F32)]
    for i in range(nx):
        for h, (first, size) in enumerate(((0, 128), (128, 64), (192, 64))):
            merged[h] = merged[h] + shares[i][h:h + 1] * outs[i][first:first + size].astype(F32)
    ab[...] = jnp.transpose(jnp.concatenate(merged, axis=0)).astype(BF16)

    share = 256 // ny

    def rows_of(y_):
        return ab.at[pl.ds(pl.multiple_of(y_ * share, share), share), :]

    def y_copy(i):
        other = lax.rem(y + i, ny)
        return remote(rows_of(other), ar.at[y], y_s.at[i - 1], y_r.at[i - 1], at(z, x, c, other))

    for i in range(1, ny):
        y_copy(i).start()
    for copy in weights[2:]:
        copy.start()
    ar[y] = ab[pl.ds(pl.multiple_of(y * share, share), share), :]
    for i in range(1, ny):
        src = lax.rem(y - i + ny, ny)
        remote(rows_of(src), ar.at[src], y_s.at[i - 1], y_r.at[i - 1], at(z, x, c, src)).wait_recv()

    for copy in fetch[:2]:
        copy.wait()
    a_wide = jnp.concatenate([ar[k, :, :128] for k in range(ny)], axis=1)
    a_narrow = jnp.concatenate([ar[k, :, 128:] for k in range(ny)], axis=1)
    mixed = jnp.dot(a_wide, ow[...], preferred_element_type=F32) + jnp.dot(a_narrow, on[...], preferred_element_type=F32)
    middle = (res_ref[...].astype(F32) + mixed).astype(BF16)
    mid[...] = middle
    middle = middle.astype(F32)
    spread = jnp.mean(middle * middle, axis=1, keepdims=True)
    normed = (middle * lax.rsqrt(spread + epsilon) * gain_ref[...]).astype(BF16)
    picker = jnp.where(chosen[0] | chosen[1], 1.0, 0.0).astype(BF16)
    perm[...] = lax.dot_general(picker, normed, (((0,), (0,)), ((), ())), preferred_element_type=F32)

    def cut(k, carry):
        v = perm[pl.ds(pl.multiple_of(8 * k, 8), 8), :]
        snd[2 * k] = v[:4].astype(BF16)
        snd[2 * k + 1] = v[4:].astype(BF16)
        return carry
    lax.fori_loop(0, count // 2, cut, 0)

    def to_plane(t):
        return lax.rem(z + far_first(t, nz) + nz, nz)

    def from_plane(t):
        return lax.rem(z - far_first(t, nz) + nz, nz)

    def out_copy(e):
        return remote(snd.at[e], arr.at[sp], a_s.at[e], a_r.at[sp], (e, y))

    def each_other(p, act):
        def one(k, carry):
            e = p * plane + k

            @pl.when(e != sp)
            def _():
                act(e)
            return carry
        lax.fori_loop(0, plane, one, 0)

    def send_rows(t, carry):
        each_other(to_plane(t), lambda e: out_copy(e).start())
        return carry
    lax.fori_loop(0, nz, send_rows, 0)
    keep = pltpu.make_async_copy(snd.at[sp], arr.at[sp], loc2.at[5])
    keep.start()
    keep.wait()

    def to_rows(take):
        for k in range(plane // 2):
            tmp[8 * k:8 * k + 8, :] = jnp.concatenate([take(2 * k).astype(F32), take(2 * k + 1).astype(F32)], axis=0)

    def rows_at(t):
        return pl.ds(pl.multiple_of(t * step, step), step)

    def cross_copy(p):
        some = pl.ds(p * plane, plane)
        return remote(arr.at[some], arc.at[some], c_s.at[p], c_r.at[p], across)

    def arrive_cross(t):
        p = from_plane(t)
        cross_copy(p).wait_recv()
        to_rows(lambda k: arc[p * plane + k])
        xs[rows_at(t), :] = tmp[...].astype(BF16)

    def arrive(t, carry):
        p = from_plane(t)
        each_other(p, lambda s: remote(snd.at[s], arr.at[s], a_s.at[s], a_r.at[s], (s, y)).wait_recv())
        cross_copy(p).start()
        to_rows(lambda k: arr[p * plane + k])
        xo[rows_at(t), :] = tmp[...].astype(BF16)

        @pl.when(t >= nz // 2)
        def _():
            arrive_cross(t - nz // 2)
        return carry
    lax.fori_loop(0, nz, arrive, 0)
    for copy in fetch[2:]:
        copy.wait()
    for copy in weights:
        copy.wait_recv()

    def hidden(x):
        both = []
        for k in range(2):
            g = jnp.dot(x, wg[k], preferred_element_type=F32)
            u = jnp.dot(x, wu[k], preferred_element_type=F32)
            both.append((jax.nn.silu(g) * u).astype(BF16))
        return both

    def down(h, put):
        width = 512
        for q in range(wd.shape[2] // width):
            cols = slice(q * width, (q + 1) * width)
            put(
                cols,
                jnp.dot(h[0], wd[0, :, cols], preferred_element_type=F32)
                + jnp.dot(h[1], wd[1, :, cols], preferred_element_type=F32),
            )

    def part_copy(t):
        some = rows_at(t)
        return remote(part.at[some, :], back.at[some, :], p_s.at[t], p_r.at[t], across)

    def send_part(t, carry):
        part_copy(t).start()
        return carry

    def cross_half(k):
        some = slice(k * step * nz // 2, (k + 1) * step * nz // 2)

        def put(cols, value):
            part[some, cols] = value.astype(BF16)
        down(hidden(xs[some, :]), put)
        lax.fori_loop(k * nz // 2, (k + 1) * nz // 2, send_part, 0)

    cross_half(0)

    def put_total(cols, value):
        total[:, cols] = value
    down(hidden(xo[...]), put_total)

    def late(t, carry):
        arrive_cross(t)
        return carry
    lax.fori_loop(nz // 2, nz, late, 0)
    cross_half(1)

    def back_copy(e):
        return remote(bsd.at[e], ret.at[sp], b_s.at[e], b_r.at[sp], (e, y))

    def finish(t, carry):
        p = from_plane(t)
        part_copy(t).wait_recv()
        some = rows_at(t)
        tmp[...] = total[some, :] + back[some, :].astype(F32)
        for k in range(plane // 2):
            v = tmp[8 * k:8 * k + 8, :]
            bsd[p * plane + 2 * k] = v[:4].astype(BF16)
            bsd[p * plane + 2 * k + 1] = v[4:].astype(BF16)
        each_other(p, lambda e: back_copy(e).start())
        return carry
    lax.fori_loop(0, nz, finish, 0)
    last = pltpu.make_async_copy(bsd.at[sp], ret.at[sp], loc2.at[6])
    last.start()
    last.wait()

    def returned(t, carry):
        p = to_plane(t)
        each_other(p, lambda e: remote(bsd.at[e], ret.at[e], b_s.at[e], b_r.at[e], (e, y)).wait_recv())
        to_rows(lambda k: ret[p * plane + k])
        rows[rows_at(p), :] = tmp[...].astype(BF16)
        return carry
    lax.fori_loop(0, nz, returned, 0)
    mix = jnp.where(chosen[0], weight_ref[:, 0:1], 0.0) + jnp.where(chosen[1], weight_ref[:, 1:2], 0.0)
    combined = mid[...].astype(F32)
    for _ in range(3):
        term = mix.astype(BF16)
        mix = mix - term.astype(F32)
        combined = combined + jnp.dot(term, rows[...], preferred_element_type=F32)
    out_ref[...] = combined.astype(BF16)

    for copy in weights:
        copy.wait_send()

    def drain(t, carry):
        each_other(t, lambda e: out_copy(e).wait_send())
        each_other(t, lambda e: back_copy(e).wait_send())
        cross_copy(t).wait_send()
        part_copy(t).wait_send()
        return carry
    lax.fori_loop(0, nz, drain, 0)
    for j in range(2):
        if up_has(1, j):
            own_up(j).wait_send()
        if dn_has(1, j):
            own_dn(j).wait_send()
        own_pr(j).wait_send()
        for s in range(1, half + 1):
            if up_has(s, j):
                if up_has(s + 1, j):
                    up_copy(s, j).wait_send()
                pr_copy(zdn(s), j).wait_send()
            if dn_has(s, j):
                if dn_has(s + 1, j):
                    dn_copy(s, j).wait_send()
                pr_copy(zup(s), j).wait_send()
    for i in range(1, 2 * nx):
        t1_copy(i).wait_send()
    for i in range(1, nz):
        t2_copy(i).wait_send()
    for i in range(1, nx):
        q_copy(i).wait_send()
        for copy in o_copies(i):
            copy.wait_send()
    for i in range(1, ny):
        y_copy(i).wait_send()


def layer(dims, arrays):
    nz, nx, ny = dims
    half, count = nz // 2, nz * nx * 2
    residual, wide, narrow, gate, up, down = (arrays[i] for i in (0, 9, 10, 14, 15, 16))
    features = residual.shape[1]
    dma = pltpu.SemaphoreType.DMA
    vmem = pl.BlockSpec(memory_space=pltpu.VMEM)
    hbm = pl.BlockSpec(memory_space=pl.ANY)
    blocks = pltpu.VMEM((count, 4, features), BF16)
    table = pltpu.VMEM((4 * count, features), BF16)
    square = pltpu.VMEM((256, 256), BF16)
    return pl.pallas_call(
        functools.partial(layer_kernel, dims),
        out_shape=jax.ShapeDtypeStruct(residual.shape, BF16),
        in_specs=[vmem] * 9 + [hbm] * 2 + [vmem] * 3 + [hbm] * 3,
        out_specs=vmem,
        scratch_shapes=[
            square,
            pltpu.VMEM((288, 256), BF16),
            square,
            pltpu.VMEM((1, 128), F32),
            pltpu.VMEM((nx, 256, 256), BF16),
            pltpu.VMEM((nz, 2, 288, 256), BF16),
            pltpu.VMEM((nz, 2, 256, 256), BF16),
            pltpu.VMEM((nz, 2 * nx, 1, 128), F32),
            pltpu.VMEM((512, 128), BF16),
            pltpu.VMEM((nx, 3, 1, 256), F32),
            pltpu.VMEM((nx, 304, 256), F32),
            pltpu.VMEM((nx, 256, 256), BF16),
            pltpu.VMEM((nx, 8, 256), F32),
            pltpu.VMEM((nx, 256, 256), BF16),
            pltpu.VMEM((nx, 8, 256), F32),
            square,
            pltpu.VMEM((ny, 256 // ny, 256), BF16),
            dma((nx,)), dma((nx,)),
            dma((half + 1, 2)), dma((half + 1, 2)), dma((half + 1, 2)), dma((half + 1, 2)),
            dma((nz, 2)), dma((nz, 2)),
            dma((2 * nx,)), dma((2 * nx,)), dma((nz,)), dma((nz,)),
            dma((nx, 2)), dma((nx, 2)), dma((ny,)), dma((ny,)), dma((4,)),
            pltpu.VMEM(wide.shape, BF16),
            pltpu.VMEM(narrow.shape, BF16),
            pltpu.VMEM((4 * count, features), F32),
            pltpu.VMEM((8 * nx, features), F32),
            blocks, blocks, blocks, table, table,
            pltpu.VMEM(residual.shape, BF16),
            pltpu.VMEM((2, *gate.shape), BF16),
            pltpu.VMEM((2, *up.shape), BF16),
            pltpu.VMEM((2, *down.shape), BF16),
            pltpu.VMEM((4 * count, features), F32),
            table, table, blocks, blocks, table,
            dma((count,)), dma((count,)), dma((nz,)), dma((nz,)), dma((nz,)), dma((nz,)),
            dma((count,)), dma((count,)), dma((4,)), dma((4,)), dma((7,)),
        ],
        compiler_params=pltpu.CompilerParams(collective_id=1, has_side_effects=True, vmem_limit_bytes=60 * 2**20),
        cost_estimate=pl.CostEstimate(flops=10**10, bytes_accessed=10**7, transcendentals=10**7),
        name="layer",
    )(*arrays)


def body(
    residual,
    query_wide,
    key_wide,
    value_wide,
    query_narrow,
    key_narrow,
    value_narrow,
    gate_wide,
    gate_narrow,
    out_wide,
    out_narrow,
    norm_gain,
    routing,
    route_weight,
    gate_weight,
    up_weight,
    down_weight,
):
    ny = lax.axis_size("tp")
    nx = NX
    dims = (lax.axis_size("sp") // (2 * nx), nx, ny)
    gate, up, down = gate_weight[0], up_weight[0], down_weight[0]
    return layer(
        dims,
        (
            residual, query_wide, key_wide, value_wide, query_narrow, key_narrow, value_narrow, gate_wide, gate_narrow,
            out_wide, out_narrow, norm_gain[None, :], routing, route_weight, gate, up, down,
        ),
    )


def solution(mesh):
    placed = (
        P(("sp", "tp"), None),
        P("sp", "tp"),
        P("sp", "tp"),
        P("sp", "tp"),
        P("sp", "tp"),
        P("sp", "tp"),
        P("sp", "tp"),
        P("sp", "tp"),
        P("sp", "tp"),
        P(),
        P(),
        P(),
        P(("sp", "tp"), None),
        P(("sp", "tp"), None),
        P("sp", None, "tp"),
        P("sp", None, "tp"),
        P("sp", "tp", None),
    )
    return jax.shard_map(
        body, mesh=mesh, in_specs=placed, out_specs=P(("sp", "tp"), None), check_vma=False
    )
```

```python
import functools
import math

import jax
import jax.numpy as jnp
from jax import lax
from jax.experimental import pallas as pl
from jax.experimental.pallas import tpu as pltpu
from jax.sharding import PartitionSpec as P

MESH = pl.DeviceIdType.MESH
F32, BF16 = jnp.float32, jnp.bfloat16
HW = 128
HN = 64
NX = 4
LOG2E = math.log2(math.e)
NEG = -1e30
LOWEST = -1e20
epsilon = 1e-06


def paired(y):
    return lax.rem(y, 2) * (y - 1) + (1 - lax.rem(y, 2)) * (y + 1)


def near_first(t, nz):
    m = (t + 1) // 2
    return jnp.where((lax.rem(t, 2) == 0) & (t > 0), -m, m)


def layer_kernel(
    dims, res_ref, qw_ref, kw_ref, vw_ref, qn_ref, kn_ref, vn_ref, gw_ref, gn_ref, wide_ref, narrow_ref, gain_ref,
    routing_ref, weight_ref, gate_ref, up_ref, down_ref, out_ref,
    q_ref, kd_ref, v_ref, tot_ref, qb, kb, vb, tt, kaug, mb, acc, ob, sb, orv, srv, ab, ar,
    q_s, q_r, up_s, up_r, dn_s, dn_r, pr_s, pr_r, t1_s, t1_r, t2_s, t2_r, o_s, o_r, y_s, y_r, loc,
    ow, on, perm, tmp, snd, arr, arc, xo, xs, mid, wg, wu, wd, total, part, back, bsd, ret, rows,
    a_s, a_r, c_s, c_r, p_s, p_r, b_s, b_r, w_s, w_r, loc2, vw_in, vn_in, qw_in, qn_in, res_in,
):
    nz, nx, ny = dims
    half = nz // 2
    plane = 2 * nx
    count = nz * plane
    step = 4 * plane
    sp, y = lax.axis_index("sp"), lax.axis_index("tp")
    early_in = [
        pltpu.make_async_copy(kw_ref, kd_ref.at[pl.ds(0, 256), pl.ds(0, 128)], loc2.at[7]),
        pltpu.make_async_copy(kn_ref, kd_ref.at[pl.ds(0, 256), pl.ds(128, 128)], loc2.at[8]),
        pltpu.make_async_copy(vw_ref, vw_in, loc2.at[9]),
        pltpu.make_async_copy(vn_ref, vn_in, loc2.at[10]),
        pltpu.make_async_copy(qw_ref, qw_in, loc2.at[11]),
        pltpu.make_async_copy(qn_ref, qn_in, loc2.at[12]),
    ]
    for copy in early_in:
        copy.start()
    fetch = [
        pltpu.make_async_copy(res_ref, res_in, loc2.at[13]),
        pltpu.make_async_copy(wide_ref, ow, loc2.at[0]),
        pltpu.make_async_copy(narrow_ref, on, loc2.at[1]),
        pltpu.make_async_copy(gate_ref, wg.at[0], loc2.at[2]),
        pltpu.make_async_copy(up_ref, wu.at[0], loc2.at[3]),
        pltpu.make_async_copy(down_ref, wd.at[0], loc2.at[4]),
    ]
    for copy in fetch:
        copy.start()
    c = lax.rem(sp, 2)
    x = lax.rem(sp // 2, nx)
    z = sp // (2 * nx)
    xc = x * 2 + c

    def at(z_, x_, c_, y_):
        return ((z_ * nx + x_) * 2 + c_, y_)

    def zup(i):
        return lax.rem(z + i, nz)

    def zdn(i):
        return lax.rem(z - i + nz, nz)

    def in_plane(i):
        other = lax.rem(xc + i, 2 * nx)
        return at(z, other // 2, lax.rem(other, 2), y)

    def remote(src, dst, send, recv, device):
        return pltpu.make_async_remote_copy(
            src_ref=src, dst_ref=dst, send_sem=send, recv_sem=recv, device_id=device, device_id_type=MESH
        )

    barrier = pltpu.get_barrier_semaphore()

    def greet(device):
        pl.semaphore_signal(barrier, inc=1, device_id=device, device_id_type=MESH)

    def greet_along(i, carry):
        greet((lax.rem(sp + i, count), y))
        return carry
    lax.fori_loop(1, count, greet_along, 0)
    for i in range(1, ny):
        greet((sp, lax.rem(y + i, ny)))
    lane = lax.broadcasted_iota(jnp.int32, (1, 128), 1)
    head = lax.broadcasted_iota(jnp.int32, (8, 1), 0)
    gates = jnp.where(head == 0, gw_ref[...], jnp.where(head == 1, gn_ref[0:1, :], gn_ref[1:2, :]))
    logs = jnp.minimum(gates, 0.0) - jnp.log1p(jnp.exp(-jnp.abs(gates)))
    until = lax.broadcasted_iota(jnp.int32, (256, 256), 0) <= lax.broadcasted_iota(jnp.int32, (256, 256), 1)
    until = jnp.where(until, 1.0, 0.0).astype(BF16)
    run = jnp.zeros((8, 256), F32)
    for _ in range(3):
        term = logs.astype(BF16)
        logs = logs - term.astype(F32)
        run = run + jnp.dot(term, until, preferred_element_type=F32)
    left = run * LOG2E
    ends = left[:, 255:256]
    tot_ref[...] = jnp.where(lane == 0, ends[0:1], jnp.where(lane == 1, ends[1:2], ends[2:3]))
    terms = []
    for _ in range(3):
        term = left.astype(BF16).astype(F32)
        left = left - term
        terms.append(term)
    kd_ref[256:288, :] = jnp.concatenate(terms + [jnp.zeros((8, 256), F32)], axis=0).astype(BF16)
    for copy in early_in:
        copy.wait()
    v_ref[0:128, :] = jnp.transpose(vw_in[...].astype(F32)).astype(BF16)
    v_ref[128:256, :] = jnp.transpose(vn_in[...].astype(F32)).astype(BF16)
    q_ref[0:128, :] = jnp.transpose(qw_in[...].astype(F32) * (HW ** -0.5 * LOG2E)).astype(BF16)
    q_ref[128:256, :] = jnp.transpose(qn_in[...].astype(F32) * (HN ** -0.5 * LOG2E)).astype(BF16)
    own_rows = routing_ref.shape[1]
    names = [routing_ref[k:k + 1, :].astype(F32) for k in range(2)]
    expert = lax.broadcasted_iota(jnp.int32, (count, own_rows), 0).astype(F32)
    hits = [jnp.where(name == expert, 1.0, 0.0) for name in names]
    earlier = lax.broadcasted_iota(jnp.int32, (own_rows, own_rows), 0) < lax.broadcasted_iota(
        jnp.int32, (own_rows, own_rows), 1
    )
    before = jnp.dot(
        (hits[0] + hits[1]).astype(BF16), jnp.where(earlier, 1.0, 0.0).astype(BF16), preferred_element_type=F32
    )
    slot = lax.broadcasted_iota(jnp.int32, (4 * count, own_rows), 0).astype(F32)
    chosen = [
        slot == names[k] * 4.0 + jnp.sum(before * hits[k], axis=0, keepdims=True) for k in range(2)
    ]
    pl.semaphore_wait(barrier, count - 1 + ny - 1)

    up_dev, dn_dev, pr_dev = at(zup(1), x, c, y), at(zdn(1), x, c, y), at(z, x, 1 - c, y)

    def up_copy(s, j):
        zb = zdn(s)
        src = (kb, vb)[j].at[zb, c]
        return remote(src, src, up_s.at[s, j], up_r.at[s, j], up_dev)

    def dn_copy(s, j):
        zb = zup(s)
        src = (kb, vb)[j].at[zb, c]
        return remote(src, src, dn_s.at[s, j], dn_r.at[s, j], dn_dev)

    def pr_copy(zb, j):
        src = (kb, vb)[j].at[zb, c]
        return remote(src, src, pr_s.at[zb, j], pr_r.at[zb, j], pr_dev)

    def pr_wait(zb, j):
        dst = (kb, vb)[j].at[zb, 1 - c]
        remote(dst, dst, pr_s.at[zb, j], pr_r.at[zb, j], pr_dev).wait_recv()

    def own_up(j):
        return remote((kd_ref, v_ref)[j], (kb, vb)[j].at[z, c], up_s.at[0, j], up_r.at[0, j], up_dev)

    def own_dn(j):
        return remote((kd_ref, v_ref)[j], (kb, vb)[j].at[z, c], dn_s.at[0, j], dn_r.at[0, j], dn_dev)

    def own_pr(j):
        return remote((kd_ref, v_ref)[j], (kb, vb)[j].at[z, c], pr_s.at[z, j], pr_r.at[z, j], pr_dev)

    def up_has(s, j):
        return s < half or (s == half and j == 0)

    def dn_has(s, j):
        return s < half or (s == half and j == 1)

    for j in range(2):
        if up_has(1, j):
            own_up(j).start()
        if dn_has(1, j):
            own_dn(j).start()

    def t1_copy(i):
        return remote(tot_ref, tt.at[z, xc], t1_s.at[i - 1], t1_r.at[i - 1], in_plane(i))

    def t2_copy(i):
        return remote(tt.at[z], tt.at[z], t2_s.at[i - 1], t2_r.at[i - 1], at(zup(i), x, c, y))

    def q_copy(i):
        return remote(q_ref, qb.at[x], q_s.at[i - 1], q_r.at[i - 1], at(z, lax.rem(x + i, nx), c, y))

    for i in range(1, 2 * nx):
        t1_copy(i).start()
    for i in range(1, nx):
        q_copy(i).start()
    for j in range(2):
        own_pr(j).start()
    pair, across = (sp, paired(y)), (sp, ny - 1 - y)
    cut_at = up_ref.shape[0] * 3 // 4
    early, rest = pl.ds(0, cut_at), pl.ds(cut_at, up_ref.shape[0] - cut_at)
    weights = [
        remote(gate_ref, wg.at[1], w_s.at[0], w_r.at[0], pair),
        remote(up_ref.at[early, :], wu.at[1, early, :], w_s.at[1], w_r.at[1], pair),
        remote(up_ref.at[rest, :], wu.at[1, rest, :], w_s.at[2], w_r.at[2], pair),
        remote(down_ref, wd.at[1], w_s.at[3], w_r.at[3], pair),
    ]
    for copy in weights[:2]:
        copy.start()
    local = [
        pltpu.make_async_copy(tot_ref, tt.at[z, xc], loc.at[0]),
        pltpu.make_async_copy(q_ref, qb.at[x], loc.at[1]),
        pltpu.make_async_copy(kd_ref, kb.at[z, c], loc.at[2]),
        pltpu.make_async_copy(v_ref, vb.at[z, c], loc.at[3]),
    ]
    for copy in local:
        copy.start()
    mb[...] = jnp.full(mb.shape, LOWEST, F32)
    acc[...] = jnp.zeros(acc.shape, F32)
    local[0].wait()
    for i in range(1, 2 * nx):
        other = lax.rem(xc - i + 2 * nx, 2 * nx)
        remote(tot_ref, tt.at[z, other], t1_s.at[i - 1], t1_r.at[i - 1], in_plane(i)).wait_recv()
    for i in range(1, nz):
        t2_copy(i).start()
    for copy in local[1:]:
        copy.wait()

    def relay(s):
        for j in range(2):
            @pl.when(s <= (half if j == 0 else half - 1))
            def _():
                slot = (kb, vb)[j].at[zdn(s), c]
                remote(slot, slot, up_s.at[s - 1, j], up_r.at[s - 1, j], up_dev).wait_recv()

                @pl.when(s + 1 <= (half if j == 0 else half - 1))
                def _():
                    up_copy(s, j).start()
                pr_copy(zdn(s), j).start()

            @pl.when(s <= (half if j == 1 else half - 1))
            def _():
                slot = (kb, vb)[j].at[zup(s), c]
                remote(slot, slot, dn_s.at[s - 1, j], dn_r.at[s - 1, j], dn_dev).wait_recv()

                @pl.when(s + 1 <= (half if j == 1 else half - 1))
                def _():
                    dn_copy(s, j).start()
                pr_copy(zup(s), j).start()

    low = lax.broadcasted_iota(jnp.int32, (128, 1), 0) < HN

    def head_offsets(zb):
        def plane(p, run):
            whole = jnp.zeros((1, 128), F32)
            for k in range(2 * nx):
                whole = whole + tt[p, k]
            return run + jnp.where(p < zb, whole, 0.0)
        run = lax.fori_loop(0, nz, plane, jnp.zeros((1, 128), F32))
        for k in range(2 * nx):
            run = run + jnp.where(k < 2 * x, tt[zb, k], 0.0)
        return run, run + tt[zb, 2 * x]

    def offsets(zb):
        return [
            [jnp.sum(jnp.where(lane == h, row, 0.0), axis=1, keepdims=True) for h in range(3)]
            for row in head_offsets(zb)
        ]

    def make_kaug(zb):
        for k in range(2):
            part = jnp.concatenate([kb[zb, k, 256:288, :].astype(F32), jnp.zeros((96, 256), F32)], axis=0)
            kaug[256 * k:256 * k + 256, :] = jnp.transpose(part).astype(BF16)

    spans = ((0, 128), (144, 64), (224, 64))
    row_of = lax.broadcasted_iota(jnp.int32, (128, 256), 0)
    minus = [jnp.where((lax.rem(row_of, 8) == h) & (row_of < 24), -1.0, 0.0).astype(BF16) for h in range(3)]

    def tiles(zb, offs, masked):
        keys = jnp.concatenate([kb[zb, 0, 0:256, :], kb[zb, 1, 0:256, :]], axis=0)
        vals = jnp.concatenate([vb[zb, 0], vb[zb, 1]], axis=1)
        more = kaug[...]
        ones = jnp.ones((16, 512), BF16)
        work = [(xq, h) for xq in range(nx) for h in range(3)]
        scores, weights_, shrinks = [], [], []
        for xq, h in work:
            side = slice(0, 128) if h == 0 else slice(128, 256)
            q = qb[xq, side, :]
            if h > 0:
                q = jnp.where(low if h == 1 else jnp.logical_not(low), q, jnp.zeros_like(q))
            scores.append(
                jnp.dot(
                    jnp.concatenate([keys[:, side], more], axis=1),
                    jnp.concatenate([q, minus[h]], axis=0),
                    preferred_element_type=F32,
                )
            )
        for (xq, h), r in zip(work, scores):
            if masked:
                places = lax.broadcasted_iota(jnp.int32, (512, 256), 0) + x * 512
                wanted = lax.broadcasted_iota(jnp.int32, (512, 256), 1) + (xq * 512 + c * 256)
                r = jnp.where(places <= wanted, r, NEG)
            old = mb[xq, h]
            new = old
            for k in range(2):
                new = jnp.maximum(new, jnp.max(r[256 * k:256 * k + 256], axis=0, keepdims=True) - offs[k][h])
            weights_.append(
                jnp.concatenate(
                    [jnp.exp2(r[256 * k:256 * k + 256] - (new + offs[k][h])).astype(BF16) for k in range(2)], axis=0
                )
            )
            shrinks.append(jnp.exp2(old - new))
            mb[xq, h] = new
        for (xq, h), p, shrink in zip(work, weights_, shrinks):
            first, size = ((0, 128), (128, 64), (192, 64))[h]
            pv = jnp.dot(jnp.concatenate([vals[first:first + size], ones], axis=0), p, preferred_element_type=F32)
            some = slice(spans[h][0], spans[h][0] + size + 16)
            acc[xq, some, :] = acc[xq, some, :] * shrink + pv

    def both(zb):
        make_kaug(zb)
        tiles(zb, offsets(zb), False)

    relay(jnp.int32(1))
    for i in range(1, nx):
        src = lax.rem(x - i + nx, nx)
        remote(q_ref, qb.at[src], q_s.at[i - 1], q_r.at[i - 1], at(z, src, c, y)).wait_recv()
    for i in range(1, nz):
        slot = tt.at[zdn(i)]
        remote(slot, slot, t2_s.at[i - 1], t2_r.at[i - 1], at(zdn(i), x, c, y)).wait_recv()
    for j in range(2):
        pr_wait(z, j)
    make_kaug(z)
    tiles(z, offsets(z), True)

    def one_step(s, carry):
        @pl.when(s < half)
        def _():
            relay(s + 1)
        for j in range(2):
            pr_wait(zdn(s), j)

            @pl.when(s < half)
            def _():
                pr_wait(zup(s), j)

        def side(w, inner):
            zb = jnp.where(w == 0, zdn(s), zup(s))

            @pl.when(((w == 0) & (z >= s)) | ((w == 1) & (z + s >= nz) & (s < half)))
            def _():
                both(zb)
            return inner
        return lax.fori_loop(0, 2, side, carry)
    lax.fori_loop(1, half + 1, one_step, 0)

    def o_copies(i):
        dev = at(z, lax.rem(x + i, nx), c, y)
        return (
            remote(ob.at[i], orv.at[i], o_s.at[i, 0], o_r.at[i, 0], dev),
            remote(sb.at[i], srv.at[i], o_s.at[i, 1], o_r.at[i, 1], dev),
        )

    def last(k, carry):
        i = lax.rem(k + 1, nx)
        xq = lax.rem(x + i, nx)

        outs, lses = [], []
        for h in range(3):
            first, size = spans[h]
            total = acc[xq, pl.ds(first + size, 1), :]
            some = total > 0.0
            safe = jnp.where(some, total, 1.0)
            outs.append(acc[xq, pl.ds(first, size), :] / safe)
            lses.append(jnp.where(some, mb[xq, h] + jnp.log2(safe), NEG))
        ob[i] = jnp.concatenate(outs, axis=0).astype(BF16)
        place = lax.broadcasted_iota(jnp.int32, (8, 256), 0)
        sb[i] = jnp.where(place == 0, lses[0], jnp.where(place == 1, lses[1], lses[2]))

        @pl.when(i > 0)
        def _():
            for copy in o_copies(i):
                copy.start()
        return carry
    lax.fori_loop(0, nx, last, 0)

    for i in range(1, nx):
        src = lax.rem(x - i + nx, nx)
        for copy in o_copies(i):
            copy.wait_recv()
    stats = [sb[0]] + [srv[i] for i in range(1, nx)]
    outs = [ob[0]] + [orv[i] for i in range(1, nx)]
    top = functools.reduce(jnp.maximum, stats)
    shares = [jnp.exp2(t - top) for t in stats]
    whole = functools.reduce(jnp.add, shares)
    shares = [t / whole for t in shares]
    merged = [jnp.zeros((128, 256), F32), jnp.zeros((64, 256), F32), jnp.zeros((64, 256), F32)]
    for i in range(nx):
        for h, (first, size) in enumerate(((0, 128), (128, 64), (192, 64))):
            merged[h] = merged[h] + shares[i][h:h + 1] * outs[i][first:first + size].astype(F32)
    ab[...] = jnp.transpose(jnp.concatenate(merged, axis=0)).astype(BF16)

    share = 256 // ny

    def rows_of(y_):
        return ab.at[pl.ds(pl.multiple_of(y_ * share, share), share), :]

    def y_copy(i):
        other = lax.rem(y + i, ny)
        return remote(rows_of(other), ar.at[y], y_s.at[i - 1], y_r.at[i - 1], at(z, x, c, other))

    for i in range(1, ny):
        y_copy(i).start()
    for copy in weights[2:]:
        copy.start()
    ar[y] = ab[pl.ds(pl.multiple_of(y * share, share), share), :]
    for i in range(1, ny):
        src = lax.rem(y - i + ny, ny)
        remote(rows_of(src), ar.at[src], y_s.at[i - 1], y_r.at[i - 1], at(z, x, c, src)).wait_recv()

    for copy in fetch[:3]:
        copy.wait()
    a_wide = jnp.concatenate([ar[k, :, :128] for k in range(ny)], axis=1)
    a_narrow = jnp.concatenate([ar[k, :, 128:] for k in range(ny)], axis=1)
    mixed = jnp.dot(a_wide, ow[...], preferred_element_type=F32) + jnp.dot(a_narrow, on[...], preferred_element_type=F32)
    middle = (res_in[...].astype(F32) + mixed).astype(BF16)
    mid[...] = middle
    middle = middle.astype(F32)
    spread = jnp.mean(middle * middle, axis=1, keepdims=True)
    normed = (middle * lax.rsqrt(spread + epsilon) * gain_ref[...]).astype(BF16)
    picker = jnp.where(chosen[0] | chosen[1], 1.0, 0.0).astype(BF16)
    perm[...] = jnp.dot(picker, normed, preferred_element_type=F32)

    def cut(k, carry):
        v = perm[pl.ds(pl.multiple_of(8 * k, 8), 8), :]
        snd[2 * k] = v[:4].astype(BF16)
        snd[2 * k + 1] = v[4:].astype(BF16)
        return carry
    lax.fori_loop(0, count // 2, cut, 0)

    def to_plane(t):
        return lax.rem(z + near_first(t, nz) + nz, nz)

    def from_plane(t):
        return lax.rem(z - near_first(t, nz) + nz, nz)

    def out_copy(e):
        return remote(snd.at[e], arr.at[sp], a_s.at[e], a_r.at[sp], (e, y))

    def each_other(p, act):
        def one(k, carry):
            e = p * plane + k

            @pl.when(e != sp)
            def _():
                act(e)
            return carry
        lax.fori_loop(0, plane, one, 0)

    def send_rows(t, carry):
        each_other(to_plane(t), lambda e: out_copy(e).start())
        return carry
    lax.fori_loop(0, nz, send_rows, 0)
    keep = pltpu.make_async_copy(snd.at[sp], arr.at[sp], loc2.at[5])
    keep.start()
    keep.wait()

    def to_rows(take):
        for k in range(plane // 2):
            tmp[8 * k:8 * k + 8, :] = jnp.concatenate([take(2 * k).astype(F32), take(2 * k + 1).astype(F32)], axis=0)

    def rows_at(t):
        return pl.ds(pl.multiple_of(t * step, step), step)

    def cross_copy(p):
        some = pl.ds(p * plane, plane)
        return remote(arr.at[some], arc.at[some], c_s.at[p], c_r.at[p], across)

    def arrive_cross(t):
        p = from_plane(t)
        cross_copy(p).wait_recv()
        to_rows(lambda k: arc[p * plane + k])
        xs[rows_at(t), :] = tmp[...].astype(BF16)

    def arrive(t, carry):
        p = from_plane(t)
        each_other(p, lambda s: remote(snd.at[s], arr.at[s], a_s.at[s], a_r.at[s], (s, y)).wait_recv())
        cross_copy(p).start()
        to_rows(lambda k: arr[p * plane + k])
        xo[rows_at(t), :] = tmp[...].astype(BF16)

        @pl.when(t >= nz // 2)
        def _():
            arrive_cross(t - nz // 2)
        return carry
    lax.fori_loop(0, nz, arrive, 0)
    for copy in fetch[3:]:
        copy.wait()
    for copy in weights:
        copy.wait_recv()

    def hidden(x):
        both = []
        for k in range(2):
            g = jnp.dot(x, wg[k], preferred_element_type=F32)
            u = jnp.dot(x, wu[k], preferred_element_type=F32)
            both.append((jax.nn.silu(g) * u).astype(BF16))
        return both

    def down(h, put):
        width = 512
        for q in range(wd.shape[2] // width):
            cols = slice(q * width, (q + 1) * width)
            put(
                cols,
                jnp.dot(h[0], wd[0, :, cols], preferred_element_type=F32)
                + jnp.dot(h[1], wd[1, :, cols], preferred_element_type=F32),
            )

    def part_copy(t):
        some = rows_at(t)
        return remote(part.at[some, :], back.at[some, :], p_s.at[t], p_r.at[t], across)

    def send_part(t, carry):
        part_copy(nz - 1 - t).start()
        return carry

    def cross_half(k):
        some = slice(k * step * nz // 2, (k + 1) * step * nz // 2)

        def put(cols, value):
            part[some, cols] = value.astype(BF16)
        down(hidden(xs[some, :]), put)

    def put_total(cols, value):
        total[:, cols] = value
    down(hidden(xo[...]), put_total)
    cross_half(0)

    def late(t, carry):
        arrive_cross(t)
        return carry
    lax.fori_loop(nz // 2, nz, late, 0)
    cross_half(1)
    lax.fori_loop(0, nz, send_part, 0)

    def back_copy(e):
        return remote(bsd.at[e], ret.at[sp], b_s.at[e], b_r.at[sp], (e, y))

    for copy in weights:
        copy.wait_send()

    def drain_rows(t, carry):
        each_other(t, lambda e: out_copy(e).wait_send())
        cross_copy(t).wait_send()
        return carry
    lax.fori_loop(0, nz, drain_rows, 0)
    for j in range(2):
        if up_has(1, j):
            own_up(j).wait_send()
        if dn_has(1, j):
            own_dn(j).wait_send()
        own_pr(j).wait_send()
        for s in range(1, half + 1):
            if up_has(s, j):
                if up_has(s + 1, j):
                    up_copy(s, j).wait_send()
                pr_copy(zdn(s), j).wait_send()
            if dn_has(s, j):
                if dn_has(s + 1, j):
                    dn_copy(s, j).wait_send()
                pr_copy(zup(s), j).wait_send()
    for i in range(1, 2 * nx):
        t1_copy(i).wait_send()
    for i in range(1, nz):
        t2_copy(i).wait_send()
    for i in range(1, nx):
        q_copy(i).wait_send()
        for copy in o_copies(i):
            copy.wait_send()
    for i in range(1, ny):
        y_copy(i).wait_send()

    def finish(u, carry):
        t = nz - 1 - u
        p = from_plane(t)
        part_copy(t).wait_recv()
        some = rows_at(t)
        tmp[...] = total[some, :] + back[some, :].astype(F32)
        for k in range(plane // 2):
            v = tmp[8 * k:8 * k + 8, :]
            bsd[p * plane + 2 * k] = v[:4].astype(BF16)
            bsd[p * plane + 2 * k + 1] = v[4:].astype(BF16)
        each_other(p, lambda e: back_copy(e).start())
        return carry
    lax.fori_loop(0, nz, finish, 0)
    last = pltpu.make_async_copy(bsd.at[sp], ret.at[sp], loc2.at[6])
    last.start()
    last.wait()

    def returned(u, carry):
        p = to_plane(nz - 1 - u)
        each_other(p, lambda e: remote(bsd.at[e], ret.at[e], b_s.at[e], b_r.at[e], (e, y)).wait_recv())
        to_rows(lambda k: ret[p * plane + k])
        rows[rows_at(p), :] = tmp[...].astype(BF16)
        return carry
    lax.fori_loop(0, nz, returned, 0)
    mix = jnp.where(chosen[0], weight_ref[0:1, :], 0.0) + jnp.where(chosen[1], weight_ref[1:2, :], 0.0)
    combined = mid[...].astype(F32)
    for _ in range(3):
        term = mix.astype(BF16)
        mix = mix - term.astype(F32)
        combined = combined + lax.dot_general(
            term, rows[...], (((0,), (0,)), ((), ())), preferred_element_type=F32
        )
    out_ref[...] = combined.astype(BF16)

    def drain(t, carry):
        each_other(t, lambda e: back_copy(e).wait_send())
        part_copy(t).wait_send()
        return carry
    lax.fori_loop(0, nz, drain, 0)


def layer(dims, arrays):
    nz, nx, ny = dims
    half, count = nz // 2, nz * nx * 2
    residual, wide, narrow, gate, up, down = (arrays[i] for i in (0, 9, 10, 14, 15, 16))
    features = residual.shape[1]
    dma = pltpu.SemaphoreType.DMA
    vmem = pl.BlockSpec(memory_space=pltpu.VMEM)
    hbm = pl.BlockSpec(memory_space=pl.ANY)
    blocks = pltpu.VMEM((count, 4, features), BF16)
    table = pltpu.VMEM((4 * count, features), BF16)
    square = pltpu.VMEM((256, 256), BF16)
    return pl.pallas_call(
        functools.partial(layer_kernel, dims),
        out_shape=jax.ShapeDtypeStruct(residual.shape, BF16),
        in_specs=[hbm] * 7 + [vmem] * 2 + [hbm] * 2 + [vmem] * 3 + [hbm] * 3,
        out_specs=vmem,
        scratch_shapes=[
            square,
            pltpu.VMEM((288, 256), BF16),
            square,
            pltpu.VMEM((1, 128), F32),
            pltpu.VMEM((nx, 256, 256), BF16),
            pltpu.VMEM((nz, 2, 288, 256), BF16),
            pltpu.VMEM((nz, 2, 256, 256), BF16),
            pltpu.VMEM((nz, 2 * nx, 1, 128), F32),
            pltpu.VMEM((512, 128), BF16),
            pltpu.VMEM((nx, 3, 1, 256), F32),
            pltpu.VMEM((nx, 304, 256), F32),
            pltpu.VMEM((nx, 256, 256), BF16),
            pltpu.VMEM((nx, 8, 256), F32),
            pltpu.VMEM((nx, 256, 256), BF16),
            pltpu.VMEM((nx, 8, 256), F32),
            square,
            pltpu.VMEM((ny, 256 // ny, 256), BF16),
            dma((nx,)), dma((nx,)),
            dma((half + 1, 2)), dma((half + 1, 2)), dma((half + 1, 2)), dma((half + 1, 2)),
            dma((nz, 2)), dma((nz, 2)),
            dma((2 * nx,)), dma((2 * nx,)), dma((nz,)), dma((nz,)),
            dma((nx, 2)), dma((nx, 2)), dma((ny,)), dma((ny,)), dma((4,)),
            pltpu.VMEM(wide.shape, BF16),
            pltpu.VMEM(narrow.shape, BF16),
            pltpu.VMEM((4 * count, features), F32),
            pltpu.VMEM((8 * nx, features), F32),
            blocks, blocks, blocks, table, table,
            pltpu.VMEM(residual.shape, BF16),
            pltpu.VMEM((2, *gate.shape), BF16),
            pltpu.VMEM((2, *up.shape), BF16),
            pltpu.VMEM((2, *down.shape), BF16),
            pltpu.VMEM((4 * count, features), F32),
            table, table, blocks, blocks, table,
            dma((count,)), dma((count,)), dma((nz,)), dma((nz,)), dma((nz,)), dma((nz,)),
            dma((count,)), dma((count,)), dma((4,)), dma((4,)), dma((14,)),
            pltpu.VMEM((256, 128), BF16), pltpu.VMEM((256, 128), BF16), pltpu.VMEM((256, 128), BF16), pltpu.VMEM((256, 128), BF16),
            pltpu.VMEM(residual.shape, BF16),
        ],
        compiler_params=pltpu.CompilerParams(collective_id=1, has_side_effects=True, vmem_limit_bytes=60 * 2**20),
        cost_estimate=pl.CostEstimate(flops=10**10, bytes_accessed=10**7, transcendentals=10**7),
        name="layer",
    )(*arrays)


def body(
    residual,
    query_wide,
    key_wide,
    value_wide,
    query_narrow,
    key_narrow,
    value_narrow,
    gate_wide,
    gate_narrow,
    out_wide,
    out_narrow,
    norm_gain,
    routing,
    route_weight,
    gate_weight,
    up_weight,
    down_weight,
):
    ny = lax.axis_size("tp")
    nx = NX
    dims = (lax.axis_size("sp") // (2 * nx), nx, ny)
    gate, up, down = gate_weight[0], up_weight[0], down_weight[0]
    return layer(
        dims,
        (
            residual, query_wide, key_wide, value_wide, query_narrow, key_narrow, value_narrow, gate_wide.T, gate_narrow.T,
            out_wide, out_narrow, norm_gain[None, :], routing.T, route_weight.T, gate, up, down,
        ),
    )


def solution(mesh):
    placed = (
        P(("sp", "tp"), None),
        P("sp", "tp"),
        P("sp", "tp"),
        P("sp", "tp"),
        P("sp", "tp"),
        P("sp", "tp"),
        P("sp", "tp"),
        P("sp", "tp"),
        P("sp", "tp"),
        P(),
        P(),
        P(),
        P(("sp", "tp"), None),
        P(("sp", "tp"), None),
        P("sp", None, "tp"),
        P("sp", None, "tp"),
        P("sp", "tp", None),
    )
    return jax.shard_map(
        body, mesh=mesh, in_specs=placed, out_specs=P(("sp", "tp"), None), check_vma=False
    )
```

```python
import functools
import math

import jax
import jax.numpy as jnp
from jax import lax
from jax.experimental import pallas as pl
from jax.experimental.pallas import tpu as pltpu
from jax.sharding import PartitionSpec as P

MESH = pl.DeviceIdType.MESH
F32, BF16 = jnp.float32, jnp.bfloat16
HW = 128
HN = 64
NX = 4
LOG2E = math.log2(math.e)
NEG = -1e30
LOWEST = -1e20
epsilon = 1e-06


def paired(y):
    return lax.rem(y, 2) * (y - 1) + (1 - lax.rem(y, 2)) * (y + 1)


def near_first(t, nz):
    near = nz // 4 * 2
    u = t - jnp.where(t > near, 1, 0)
    m = u // 2 + 1
    return jnp.where(t == near, 0, jnp.where(lax.rem(u, 2) == 0, m, -m))


def return_order(nz):
    if nz == 8:
        return (2, 3, 7, 6, 5, 0, 1, 4), 2
    return tuple(range(nz - 1, -1, -1)), 0


def entry(table, u):
    value = 0
    for i, v in enumerate(table):
        value = jnp.where(u == i, v, value)
    return value


def layer_kernel(
    dims, res_ref, qw_ref, kw_ref, vw_ref, qn_ref, kn_ref, vn_ref, gw_ref, gn_ref, wide_ref, narrow_ref, gain_ref,
    routing_ref, weight_ref, gate_ref, up_ref, down_ref, out_ref,
    q_ref, kd_ref, v_ref, tot_ref, qb, kb, vb, tt, kaug, mb, acc, ob, sb, orv, srv, ab, ar,
    q_s, q_r, up_s, up_r, dn_s, dn_r, pr_s, pr_r, t1_s, t1_r, t2_s, t2_r, o_s, o_r, y_s, y_r, loc,
    ow, on, perm, tmp, snd, arr, arc, xo, xs, mid, wg, wu, wd, total, part, back, bsd, ret, rows,
    a_s, a_r, c_s, c_r, p_s, p_r, b_s, b_r, w_s, w_r, loc2, vw_in, vn_in, qw_in, qn_in, res_in,
):
    nz, nx, ny = dims
    half = nz // 2
    plane = 2 * nx
    count = nz * plane
    step = 4 * plane
    sp, y = lax.axis_index("sp"), lax.axis_index("tp")
    early_in = [
        pltpu.make_async_copy(kw_ref, kd_ref.at[pl.ds(0, 256), pl.ds(0, 128)], loc2.at[7]),
        pltpu.make_async_copy(kn_ref, kd_ref.at[pl.ds(0, 256), pl.ds(128, 128)], loc2.at[8]),
        pltpu.make_async_copy(vw_ref, vw_in, loc2.at[9]),
        pltpu.make_async_copy(vn_ref, vn_in, loc2.at[10]),
        pltpu.make_async_copy(qw_ref, qw_in, loc2.at[11]),
        pltpu.make_async_copy(qn_ref, qn_in, loc2.at[12]),
    ]
    for copy in early_in:
        copy.start()
    fetch = [
        pltpu.make_async_copy(res_ref, res_in, loc2.at[13]),
        pltpu.make_async_copy(wide_ref, ow, loc2.at[0]),
        pltpu.make_async_copy(narrow_ref, on, loc2.at[1]),
        pltpu.make_async_copy(gate_ref, wg.at[0], loc2.at[2]),
        pltpu.make_async_copy(up_ref, wu.at[0], loc2.at[3]),
        pltpu.make_async_copy(down_ref, wd.at[0], loc2.at[4]),
    ]
    for copy in fetch:
        copy.start()
    c = lax.rem(sp, 2)
    x = lax.rem(sp // 2, nx)
    z = sp // (2 * nx)
    xc = x * 2 + c

    def at(z_, x_, c_, y_):
        return ((z_ * nx + x_) * 2 + c_, y_)

    def zup(i):
        return lax.rem(z + i, nz)

    def zdn(i):
        return lax.rem(z - i + nz, nz)

    def in_plane(i):
        other = lax.rem(xc + i, 2 * nx)
        return at(z, other // 2, lax.rem(other, 2), y)

    def remote(src, dst, send, recv, device):
        return pltpu.make_async_remote_copy(
            src_ref=src, dst_ref=dst, send_sem=send, recv_sem=recv, device_id=device, device_id_type=MESH
        )

    barrier = pltpu.get_barrier_semaphore()

    def greet(device):
        pl.semaphore_signal(barrier, inc=1, device_id=device, device_id_type=MESH)

    def greet_along(i, carry):
        greet((lax.rem(sp + i, count), y))
        return carry
    lax.fori_loop(1, count, greet_along, 0)
    for i in range(1, ny):
        greet((sp, lax.rem(y + i, ny)))
    lane = lax.broadcasted_iota(jnp.int32, (1, 128), 1)
    head = lax.broadcasted_iota(jnp.int32, (8, 1), 0)
    gates = jnp.where(head == 0, gw_ref[...], jnp.where(head == 1, gn_ref[0:1, :], gn_ref[1:2, :]))
    logs = jnp.minimum(gates, 0.0) - jnp.log1p(jnp.exp(-jnp.abs(gates)))
    until = lax.broadcasted_iota(jnp.int32, (256, 256), 0) <= lax.broadcasted_iota(jnp.int32, (256, 256), 1)
    until = jnp.where(until, 1.0, 0.0).astype(BF16)
    run = jnp.zeros((8, 256), F32)
    for _ in range(3):
        term = logs.astype(BF16)
        logs = logs - term.astype(F32)
        run = run + jnp.dot(term, until, preferred_element_type=F32)
    left = run * LOG2E
    ends = left[:, 255:256]
    tot_ref[...] = jnp.where(lane == 0, ends[0:1], jnp.where(lane == 1, ends[1:2], ends[2:3]))
    terms = []
    for _ in range(3):
        term = left.astype(BF16).astype(F32)
        left = left - term
        terms.append(term)
    extra = lax.broadcasted_iota(jnp.int32, (16, 1), 0)
    placed = jnp.zeros((16, 256), F32)
    for i in range(3):
        for h in range(3):
            placed = jnp.where(extra == 3 * i + h, terms[i][h:h + 1], placed)
    kd_ref[256:272, :] = placed.astype(BF16)
    for copy in early_in:
        copy.wait()
    v_ref[0:128, :] = jnp.transpose(vw_in[...].astype(F32)).astype(BF16)
    v_ref[128:256, :] = jnp.transpose(vn_in[...].astype(F32)).astype(BF16)
    q_ref[0:128, :] = jnp.transpose(qw_in[...].astype(F32) * (HW ** -0.5 * LOG2E)).astype(BF16)
    q_ref[128:256, :] = jnp.transpose(qn_in[...].astype(F32) * (HN ** -0.5 * LOG2E)).astype(BF16)
    own_rows = routing_ref.shape[1]
    names = [routing_ref[k:k + 1, :].astype(F32) for k in range(2)]
    expert = lax.broadcasted_iota(jnp.int32, (count, own_rows), 0).astype(F32)
    hits = [jnp.where(name == expert, 1.0, 0.0) for name in names]
    earlier = lax.broadcasted_iota(jnp.int32, (own_rows, own_rows), 0) < lax.broadcasted_iota(
        jnp.int32, (own_rows, own_rows), 1
    )
    before = jnp.dot(
        (hits[0] + hits[1]).astype(BF16), jnp.where(earlier, 1.0, 0.0).astype(BF16), preferred_element_type=F32
    )
    slot = lax.broadcasted_iota(jnp.int32, (4 * count, own_rows), 0).astype(F32)
    chosen = [
        slot == names[k] * 4.0 + jnp.sum(before * hits[k], axis=0, keepdims=True) for k in range(2)
    ]
    pl.semaphore_wait(barrier, count - 1 + ny - 1)

    up_dev, dn_dev, pr_dev = at(zup(1), x, c, y), at(zdn(1), x, c, y), at(z, x, 1 - c, y)

    def up_copy(s, j):
        zb = zdn(s)
        src = (kb, vb)[j].at[zb, c]
        return remote(src, src, up_s.at[s, j], up_r.at[s, j], up_dev)

    def dn_copy(s, j):
        zb = zup(s)
        src = (kb, vb)[j].at[zb, c]
        return remote(src, src, dn_s.at[s, j], dn_r.at[s, j], dn_dev)

    def pr_copy(zb, j):
        src = (kb, vb)[j].at[zb, c]
        return remote(src, src, pr_s.at[zb, j], pr_r.at[zb, j], pr_dev)

    def pr_wait(zb, j):
        dst = (kb, vb)[j].at[zb, 1 - c]
        remote(dst, dst, pr_s.at[zb, j], pr_r.at[zb, j], pr_dev).wait_recv()

    def own_up(j):
        return remote((kd_ref, v_ref)[j], (kb, vb)[j].at[z, c], up_s.at[0, j], up_r.at[0, j], up_dev)

    def own_dn(j):
        return remote((kd_ref, v_ref)[j], (kb, vb)[j].at[z, c], dn_s.at[0, j], dn_r.at[0, j], dn_dev)

    def own_pr(j):
        return remote((kd_ref, v_ref)[j], (kb, vb)[j].at[z, c], pr_s.at[z, j], pr_r.at[z, j], pr_dev)

    def up_has(s, j):
        return s < half or (s == half and j == 0)

    def dn_has(s, j):
        return s < half or (s == half and j == 1)

    for j in range(2):
        if up_has(1, j):
            own_up(j).start()
        if dn_has(1, j):
            own_dn(j).start()

    def t1_copy(i):
        return remote(tot_ref, tt.at[z, xc], t1_s.at[i - 1], t1_r.at[i - 1], in_plane(i))

    def t2_copy(i):
        return remote(tt.at[z], tt.at[z], t2_s.at[i - 1], t2_r.at[i - 1], at(zup(i), x, c, y))

    def q_copy(i):
        return remote(q_ref, qb.at[x], q_s.at[i - 1], q_r.at[i - 1], at(z, lax.rem(x + i, nx), c, y))

    for i in range(1, 2 * nx):
        t1_copy(i).start()
    for i in range(1, nx):
        q_copy(i).start()
    for j in range(2):
        own_pr(j).start()
    pair, across = (sp, paired(y)), (sp, ny - 1 - y)
    cut_at = up_ref.shape[0] * 3 // 4
    early, rest = pl.ds(0, cut_at), pl.ds(cut_at, up_ref.shape[0] - cut_at)
    weights = [
        remote(gate_ref, wg.at[1], w_s.at[0], w_r.at[0], pair),
        remote(up_ref.at[early, :], wu.at[1, early, :], w_s.at[1], w_r.at[1], pair),
        remote(up_ref.at[rest, :], wu.at[1, rest, :], w_s.at[2], w_r.at[2], pair),
        remote(down_ref, wd.at[1], w_s.at[3], w_r.at[3], pair),
    ]
    for copy in weights[:2]:
        copy.start()
    local = [
        pltpu.make_async_copy(tot_ref, tt.at[z, xc], loc.at[0]),
        pltpu.make_async_copy(q_ref, qb.at[x], loc.at[1]),
        pltpu.make_async_copy(kd_ref, kb.at[z, c], loc.at[2]),
        pltpu.make_async_copy(v_ref, vb.at[z, c], loc.at[3]),
    ]
    for copy in local:
        copy.start()
    mb[...] = jnp.full(mb.shape, LOWEST, F32)
    acc[...] = jnp.zeros(acc.shape, F32)
    local[0].wait()
    for i in range(1, 2 * nx):
        other = lax.rem(xc - i + 2 * nx, 2 * nx)
        remote(tot_ref, tt.at[z, other], t1_s.at[i - 1], t1_r.at[i - 1], in_plane(i)).wait_recv()
    for i in range(1, nz):
        t2_copy(i).start()
    for copy in local[1:]:
        copy.wait()

    def relay(s):
        for j in range(2):
            @pl.when(s <= (half if j == 0 else half - 1))
            def _():
                slot = (kb, vb)[j].at[zdn(s), c]
                remote(slot, slot, up_s.at[s - 1, j], up_r.at[s - 1, j], up_dev).wait_recv()

                @pl.when(s + 1 <= (half if j == 0 else half - 1))
                def _():
                    up_copy(s, j).start()
                pr_copy(zdn(s), j).start()

            @pl.when(s <= (half if j == 1 else half - 1))
            def _():
                slot = (kb, vb)[j].at[zup(s), c]
                remote(slot, slot, dn_s.at[s - 1, j], dn_r.at[s - 1, j], dn_dev).wait_recv()

                @pl.when(s + 1 <= (half if j == 1 else half - 1))
                def _():
                    dn_copy(s, j).start()
                pr_copy(zup(s), j).start()

    low = lax.broadcasted_iota(jnp.int32, (128, 1), 0) < HN

    def head_offsets(zb):
        def plane(p, run):
            whole = jnp.zeros((1, 128), F32)
            for k in range(2 * nx):
                whole = whole + tt[p, k]
            return run + jnp.where(p < zb, whole, 0.0)
        run = lax.fori_loop(0, nz, plane, jnp.zeros((1, 128), F32))
        for k in range(2 * nx):
            run = run + jnp.where(k < 2 * x, tt[zb, k], 0.0)
        return run, run + tt[zb, 2 * x]

    def offsets(zb):
        return [
            [jnp.sum(jnp.where(lane == h, row, 0.0), axis=1, keepdims=True) for h in range(3)]
            for row in head_offsets(zb)
        ]

    def make_kaug(zb):
        for k in range(2):
            part = jnp.concatenate([kb[zb, k, 256:272, :].astype(F32), jnp.zeros((112, 256), F32)], axis=0)
            kaug[256 * k:256 * k + 256, :] = jnp.transpose(part).astype(BF16)

    spans = ((0, 128), (144, 64), (224, 64))
    row_of = lax.broadcasted_iota(jnp.int32, (128, 256), 0)
    minus = [jnp.where((lax.rem(row_of, 3) == h) & (row_of < 9), -1.0, 0.0).astype(BF16) for h in range(3)]

    def tiles(zb, offs, masked, blocks):
        keys = jnp.concatenate([kb[zb, 0, 0:256, :], kb[zb, 1, 0:256, :]], axis=0)
        vals = jnp.concatenate([vb[zb, 0], vb[zb, 1]], axis=1)
        more = kaug[...]
        ones = jnp.ones((16, 512), BF16)
        work = [(xq, h) for xq in blocks for h in range(3)]
        scores, weights_, shrinks = [], [], []
        for xq, h in work:
            side = slice(0, 128) if h == 0 else slice(128, 256)
            q = qb[xq, side, :]
            if h > 0:
                q = jnp.where(low if h == 1 else jnp.logical_not(low), q, jnp.zeros_like(q))
            scores.append(
                jnp.dot(
                    jnp.concatenate([keys[:, side], more], axis=1),
                    jnp.concatenate([q, minus[h]], axis=0),
                    preferred_element_type=F32,
                )
            )
        for (xq, h), r in zip(work, scores):
            if masked:
                places = lax.broadcasted_iota(jnp.int32, (512, 256), 0) + x * 512
                wanted = lax.broadcasted_iota(jnp.int32, (512, 256), 1) + (xq * 512 + c * 256)
                r = jnp.where(places <= wanted, r, NEG)
            old = mb[xq, h]
            new = old
            for k in range(2):
                new = jnp.maximum(new, jnp.max(r[256 * k:256 * k + 256], axis=0, keepdims=True) - offs[k][h])
            weights_.append(
                jnp.concatenate(
                    [jnp.exp2(r[256 * k:256 * k + 256] - (new + offs[k][h])).astype(BF16) for k in range(2)], axis=0
                )
            )
            shrinks.append(jnp.exp2(old - new))
            mb[xq, h] = new
        for (xq, h), p, shrink in zip(work, weights_, shrinks):
            first, size = ((0, 128), (128, 64), (192, 64))[h]
            pv = jnp.dot(jnp.concatenate([vals[first:first + size], ones], axis=0), p, preferred_element_type=F32)
            some = slice(spans[h][0], spans[h][0] + size + 16)
            acc[xq, some, :] = acc[xq, some, :] * shrink + pv

    def both(zb):
        make_kaug(zb)
        tiles(zb, offsets(zb), False, range(nx))

    relay(jnp.int32(1))
    for i in range(1, nx):
        src = lax.rem(x - i + nx, nx)
        remote(q_ref, qb.at[src], q_s.at[i - 1], q_r.at[i - 1], at(z, src, c, y)).wait_recv()
    for i in range(1, nz):
        slot = tt.at[zdn(i)]
        remote(slot, slot, t2_s.at[i - 1], t2_r.at[i - 1], at(zdn(i), x, c, y)).wait_recv()
    for j in range(2):
        pr_wait(z, j)
    make_kaug(z)
    tiles(z, offsets(z), True, range(nx))

    def one_step(s, carry):
        for j in range(2):
            pr_wait(zdn(s), j)

        @pl.when(z >= s)
        def _():
            both(zdn(s))

        @pl.when(s < half)
        def _():
            relay(s + 1)
            for j in range(2):
                pr_wait(zup(s), j)

        @pl.when((z + s >= nz) & (s < half))
        def _():
            both(zup(s))
        return carry
    lax.fori_loop(1, half, one_step, 0)
    for j in range(2):
        pr_wait(zdn(half), j)
    make_kaug(zdn(half))
    last_offs = offsets(zdn(half))

    def o_copies(i):
        dev = at(z, lax.rem(x + i, nx), c, y)
        return (
            remote(ob.at[i], orv.at[i], o_s.at[i, 0], o_r.at[i, 0], dev),
            remote(sb.at[i], srv.at[i], o_s.at[i, 1], o_r.at[i, 1], dev),
        )

    def finalize(i):
        xq = lax.rem(x + i, nx)
        outs, lses = [], []
        for h in range(3):
            first, size = spans[h]
            total = acc[xq, pl.ds(first + size, 1), :]
            some = total > 0.0
            safe = jnp.where(some, total, 1.0)
            outs.append(acc[xq, pl.ds(first, size), :] / safe)
            lses.append(jnp.where(some, mb[xq, h] + jnp.log2(safe), NEG))
        ob[i] = jnp.concatenate(outs, axis=0).astype(BF16)
        place = lax.broadcasted_iota(jnp.int32, (8, 256), 0)
        sb[i] = jnp.where(place == 0, lses[0], jnp.where(place == 1, lses[1], lses[2]))

        if i > 0:
            for copy in o_copies(i):
                copy.start()

    places_ = [(i + 1) % nx for i in range(nx)]
    for group in ((places_[:nx // 2], places_[nx // 2:]) if nx > 1 else (places_,)):
        @pl.when(z >= half)
        def _():
            tiles(zdn(half), last_offs, False, [lax.rem(x + i, nx) for i in group])
        for i in group:
            finalize(i)

    for i in range(1, nx):
        src = lax.rem(x - i + nx, nx)
        for copy in o_copies(i):
            copy.wait_recv()
    stats = [sb[0]] + [srv[i] for i in range(1, nx)]
    outs = [ob[0]] + [orv[i] for i in range(1, nx)]
    top = functools.reduce(jnp.maximum, stats)
    shares = [jnp.exp2(t - top) for t in stats]
    whole = functools.reduce(jnp.add, shares)
    shares = [t / whole for t in shares]
    merged = [jnp.zeros((128, 256), F32), jnp.zeros((64, 256), F32), jnp.zeros((64, 256), F32)]
    for i in range(nx):
        for h, (first, size) in enumerate(((0, 128), (128, 64), (192, 64))):
            merged[h] = merged[h] + shares[i][h:h + 1] * outs[i][first:first + size].astype(F32)
    ab[...] = jnp.transpose(jnp.concatenate(merged, axis=0)).astype(BF16)

    share = 256 // ny

    def rows_of(y_):
        return ab.at[pl.ds(pl.multiple_of(y_ * share, share), share), :]

    def y_copy(i):
        other = lax.rem(y + i, ny)
        return remote(rows_of(other), ar.at[y], y_s.at[i - 1], y_r.at[i - 1], at(z, x, c, other))

    for i in range(1, ny):
        y_copy(i).start()
    for copy in weights[2:]:
        copy.start()
    ar[y] = ab[pl.ds(pl.multiple_of(y * share, share), share), :]
    for i in range(1, ny):
        src = lax.rem(y - i + ny, ny)
        remote(rows_of(src), ar.at[src], y_s.at[i - 1], y_r.at[i - 1], at(z, x, c, src)).wait_recv()

    for copy in fetch[:3]:
        copy.wait()
    a_wide = jnp.concatenate([ar[k, :, :128] for k in range(ny)], axis=1)
    a_narrow = jnp.concatenate([ar[k, :, 128:] for k in range(ny)], axis=1)
    mixed = jnp.dot(a_wide, ow[...], preferred_element_type=F32) + jnp.dot(a_narrow, on[...], preferred_element_type=F32)
    middle = (res_in[...].astype(F32) + mixed).astype(BF16)
    mid[...] = middle
    middle = middle.astype(F32)
    spread = jnp.mean(middle * middle, axis=1, keepdims=True)
    normed = (middle * lax.rsqrt(spread + epsilon) * gain_ref[...]).astype(BF16)
    picker = jnp.where(chosen[0] | chosen[1], 1.0, 0.0).astype(BF16)
    perm[...] = jnp.dot(picker, normed, preferred_element_type=F32)

    def cut(k, carry):
        v = perm[pl.ds(pl.multiple_of(8 * k, 8), 8), :]
        snd[2 * k] = v[:4].astype(BF16)
        snd[2 * k + 1] = v[4:].astype(BF16)
        return carry
    lax.fori_loop(0, count // 2, cut, 0)

    def to_plane(t):
        return lax.rem(z + near_first(t, nz) + nz, nz)

    def from_plane(t):
        return lax.rem(z - near_first(t, nz) + nz, nz)

    def out_copy(e):
        return remote(snd.at[e], arr.at[sp], a_s.at[e], a_r.at[sp], (e, y))

    def each_other(p, act):
        def one(k, carry):
            e = p * plane + k

            @pl.when(e != sp)
            def _():
                act(e)
            return carry
        lax.fori_loop(0, plane, one, 0)

    def send_rows(t, carry):
        each_other(to_plane(t), lambda e: out_copy(e).start())
        return carry
    lax.fori_loop(0, nz, send_rows, 0)
    keep = pltpu.make_async_copy(snd.at[sp], arr.at[sp], loc2.at[5])
    keep.start()
    keep.wait()

    def to_rows(take):
        for k in range(plane // 2):
            tmp[8 * k:8 * k + 8, :] = jnp.concatenate([take(2 * k).astype(F32), take(2 * k + 1).astype(F32)], axis=0)

    def rows_at(t):
        return pl.ds(pl.multiple_of(t * step, step), step)

    def cross_copy(p):
        some = pl.ds(p * plane, plane)
        return remote(arr.at[some], arc.at[some], c_s.at[p], c_r.at[p], across)

    def arrive_cross(t):
        p = from_plane(t)
        cross_copy(p).wait_recv()
        to_rows(lambda k: arc[p * plane + k])
        xs[rows_at(t), :] = tmp[...].astype(BF16)

    def arrive(t, carry):
        p = from_plane(t)
        each_other(p, lambda s: remote(snd.at[s], arr.at[s], a_s.at[s], a_r.at[s], (s, y)).wait_recv())
        cross_copy(p).start()
        to_rows(lambda k: arr[p * plane + k])
        xo[rows_at(t), :] = tmp[...].astype(BF16)

        @pl.when(t >= nz // 2)
        def _():
            arrive_cross(t - nz // 2)
        return carry
    lax.fori_loop(0, nz, arrive, 0)
    for copy in fetch[3:]:
        copy.wait()
    for copy in weights:
        copy.wait_recv()

    def hidden(x):
        both = []
        for k in range(2):
            g = jnp.dot(x, wg[k], preferred_element_type=F32)
            u = jnp.dot(x, wu[k], preferred_element_type=F32)
            both.append((jax.nn.silu(g) * u).astype(BF16))
        return both

    def down(h, put):
        width = 512
        for q in range(wd.shape[2] // width):
            cols = slice(q * width, (q + 1) * width)
            put(
                cols,
                jnp.dot(h[0], wd[0, :, cols], preferred_element_type=F32)
                + jnp.dot(h[1], wd[1, :, cols], preferred_element_type=F32),
            )

    def part_copy(t):
        some = rows_at(t)
        return remote(part.at[some, :], back.at[some, :], p_s.at[t], p_r.at[t], across)

    order, ahead = return_order(nz)

    def send_part(t, carry):
        part_copy(entry(order, t)).start()
        return carry

    def cross_half(k):
        some = slice(k * step * nz // 2, (k + 1) * step * nz // 2)

        def put(cols, value):
            part[some, cols] = value.astype(BF16)
        down(hidden(xs[some, :]), put)

    def put_total(cols, value):
        total[:, cols] = value
    down(hidden(xo[...]), put_total)
    cross_half(0)
    for t in range(ahead):
        send_part(t, 0)

    def late(t, carry):
        arrive_cross(t)
        return carry
    lax.fori_loop(nz // 2, nz, late, 0)
    cross_half(1)
    lax.fori_loop(ahead, nz, send_part, 0)

    def back_copy(e):
        return remote(bsd.at[e], ret.at[sp], b_s.at[e], b_r.at[sp], (e, y))

    for copy in weights:
        copy.wait_send()

    def drain_rows(t, carry):
        each_other(t, lambda e: out_copy(e).wait_send())
        cross_copy(t).wait_send()
        return carry
    lax.fori_loop(0, nz, drain_rows, 0)
    for j in range(2):
        if up_has(1, j):
            own_up(j).wait_send()
        if dn_has(1, j):
            own_dn(j).wait_send()
        own_pr(j).wait_send()
        for s in range(1, half + 1):
            if up_has(s, j):
                if up_has(s + 1, j):
                    up_copy(s, j).wait_send()
                pr_copy(zdn(s), j).wait_send()
            if dn_has(s, j):
                if dn_has(s + 1, j):
                    dn_copy(s, j).wait_send()
                pr_copy(zup(s), j).wait_send()
    for i in range(1, 2 * nx):
        t1_copy(i).wait_send()
    for i in range(1, nz):
        t2_copy(i).wait_send()
    for i in range(1, nx):
        q_copy(i).wait_send()
        for copy in o_copies(i):
            copy.wait_send()
    for i in range(1, ny):
        y_copy(i).wait_send()

    def finish(u, carry):
        t = entry(order, u)
        p = from_plane(t)
        part_copy(t).wait_recv()
        some = rows_at(t)
        tmp[...] = total[some, :] + back[some, :].astype(F32)
        for k in range(plane // 2):
            v = tmp[8 * k:8 * k + 8, :]
            bsd[p * plane + 2 * k] = v[:4].astype(BF16)
            bsd[p * plane + 2 * k + 1] = v[4:].astype(BF16)
        each_other(p, lambda e: back_copy(e).start())
        return carry
    lax.fori_loop(0, nz, finish, 0)
    last = pltpu.make_async_copy(bsd.at[sp], ret.at[sp], loc2.at[6])
    last.start()
    last.wait()

    def returned(u, carry):
        p = to_plane(entry(order, u))
        each_other(p, lambda e: remote(bsd.at[e], ret.at[e], b_s.at[e], b_r.at[e], (e, y)).wait_recv())
        to_rows(lambda k: ret[p * plane + k])
        rows[rows_at(p), :] = tmp[...].astype(BF16)
        return carry
    lax.fori_loop(0, nz, returned, 0)
    mix = jnp.where(chosen[0], weight_ref[0:1, :], 0.0) + jnp.where(chosen[1], weight_ref[1:2, :], 0.0)
    combined = mid[...].astype(F32)
    for _ in range(3):
        term = mix.astype(BF16)
        mix = mix - term.astype(F32)
        combined = combined + lax.dot_general(
            term, rows[...], (((0,), (0,)), ((), ())), preferred_element_type=F32
        )
    out_ref[...] = combined.astype(BF16)

    def drain(t, carry):
        each_other(t, lambda e: back_copy(e).wait_send())
        part_copy(t).wait_send()
        return carry
    lax.fori_loop(0, nz, drain, 0)


def layer(dims, arrays):
    nz, nx, ny = dims
    half, count = nz // 2, nz * nx * 2
    residual, wide, narrow, gate, up, down = (arrays[i] for i in (0, 9, 10, 14, 15, 16))
    features = residual.shape[1]
    dma = pltpu.SemaphoreType.DMA
    vmem = pl.BlockSpec(memory_space=pltpu.VMEM)
    hbm = pl.BlockSpec(memory_space=pl.ANY)
    blocks = pltpu.VMEM((count, 4, features), BF16)
    table = pltpu.VMEM((4 * count, features), BF16)
    square = pltpu.VMEM((256, 256), BF16)
    return pl.pallas_call(
        functools.partial(layer_kernel, dims),
        out_shape=jax.ShapeDtypeStruct(residual.shape, BF16),
        in_specs=[hbm] * 7 + [vmem] * 2 + [hbm] * 2 + [vmem] * 3 + [hbm] * 3,
        out_specs=vmem,
        scratch_shapes=[
            square,
            pltpu.VMEM((272, 256), BF16),
            square,
            pltpu.VMEM((1, 128), F32),
            pltpu.VMEM((nx, 256, 256), BF16),
            pltpu.VMEM((nz, 2, 272, 256), BF16),
            pltpu.VMEM((nz, 2, 256, 256), BF16),
            pltpu.VMEM((nz, 2 * nx, 1, 128), F32),
            pltpu.VMEM((512, 128), BF16),
            pltpu.VMEM((nx, 3, 1, 256), F32),
            pltpu.VMEM((nx, 304, 256), F32),
            pltpu.VMEM((nx, 256, 256), BF16),
            pltpu.VMEM((nx, 8, 256), F32),
            pltpu.VMEM((nx, 256, 256), BF16),
            pltpu.VMEM((nx, 8, 256), F32),
            square,
            pltpu.VMEM((ny, 256 // ny, 256), BF16),
            dma((nx,)), dma((nx,)),
            dma((half + 1, 2)), dma((half + 1, 2)), dma((half + 1, 2)), dma((half + 1, 2)),
            dma((nz, 2)), dma((nz, 2)),
            dma((2 * nx,)), dma((2 * nx,)), dma((nz,)), dma((nz,)),
            dma((nx, 2)), dma((nx, 2)), dma((ny,)), dma((ny,)), dma((4,)),
            pltpu.VMEM(wide.shape, BF16),
            pltpu.VMEM(narrow.shape, BF16),
            pltpu.VMEM((4 * count, features), F32),
            pltpu.VMEM((8 * nx, features), F32),
            blocks, blocks, blocks, table, table,
            pltpu.VMEM(residual.shape, BF16),
            pltpu.VMEM((2, *gate.shape), BF16),
            pltpu.VMEM((2, *up.shape), BF16),
            pltpu.VMEM((2, *down.shape), BF16),
            pltpu.VMEM((4 * count, features), F32),
            table, table, blocks, blocks, table,
            dma((count,)), dma((count,)), dma((nz,)), dma((nz,)), dma((nz,)), dma((nz,)),
            dma((count,)), dma((count,)), dma((4,)), dma((4,)), dma((14,)),
            pltpu.VMEM((256, 128), BF16), pltpu.VMEM((256, 128), BF16), pltpu.VMEM((256, 128), BF16), pltpu.VMEM((256, 128), BF16),
            pltpu.VMEM(residual.shape, BF16),
        ],
        compiler_params=pltpu.CompilerParams(collective_id=1, has_side_effects=True, vmem_limit_bytes=60 * 2**20),
        cost_estimate=pl.CostEstimate(flops=10**10, bytes_accessed=10**7, transcendentals=10**7),
        name="layer",
    )(*arrays)


def body(
    residual,
    query_wide,
    key_wide,
    value_wide,
    query_narrow,
    key_narrow,
    value_narrow,
    gate_wide,
    gate_narrow,
    out_wide,
    out_narrow,
    norm_gain,
    routing,
    route_weight,
    gate_weight,
    up_weight,
    down_weight,
):
    ny = lax.axis_size("tp")
    nx = NX
    dims = (lax.axis_size("sp") // (2 * nx), nx, ny)
    gate, up, down = gate_weight[0], up_weight[0], down_weight[0]
    return layer(
        dims,
        (
            residual, query_wide, key_wide, value_wide, query_narrow, key_narrow, value_narrow, gate_wide.T, gate_narrow.T,
            out_wide, out_narrow, norm_gain[None, :], routing.T, route_weight.T, gate, up, down,
        ),
    )


def solution(mesh):
    placed = (
        P(("sp", "tp"), None),
        P("sp", "tp"),
        P("sp", "tp"),
        P("sp", "tp"),
        P("sp", "tp"),
        P("sp", "tp"),
        P("sp", "tp"),
        P("sp", "tp"),
        P("sp", "tp"),
        P(),
        P(),
        P(),
        P(("sp", "tp"), None),
        P(("sp", "tp"), None),
        P("sp", None, "tp"),
        P("sp", None, "tp"),
        P("sp", "tp", None),
    )
    return jax.shard_map(
        body, mesh=mesh, in_specs=placed, out_specs=P(("sp", "tp"), None), check_vma=False
    )
```

```python
import functools
import math

import jax
import jax.numpy as jnp
from jax import lax
from jax.experimental import pallas as pl
from jax.experimental.pallas import tpu as pltpu
from jax.sharding import PartitionSpec as P

MESH = pl.DeviceIdType.MESH
F32, BF16 = jnp.float32, jnp.bfloat16
HW = 128
HN = 64
NX = 4
LOG2E = math.log2(math.e)
NEG = -1e30
LOWEST = -1e20
epsilon = 1e-06


def paired(y):
    return lax.rem(y, 2) * (y - 1) + (1 - lax.rem(y, 2)) * (y + 1)


def near_first(t, nz):
    near = nz // 4 * 2
    u = t - jnp.where(t > near, 1, 0)
    m = u // 2 + 1
    return jnp.where(t == near, 0, jnp.where(lax.rem(u, 2) == 0, m, -m))


def return_order(nz):
    if nz == 8:
        return (2, 3, 0, 7, 6, 5, 1, 4), 3
    return tuple(range(nz - 1, -1, -1)), 0


def entry(table, u):
    value = 0
    for i, v in enumerate(table):
        value = jnp.where(u == i, v, value)
    return value


def layer_kernel(
    dims, res_ref, qw_ref, kw_ref, vw_ref, qn_ref, kn_ref, vn_ref, gw_ref, gn_ref, wide_ref, narrow_ref, gain_ref,
    routing_ref, weight_ref, gate_ref, up_ref, down_ref, out_ref,
    q_ref, kd_ref, v_ref, tot_ref, qb, kb, vb, tt, kaug, mb, acc, ob, sb, orv, srv, ab, ar,
    q_s, q_r, up_s, up_r, dn_s, dn_r, pr_s, pr_r, t1_s, t1_r, t2_s, t2_r, o_s, o_r, y_s, y_r, loc,
    ow, on, perm, tmp, snd, arr, arc, xo, xs, mid, wg, wu, wd, total, part, back, bsd, ret, rows,
    a_s, a_r, c_s, c_r, p_s, p_r, b_s, b_r, w_s, w_r, loc2, vw_in, vn_in, qw_in, qn_in, res_in,
):
    nz, nx, ny = dims
    half = nz // 2
    plane = 2 * nx
    count = nz * plane
    step = 4 * plane
    sp, y = lax.axis_index("sp"), lax.axis_index("tp")
    early_in = [
        pltpu.make_async_copy(kw_ref, kd_ref.at[pl.ds(0, 256), pl.ds(0, 128)], loc2.at[7]),
        pltpu.make_async_copy(kn_ref, kd_ref.at[pl.ds(0, 256), pl.ds(128, 128)], loc2.at[8]),
        pltpu.make_async_copy(vw_ref, vw_in, loc2.at[9]),
        pltpu.make_async_copy(vn_ref, vn_in, loc2.at[10]),
        pltpu.make_async_copy(qw_ref, qw_in, loc2.at[11]),
        pltpu.make_async_copy(qn_ref, qn_in, loc2.at[12]),
    ]
    for copy in early_in:
        copy.start()
    fetch = [
        pltpu.make_async_copy(res_ref, res_in, loc2.at[13]),
        pltpu.make_async_copy(wide_ref, ow, loc2.at[0]),
        pltpu.make_async_copy(narrow_ref, on, loc2.at[1]),
        pltpu.make_async_copy(gate_ref, wg.at[0], loc2.at[2]),
        pltpu.make_async_copy(up_ref, wu.at[0], loc2.at[3]),
        pltpu.make_async_copy(down_ref, wd.at[0], loc2.at[4]),
    ]
    for copy in fetch:
        copy.start()
    c = lax.rem(sp, 2)
    x = lax.rem(sp // 2, nx)
    z = sp // (2 * nx)
    xc = x * 2 + c

    def at(z_, x_, c_, y_):
        return ((z_ * nx + x_) * 2 + c_, y_)

    def zup(i):
        return lax.rem(z + i, nz)

    def zdn(i):
        return lax.rem(z - i + nz, nz)

    def in_plane(i):
        other = lax.rem(xc + i, 2 * nx)
        return at(z, other // 2, lax.rem(other, 2), y)

    def remote(src, dst, send, recv, device):
        return pltpu.make_async_remote_copy(
            src_ref=src, dst_ref=dst, send_sem=send, recv_sem=recv, device_id=device, device_id_type=MESH
        )

    barrier = pltpu.get_barrier_semaphore()

    def greet(device):
        pl.semaphore_signal(barrier, inc=1, device_id=device, device_id_type=MESH)

    def greet_along(i, carry):
        greet((lax.rem(sp + i, count), y))
        return carry
    lax.fori_loop(1, count, greet_along, 0)
    for i in range(1, ny):
        greet((sp, lax.rem(y + i, ny)))
    lane = lax.broadcasted_iota(jnp.int32, (1, 128), 1)
    head = lax.broadcasted_iota(jnp.int32, (8, 1), 0)
    gates = jnp.where(head == 0, gw_ref[...], jnp.where(head == 1, gn_ref[0:1, :], gn_ref[1:2, :]))
    logs = jnp.minimum(gates, 0.0) - jnp.log1p(jnp.exp(-jnp.abs(gates)))
    until = lax.broadcasted_iota(jnp.int32, (256, 256), 0) <= lax.broadcasted_iota(jnp.int32, (256, 256), 1)
    until = jnp.where(until, 1.0, 0.0).astype(BF16)
    run = jnp.zeros((8, 256), F32)
    for _ in range(3):
        term = logs.astype(BF16)
        logs = logs - term.astype(F32)
        run = run + jnp.dot(term, until, preferred_element_type=F32)
    left = run * LOG2E
    ends = left[:, 255:256]
    tot_ref[...] = jnp.where(lane == 0, ends[0:1], jnp.where(lane == 1, ends[1:2], ends[2:3]))
    terms = []
    for _ in range(3):
        term = left.astype(BF16).astype(F32)
        left = left - term
        terms.append(term)
    extra = lax.broadcasted_iota(jnp.int32, (16, 1), 0)
    placed = jnp.zeros((16, 256), F32)
    for i in range(3):
        for h in range(3):
            placed = jnp.where(extra == 3 * i + h, terms[i][h:h + 1], placed)
    kd_ref[256:272, :] = placed.astype(BF16)
    for copy in early_in:
        copy.wait()
    v_ref[0:128, :] = jnp.transpose(vw_in[...].astype(F32)).astype(BF16)
    v_ref[128:256, :] = jnp.transpose(vn_in[...].astype(F32)).astype(BF16)
    q_ref[0:128, :] = jnp.transpose(qw_in[...].astype(F32) * (HW ** -0.5 * LOG2E)).astype(BF16)
    q_ref[128:256, :] = jnp.transpose(qn_in[...].astype(F32) * (HN ** -0.5 * LOG2E)).astype(BF16)
    own_rows = routing_ref.shape[1]
    names = [routing_ref[k:k + 1, :].astype(F32) for k in range(2)]
    expert = lax.broadcasted_iota(jnp.int32, (count, own_rows), 0).astype(F32)
    hits = [jnp.where(name == expert, 1.0, 0.0) for name in names]
    earlier = lax.broadcasted_iota(jnp.int32, (own_rows, own_rows), 0) < lax.broadcasted_iota(
        jnp.int32, (own_rows, own_rows), 1
    )
    before = jnp.dot(
        (hits[0] + hits[1]).astype(BF16), jnp.where(earlier, 1.0, 0.0).astype(BF16), preferred_element_type=F32
    )
    slot = lax.broadcasted_iota(jnp.int32, (4 * count, own_rows), 0).astype(F32)
    chosen = [
        slot == names[k] * 4.0 + jnp.sum(before * hits[k], axis=0, keepdims=True) for k in range(2)
    ]
    pl.semaphore_wait(barrier, count - 1 + ny - 1)

    up_dev, dn_dev, pr_dev = at(zup(1), x, c, y), at(zdn(1), x, c, y), at(z, x, 1 - c, y)

    def up_copy(s, j):
        zb = zdn(s)
        src = (kb, vb)[j].at[zb, c]
        return remote(src, src, up_s.at[s, j], up_r.at[s, j], up_dev)

    def dn_copy(s, j):
        zb = zup(s)
        src = (kb, vb)[j].at[zb, c]
        return remote(src, src, dn_s.at[s, j], dn_r.at[s, j], dn_dev)

    def pr_copy(zb, j):
        src = (kb, vb)[j].at[zb, c]
        return remote(src, src, pr_s.at[zb, j], pr_r.at[zb, j], pr_dev)

    def pr_wait(zb, j):
        dst = (kb, vb)[j].at[zb, 1 - c]
        remote(dst, dst, pr_s.at[zb, j], pr_r.at[zb, j], pr_dev).wait_recv()

    def own_up(j):
        return remote((kd_ref, v_ref)[j], (kb, vb)[j].at[z, c], up_s.at[0, j], up_r.at[0, j], up_dev)

    def own_dn(j):
        return remote((kd_ref, v_ref)[j], (kb, vb)[j].at[z, c], dn_s.at[0, j], dn_r.at[0, j], dn_dev)

    def own_pr(j):
        return remote((kd_ref, v_ref)[j], (kb, vb)[j].at[z, c], pr_s.at[z, j], pr_r.at[z, j], pr_dev)

    def up_has(s, j):
        return s < half or (s == half and j == 0)

    def dn_has(s, j):
        return s < half or (s == half and j == 1)

    for j in range(2):
        if up_has(1, j):
            own_up(j).start()
        if dn_has(1, j):
            own_dn(j).start()

    def t1_copy(i):
        return remote(tot_ref, tt.at[z, xc], t1_s.at[i - 1], t1_r.at[i - 1], in_plane(i))

    def t2_copy(i):
        return remote(tt.at[z], tt.at[z], t2_s.at[i - 1], t2_r.at[i - 1], at(zup(i), x, c, y))

    def q_copy(i):
        return remote(q_ref, qb.at[x], q_s.at[i - 1], q_r.at[i - 1], at(z, lax.rem(x + i, nx), c, y))

    for i in range(1, 2 * nx):
        t1_copy(i).start()
    for i in range(1, nx):
        q_copy(i).start()
    for j in range(2):
        own_pr(j).start()
    pair, across = (sp, paired(y)), (sp, ny - 1 - y)
    cut_at = up_ref.shape[0] * 3 // 4
    early, rest = pl.ds(0, cut_at), pl.ds(cut_at, up_ref.shape[0] - cut_at)
    weights = [
        remote(gate_ref, wg.at[1], w_s.at[0], w_r.at[0], pair),
        remote(up_ref.at[early, :], wu.at[1, early, :], w_s.at[1], w_r.at[1], pair),
        remote(up_ref.at[rest, :], wu.at[1, rest, :], w_s.at[2], w_r.at[2], pair),
        remote(down_ref, wd.at[1], w_s.at[3], w_r.at[3], pair),
    ]
    for copy in weights[:2]:
        copy.start()
    local = [
        pltpu.make_async_copy(tot_ref, tt.at[z, xc], loc.at[0]),
        pltpu.make_async_copy(q_ref, qb.at[x], loc.at[1]),
        pltpu.make_async_copy(kd_ref, kb.at[z, c], loc.at[2]),
        pltpu.make_async_copy(v_ref, vb.at[z, c], loc.at[3]),
    ]
    for copy in local:
        copy.start()
    mb[...] = jnp.full(mb.shape, LOWEST, F32)
    acc[...] = jnp.zeros(acc.shape, F32)
    local[0].wait()
    for i in range(1, 2 * nx):
        other = lax.rem(xc - i + 2 * nx, 2 * nx)
        remote(tot_ref, tt.at[z, other], t1_s.at[i - 1], t1_r.at[i - 1], in_plane(i)).wait_recv()
    for i in range(1, nz):
        t2_copy(i).start()
    for copy in local[1:]:
        copy.wait()

    def relay(s, chunks=(0, 1)):
        for j in chunks:
            @pl.when(s <= (half if j == 0 else half - 1))
            def _():
                slot = (kb, vb)[j].at[zdn(s), c]
                remote(slot, slot, up_s.at[s - 1, j], up_r.at[s - 1, j], up_dev).wait_recv()

                @pl.when(s + 1 <= (half if j == 0 else half - 1))
                def _():
                    up_copy(s, j).start()
                pr_copy(zdn(s), j).start()

            @pl.when(s <= (half if j == 1 else half - 1))
            def _():
                slot = (kb, vb)[j].at[zup(s), c]
                remote(slot, slot, dn_s.at[s - 1, j], dn_r.at[s - 1, j], dn_dev).wait_recv()

                @pl.when(s + 1 <= (half if j == 1 else half - 1))
                def _():
                    dn_copy(s, j).start()
                pr_copy(zup(s), j).start()

    low = lax.broadcasted_iota(jnp.int32, (128, 1), 0) < HN

    def head_offsets(zb):
        def plane(p, run):
            whole = jnp.zeros((1, 128), F32)
            for k in range(2 * nx):
                whole = whole + tt[p, k]
            return run + jnp.where(p < zb, whole, 0.0)
        run = lax.fori_loop(0, nz, plane, jnp.zeros((1, 128), F32))
        for k in range(2 * nx):
            run = run + jnp.where(k < 2 * x, tt[zb, k], 0.0)
        return run, run + tt[zb, 2 * x]

    def offsets(zb):
        return [
            [jnp.sum(jnp.where(lane == h, row, 0.0), axis=1, keepdims=True) for h in range(3)]
            for row in head_offsets(zb)
        ]

    def make_kaug(zb):
        for k in range(2):
            part = jnp.concatenate([kb[zb, k, 256:272, :].astype(F32), jnp.zeros((112, 256), F32)], axis=0)
            kaug[256 * k:256 * k + 256, :] = jnp.transpose(part).astype(BF16)

    spans = ((0, 128), (144, 64), (224, 64))
    row_of = lax.broadcasted_iota(jnp.int32, (128, 256), 0)
    minus = [jnp.where((lax.rem(row_of, 3) == h) & (row_of < 9), -1.0, 0.0).astype(BF16) for h in range(3)]

    def tiles(zb, offs, masked, blocks):
        keys = jnp.concatenate([kb[zb, 0, 0:256, :], kb[zb, 1, 0:256, :]], axis=0)
        vals = jnp.concatenate([vb[zb, 0], vb[zb, 1]], axis=1)
        more = kaug[...]
        ones = jnp.ones((16, 512), BF16)
        work = [(xq, h) for xq in blocks for h in range(3)]
        scores, weights_, shrinks = [], [], []
        for xq, h in work:
            side = slice(0, 128) if h == 0 else slice(128, 256)
            q = qb[xq, side, :]
            if h > 0:
                q = jnp.where(low if h == 1 else jnp.logical_not(low), q, jnp.zeros_like(q))
            scores.append(
                jnp.dot(
                    jnp.concatenate([keys[:, side], more], axis=1),
                    jnp.concatenate([q, minus[h]], axis=0),
                    preferred_element_type=F32,
                )
            )
        for (xq, h), r in zip(work, scores):
            if masked:
                places = lax.broadcasted_iota(jnp.int32, (512, 256), 0) + x * 512
                wanted = lax.broadcasted_iota(jnp.int32, (512, 256), 1) + (xq * 512 + c * 256)
                r = jnp.where(places <= wanted, r, NEG)
            old = mb[xq, h]
            new = old
            for k in range(2):
                new = jnp.maximum(new, jnp.max(r[256 * k:256 * k + 256], axis=0, keepdims=True) - offs[k][h])
            weights_.append(
                jnp.concatenate(
                    [jnp.exp2(r[256 * k:256 * k + 256] - (new + offs[k][h])).astype(BF16) for k in range(2)], axis=0
                )
            )
            shrinks.append(jnp.exp2(old - new))
            mb[xq, h] = new
        for (xq, h), p, shrink in zip(work, weights_, shrinks):
            first, size = ((0, 128), (128, 64), (192, 64))[h]
            pv = jnp.dot(jnp.concatenate([vals[first:first + size], ones], axis=0), p, preferred_element_type=F32)
            some = slice(spans[h][0], spans[h][0] + size + 16)
            acc[xq, some, :] = acc[xq, some, :] * shrink + pv

    def both(zb):
        make_kaug(zb)
        tiles(zb, offsets(zb), False, range(nx))

    relay(jnp.int32(1))
    for i in range(1, nx):
        src = lax.rem(x - i + nx, nx)
        remote(q_ref, qb.at[src], q_s.at[i - 1], q_r.at[i - 1], at(z, src, c, y)).wait_recv()
    for i in range(1, nz):
        slot = tt.at[zdn(i)]
        remote(slot, slot, t2_s.at[i - 1], t2_r.at[i - 1], at(zdn(i), x, c, y)).wait_recv()
    for j in range(2):
        pr_wait(z, j)
    relay(jnp.int32(2), (0,))
    make_kaug(z)
    tiles(z, offsets(z), True, range(nx))
    relay(jnp.int32(2), (1,))

    def one_step(s, carry):
        for j in range(2):
            pr_wait(zdn(s), j)

        @pl.when(z >= s)
        def _():
            both(zdn(s))

        @pl.when((s > 1) & (s < half))
        def _():
            relay(s + 1)
        for j in range(2):
            pr_wait(zup(s), j)

        @pl.when((z + s >= nz) & (s < half))
        def _():
            both(zup(s))
        return carry
    lax.fori_loop(1, half, one_step, 0)
    for j in range(2):
        pr_wait(zdn(half), j)
    make_kaug(zdn(half))
    last_offs = offsets(zdn(half))

    def o_copies(i):
        dev = at(z, lax.rem(x + i, nx), c, y)
        return (
            remote(ob.at[i], orv.at[i], o_s.at[i, 0], o_r.at[i, 0], dev),
            remote(sb.at[i], srv.at[i], o_s.at[i, 1], o_r.at[i, 1], dev),
        )

    def finalize(i):
        xq = lax.rem(x + i, nx)
        outs, lses = [], []
        for h in range(3):
            first, size = spans[h]
            total = acc[xq, pl.ds(first + size, 1), :]
            some = total > 0.0
            safe = jnp.where(some, total, 1.0)
            outs.append(acc[xq, pl.ds(first, size), :] / safe)
            lses.append(jnp.where(some, mb[xq, h] + jnp.log2(safe), NEG))
        ob[i] = jnp.concatenate(outs, axis=0).astype(BF16)
        place = lax.broadcasted_iota(jnp.int32, (8, 256), 0)
        sb[i] = jnp.where(place == 0, lses[0], jnp.where(place == 1, lses[1], lses[2]))

        if i > 0:
            for copy in o_copies(i):
                copy.start()

    places_ = [(i + 1) % nx for i in range(nx)]
    for group in ((places_[:nx // 2], places_[nx // 2:]) if nx > 1 else (places_,)):
        @pl.when(z >= half)
        def _():
            tiles(zdn(half), last_offs, False, [lax.rem(x + i, nx) for i in group])
        for i in group:
            finalize(i)

    for i in range(1, nx):
        src = lax.rem(x - i + nx, nx)
        for copy in o_copies(i):
            copy.wait_recv()
    stats = [sb[0]] + [srv[i] for i in range(1, nx)]
    outs = [ob[0]] + [orv[i] for i in range(1, nx)]
    top = functools.reduce(jnp.maximum, stats)
    shares = [jnp.exp2(t - top) for t in stats]
    whole = functools.reduce(jnp.add, shares)
    shares = [t / whole for t in shares]
    merged = [jnp.zeros((128, 256), F32), jnp.zeros((64, 256), F32), jnp.zeros((64, 256), F32)]
    for i in range(nx):
        for h, (first, size) in enumerate(((0, 128), (128, 64), (192, 64))):
            merged[h] = merged[h] + shares[i][h:h + 1] * outs[i][first:first + size].astype(F32)
    ab[...] = jnp.transpose(jnp.concatenate(merged, axis=0)).astype(BF16)

    share = 256 // ny

    def rows_of(y_):
        return ab.at[pl.ds(pl.multiple_of(y_ * share, share), share), :]

    def y_copy(i):
        other = lax.rem(y + i, ny)
        return remote(rows_of(other), ar.at[y], y_s.at[i - 1], y_r.at[i - 1], at(z, x, c, other))

    for i in range(1, ny):
        y_copy(i).start()
    for copy in weights[2:]:
        copy.start()
    ar[y] = ab[pl.ds(pl.multiple_of(y * share, share), share), :]
    for i in range(1, ny):
        src = lax.rem(y - i + ny, ny)
        remote(rows_of(src), ar.at[src], y_s.at[i - 1], y_r.at[i - 1], at(z, x, c, src)).wait_recv()

    for copy in fetch[:3]:
        copy.wait()
    a_wide = jnp.concatenate([ar[k, :, :128] for k in range(ny)], axis=1)
    a_narrow = jnp.concatenate([ar[k, :, 128:] for k in range(ny)], axis=1)
    mixed = jnp.dot(a_wide, ow[...], preferred_element_type=F32) + jnp.dot(a_narrow, on[...], preferred_element_type=F32)
    middle = (res_in[...].astype(F32) + mixed).astype(BF16)
    mid[...] = middle
    middle = middle.astype(F32)
    spread = jnp.mean(middle * middle, axis=1, keepdims=True)
    normed = (middle * lax.rsqrt(spread + epsilon) * gain_ref[...]).astype(BF16)
    picker = jnp.where(chosen[0] | chosen[1], 1.0, 0.0).astype(BF16)
    perm[...] = jnp.dot(picker, normed, preferred_element_type=F32)

    def cut(k, carry):
        v = perm[pl.ds(pl.multiple_of(8 * k, 8), 8), :]
        snd[2 * k] = v[:4].astype(BF16)
        snd[2 * k + 1] = v[4:].astype(BF16)
        return carry
    lax.fori_loop(0, count // 2, cut, 0)

    def to_plane(t):
        return lax.rem(z + near_first(t, nz) + nz, nz)

    def from_plane(t):
        return lax.rem(z - near_first(t, nz) + nz, nz)

    def out_copy(e):
        return remote(snd.at[e], arr.at[sp], a_s.at[e], a_r.at[sp], (e, y))

    def each_other(p, act):
        def one(k, carry):
            e = p * plane + k

            @pl.when(e != sp)
            def _():
                act(e)
            return carry
        lax.fori_loop(0, plane, one, 0)

    def send_rows(t, carry):
        each_other(to_plane(t), lambda e: out_copy(e).start())
        return carry
    lax.fori_loop(0, nz, send_rows, 0)
    keep = pltpu.make_async_copy(snd.at[sp], arr.at[sp], loc2.at[5])
    keep.start()
    keep.wait()

    def to_rows(take):
        for k in range(plane // 2):
            tmp[8 * k:8 * k + 8, :] = jnp.concatenate([take(2 * k).astype(F32), take(2 * k + 1).astype(F32)], axis=0)

    def rows_at(t):
        return pl.ds(pl.multiple_of(t * step, step), step)

    def cross_copy(p):
        some = pl.ds(p * plane, plane)
        return remote(arr.at[some], arc.at[some], c_s.at[p], c_r.at[p], across)

    def arrive_cross(t):
        p = from_plane(t)
        cross_copy(p).wait_recv()
        to_rows(lambda k: arc[p * plane + k])
        xs[rows_at(t), :] = tmp[...].astype(BF16)

    def arrive(t, carry):
        p = from_plane(t)
        each_other(p, lambda s: remote(snd.at[s], arr.at[s], a_s.at[s], a_r.at[s], (s, y)).wait_recv())
        cross_copy(p).start()
        to_rows(lambda k: arr[p * plane + k])
        xo[rows_at(t), :] = tmp[...].astype(BF16)

        @pl.when(t >= nz // 2)
        def _():
            arrive_cross(t - nz // 2)
        return carry
    lax.fori_loop(0, nz, arrive, 0)
    for copy in fetch[3:]:
        copy.wait()
    for copy in weights:
        copy.wait_recv()

    def hidden(x):
        both = []
        for k in range(2):
            g = jnp.dot(x, wg[k], preferred_element_type=F32)
            u = jnp.dot(x, wu[k], preferred_element_type=F32)
            both.append((jax.nn.silu(g) * u).astype(BF16))
        return both

    def down(h, put):
        width = 512
        for q in range(wd.shape[2] // width):
            cols = slice(q * width, (q + 1) * width)
            put(
                cols,
                jnp.dot(h[0], wd[0, :, cols], preferred_element_type=F32)
                + jnp.dot(h[1], wd[1, :, cols], preferred_element_type=F32),
            )

    def part_copy(t):
        some = rows_at(t)
        return remote(part.at[some, :], back.at[some, :], p_s.at[t], p_r.at[t], across)

    order, ahead = return_order(nz)

    def send_part(t, carry):
        part_copy(entry(order, t)).start()
        return carry

    def cross_half(k):
        some = slice(k * step * nz // 2, (k + 1) * step * nz // 2)

        def put(cols, value):
            part[some, cols] = value.astype(BF16)
        down(hidden(xs[some, :]), put)

    def put_total(cols, value):
        total[:, cols] = value
    down(hidden(xo[...]), put_total)
    cross_half(0)
    for t in range(ahead):
        send_part(t, 0)

    def late(t, carry):
        arrive_cross(t)
        return carry
    lax.fori_loop(nz // 2, nz, late, 0)
    cross_half(1)
    lax.fori_loop(ahead, nz, send_part, 0)

    def back_copy(e):
        return remote(bsd.at[e], ret.at[sp], b_s.at[e], b_r.at[sp], (e, y))

    for copy in weights:
        copy.wait_send()

    def drain_rows(t, carry):
        each_other(t, lambda e: out_copy(e).wait_send())
        cross_copy(t).wait_send()
        return carry
    lax.fori_loop(0, nz, drain_rows, 0)
    for j in range(2):
        if up_has(1, j):
            own_up(j).wait_send()
        if dn_has(1, j):
            own_dn(j).wait_send()
        own_pr(j).wait_send()
        for s in range(1, half + 1):
            if up_has(s, j):
                if up_has(s + 1, j):
                    up_copy(s, j).wait_send()
                pr_copy(zdn(s), j).wait_send()
            if dn_has(s, j):
                if dn_has(s + 1, j):
                    dn_copy(s, j).wait_send()
                pr_copy(zup(s), j).wait_send()
    for i in range(1, 2 * nx):
        t1_copy(i).wait_send()
    for i in range(1, nz):
        t2_copy(i).wait_send()
    for i in range(1, nx):
        q_copy(i).wait_send()
        for copy in o_copies(i):
            copy.wait_send()
    for i in range(1, ny):
        y_copy(i).wait_send()

    def finish(u, carry):
        t = entry(order, u)
        p = from_plane(t)
        part_copy(t).wait_recv()
        some = rows_at(t)
        tmp[...] = total[some, :] + back[some, :].astype(F32)
        for k in range(plane // 2):
            v = tmp[8 * k:8 * k + 8, :]
            bsd[p * plane + 2 * k] = v[:4].astype(BF16)
            bsd[p * plane + 2 * k + 1] = v[4:].astype(BF16)
        each_other(p, lambda e: back_copy(e).start())
        return carry
    lax.fori_loop(0, nz, finish, 0)
    last = pltpu.make_async_copy(bsd.at[sp], ret.at[sp], loc2.at[6])
    last.start()
    last.wait()

    def returned(u, carry):
        p = to_plane(entry(order, u))
        each_other(p, lambda e: remote(bsd.at[e], ret.at[e], b_s.at[e], b_r.at[e], (e, y)).wait_recv())
        to_rows(lambda k: ret[p * plane + k])
        rows[rows_at(p), :] = tmp[...].astype(BF16)
        return carry
    lax.fori_loop(0, nz - 1, returned, 0)

    def drain(t, carry):
        each_other(t, lambda e: back_copy(e).wait_send())
        part_copy(t).wait_send()
        return carry
    lax.fori_loop(0, nz, drain, 0)
    returned(nz - 1, 0)
    mix = jnp.where(chosen[0], weight_ref[0:1, :], 0.0) + jnp.where(chosen[1], weight_ref[1:2, :], 0.0)
    combined = mid[...].astype(F32)
    for _ in range(3):
        term = mix.astype(BF16)
        mix = mix - term.astype(F32)
        combined = combined + lax.dot_general(
            term, rows[...], (((0,), (0,)), ((), ())), preferred_element_type=F32
        )
    out_ref[...] = combined.astype(BF16)


def layer(dims, arrays):
    nz, nx, ny = dims
    half, count = nz // 2, nz * nx * 2
    residual, wide, narrow, gate, up, down = (arrays[i] for i in (0, 9, 10, 14, 15, 16))
    features = residual.shape[1]
    dma = pltpu.SemaphoreType.DMA
    vmem = pl.BlockSpec(memory_space=pltpu.VMEM)
    hbm = pl.BlockSpec(memory_space=pl.ANY)
    blocks = pltpu.VMEM((count, 4, features), BF16)
    table = pltpu.VMEM((4 * count, features), BF16)
    square = pltpu.VMEM((256, 256), BF16)
    return pl.pallas_call(
        functools.partial(layer_kernel, dims),
        out_shape=jax.ShapeDtypeStruct(residual.shape, BF16),
        in_specs=[hbm] * 7 + [vmem] * 2 + [hbm] * 2 + [vmem] * 3 + [hbm] * 3,
        out_specs=vmem,
        scratch_shapes=[
            square,
            pltpu.VMEM((272, 256), BF16),
            square,
            pltpu.VMEM((1, 128), F32),
            pltpu.VMEM((nx, 256, 256), BF16),
            pltpu.VMEM((nz, 2, 272, 256), BF16),
            pltpu.VMEM((nz, 2, 256, 256), BF16),
            pltpu.VMEM((nz, 2 * nx, 1, 128), F32),
            pltpu.VMEM((512, 128), BF16),
            pltpu.VMEM((nx, 3, 1, 256), F32),
            pltpu.VMEM((nx, 304, 256), F32),
            pltpu.VMEM((nx, 256, 256), BF16),
            pltpu.VMEM((nx, 8, 256), F32),
            pltpu.VMEM((nx, 256, 256), BF16),
            pltpu.VMEM((nx, 8, 256), F32),
            square,
            pltpu.VMEM((ny, 256 // ny, 256), BF16),
            dma((nx,)), dma((nx,)),
            dma((half + 1, 2)), dma((half + 1, 2)), dma((half + 1, 2)), dma((half + 1, 2)),
            dma((nz, 2)), dma((nz, 2)),
            dma((2 * nx,)), dma((2 * nx,)), dma((nz,)), dma((nz,)),
            dma((nx, 2)), dma((nx, 2)), dma((ny,)), dma((ny,)), dma((4,)),
            pltpu.VMEM(wide.shape, BF16),
            pltpu.VMEM(narrow.shape, BF16),
            pltpu.VMEM((4 * count, features), F32),
            pltpu.VMEM((8 * nx, features), F32),
            blocks, blocks, blocks, table, table,
            pltpu.VMEM(residual.shape, BF16),
            pltpu.VMEM((2, *gate.shape), BF16),
            pltpu.VMEM((2, *up.shape), BF16),
            pltpu.VMEM((2, *down.shape), BF16),
            pltpu.VMEM((4 * count, features), F32),
            table, table, blocks, blocks, table,
            dma((count,)), dma((count,)), dma((nz,)), dma((nz,)), dma((nz,)), dma((nz,)),
            dma((count,)), dma((count,)), dma((4,)), dma((4,)), dma((14,)),
            pltpu.VMEM((256, 128), BF16), pltpu.VMEM((256, 128), BF16), pltpu.VMEM((256, 128), BF16), pltpu.VMEM((256, 128), BF16),
            pltpu.VMEM(residual.shape, BF16),
        ],
        compiler_params=pltpu.CompilerParams(collective_id=1, has_side_effects=True, vmem_limit_bytes=60 * 2**20),
        cost_estimate=pl.CostEstimate(flops=10**10, bytes_accessed=10**7, transcendentals=10**7),
        name="layer",
    )(*arrays)


def body(
    residual,
    query_wide,
    key_wide,
    value_wide,
    query_narrow,
    key_narrow,
    value_narrow,
    gate_wide,
    gate_narrow,
    out_wide,
    out_narrow,
    norm_gain,
    routing,
    route_weight,
    gate_weight,
    up_weight,
    down_weight,
):
    ny = lax.axis_size("tp")
    nx = NX
    dims = (lax.axis_size("sp") // (2 * nx), nx, ny)
    gate, up, down = gate_weight[0], up_weight[0], down_weight[0]
    return layer(
        dims,
        (
            residual, query_wide, key_wide, value_wide, query_narrow, key_narrow, value_narrow, gate_wide.T, gate_narrow.T,
            out_wide, out_narrow, norm_gain[None, :], routing.T, route_weight.T, gate, up, down,
        ),
    )


def solution(mesh):
    placed = (
        P(("sp", "tp"), None),
        P("sp", "tp"),
        P("sp", "tp"),
        P("sp", "tp"),
        P("sp", "tp"),
        P("sp", "tp"),
        P("sp", "tp"),
        P("sp", "tp"),
        P("sp", "tp"),
        P(),
        P(),
        P(),
        P(("sp", "tp"), None),
        P(("sp", "tp"), None),
        P("sp", None, "tp"),
        P("sp", None, "tp"),
        P("sp", "tp", None),
    )
    return jax.shard_map(
        body, mesh=mesh, in_specs=placed, out_specs=P(("sp", "tp"), None), check_vma=False
    )
```
